32 devices in a mesh: grp: 2 (over y), sp: 4 (over z), fs: 2 (over x), tp: 2 (over core).
Axes of the slice: x: 2, y: 2, z: 4, core: 2. Of those that a mesh axis runs over, the one named last changes fastest.
Arguments:
- tokens: bfloat16 [4, 512, 2048], P(('grp', 'fs'), 'sp'), parts along dimension 0, may hold values from -6 to 6
- norm_gain: float32 [2048], replicated, may hold values from 0.1 to 1.9
- query_attend: bfloat16 [2048, 8, 128], P(None, ('fs', 'tp')), may hold values from -0.125 to 0.125
- key_attend: bfloat16 [2048, 8, 128], P(None, ('fs', 'tp')), may hold values from -0.125 to 0.125
- value_attend: bfloat16 [2048, 8, 128], P(None, ('fs', 'tp')), may hold values from -0.125 to 0.125
- query_linear: bfloat16 [2048, 8, 128], P(None, ('fs', 'tp')), may hold values from -0.125 to 0.125
- key_linear: bfloat16 [2048, 8, 128], P(None, ('fs', 'tp')), may hold values from -0.125 to 0.125
- value_linear: bfloat16 [2048, 8, 256], P(None, ('fs', 'tp')), may hold values from -0.125 to 0.125
- decay_down: bfloat16 [2048, 32], replicated, may hold values from -0.125 to 0.125
- decay_up: bfloat16 [32, 8, 128], replicated, may hold values from -2.109375 to 2.109375
- decay_bias: float32 [8, 128], replicated, may hold values from -1.5 to 7.5
- log_retain: float32 [4, 512, 8], P(('grp', 'fs'), 'sp'), parts along dimension 0, may hold values from -1.5 to 0
- query_gain: float32 [64], replicated, may hold values from 0.6 to 4
- key_gain: float32 [8, 2, 64], replicated, may hold values from 0.8 to 14
- diff_lambda: float32 [8], replicated, may hold values from 0.3 to 0.8
- mix_gain: float32 [128], replicated, may hold values from 0.1 to 1.9
- state_gain: float32 [256], replicated, may hold values from 0.1 to 1.9
- init_state: float32 [4, 8, 128, 256], P('grp', ('fs', 'tp')), parts along dimension 0, may hold values from -80 to 80
- output_attend: bfloat16 [1024, 2048], P(None, 'tp'), may hold values from -0.109375 to 0.109375
- output_linear: bfloat16 [2048, 2048], P(None, 'tp'), may hold values from -0.109375 to 0.109375
Outputs:
- mixed_out: bfloat16 [4, 512, 2048], P(('grp', 'fs'), 'sp', 'tp'), parts along dimension 0
The draws below stay inside these ranges and needn't reach their ends.
There are 2 independent parts, one for each index of `grp`. The reference program is written for one: setup_inputs(seed, part) draws one part's arguments, and reference() takes and returns one part's arrays. A program takes and returns all parts, laid end to end along the dimension named above; an argument that names none is the same for every part. Nothing has to cross between parts.
All inputs are finite; a program needn't handle non-finite values.
Results may differ from the reference program's by a relative error of at most 0.018.
The reference program's roundings to bfloat16 on the way count: a program that leaves them out, or rounds other values in their place, can miss the bound.
Values may be sent and summed in bfloat16 or wider, within the bound.
A program may use at most 128 MiB of HBM per device.

```python
import math
import jax
import jax.numpy as jnp
from jax import lax

D = 2048
MIXER_HEADS = 8
HD_A = 64
DV_A = 128
HDK = 128
HDV = 256
RANK = 32
BLK = 64
TOK_DEV = 128
SEQUENCE_LENGTH = 512
SEQUENCE_COUNT = 2
N_SP = 4


def draw_query_gain(key, part):
    return jax.random.uniform(key, (HD_A,), jnp.float32, 0.6, 2.0)


def draw_key_gain(key, part):
    level_key = jax.random.fold_in(key, 11)
    channel_key = jax.random.fold_in(key, 12)
    level = jax.random.uniform(level_key, (MIXER_HEADS, 2, 1), jnp.float32, 1.2, 1.6)
    return level * jax.random.uniform(channel_key, (MIXER_HEADS, 2, HD_A), jnp.float32, 0.85, 1.15)


def draw_decay_bias(key, part):
    pick_key = jax.random.fold_in(key, 21)
    fast_key = jax.random.fold_in(key, 22)
    slow_key = jax.random.fold_in(key, 23)
    share = 0.5
    fast_pick = jax.random.uniform(pick_key, (MIXER_HEADS, HDK), jnp.float32) < share
    fast_value = jax.random.uniform(fast_key, (MIXER_HEADS, HDK), jnp.float32, -1.5, 0.5)
    slow_value = jax.random.uniform(slow_key, (MIXER_HEADS, HDK), jnp.float32, 6.0, 7.5)
    return jnp.where(fast_pick, fast_value, slow_value)


def draw_log_retain(key, part):
    rate_key = jax.random.fold_in(key, 31)
    spot_key = jax.random.fold_in(key, 32)
    random_depth_key = jax.random.fold_in(key, 33)
    block_total = SEQUENCE_LENGTH // TOK_DEV
    factor = jnp.exp(jax.random.uniform(rate_key, (SEQUENCE_COUNT, block_total, 1, MIXER_HEADS), jnp.float32, math.log(0.5), math.log(2.0)))
    position_offset = jnp.broadcast_to(-0.8 / SEQUENCE_LENGTH * factor, (SEQUENCE_COUNT, block_total, TOK_DEV, MIXER_HEADS)).reshape(SEQUENCE_COUNT, SEQUENCE_LENGTH, MIXER_HEADS)
    spike_positions = jax.random.randint(spot_key, (SEQUENCE_COUNT, 1, MIXER_HEADS, 2), 0, SEQUENCE_LENGTH)
    spike_depth = jnp.log(jax.random.uniform(random_depth_key, (SEQUENCE_COUNT, 1, MIXER_HEADS, 2), jnp.float32, 0.5, 0.8))
    spike_location = jnp.arange(SEQUENCE_LENGTH, dtype=jnp.int32)[None, :, None, None] == spike_positions
    spike_total = jnp.sum(jnp.where(spike_location, spike_depth, 0.0), axis=-1)
    return position_offset + spike_total


def shard_levels(key, extent, shards, smallest, high):
    loudness, own = 1.0, jax.random.fold_in(key, 6)
    for dim, blocks in shards:
        draws = jnp.exp(jax.random.uniform(jax.random.fold_in(own, dim), (blocks,), jnp.float32, smallest / len(shards), high / len(shards)))
        loudness = loudness * jnp.repeat(draws, extent[dim] // blocks).reshape([-1 if axis == dim else 1 for axis in range(len(extent))])
    return loudness


def normal_values(own_key, shape, width, reach, split=(), kind=jnp.bfloat16):
    result = jax.random.normal(own_key, shape, jnp.float32) * width
    if len(split) > 0:
        result = shard_levels(own_key, shape, split, -0.22, 0.18) * result
    return jnp.clip(result, min=-reach, max=reach).astype(kind)


def setup_inputs(seed: int = 0, part: int = 0) -> dict:
    arg_keys = jax.random.split(jax.random.key(seed), 21)
    part_splits = jax.random.split(jax.random.fold_in(arg_keys[20], part), 21)
    tokens = normal_values(part_splits[0], (SEQUENCE_COUNT, SEQUENCE_LENGTH, D), 1.0, 6.0, ((0, 2), (1, 4)))
    norm_gain = jnp.clip(1.0 + 0.18 * jax.random.normal(arg_keys[1], (D,), jnp.float32), 0.1, 1.9)
    query_attend = normal_values(arg_keys[2], (D, MIXER_HEADS, 2 * HD_A), D ** -0.5, 0.125, ((1, 4),))
    key_attend = normal_values(arg_keys[3], (D, MIXER_HEADS, 2 * HD_A), D ** -0.5, 0.125, ((1, 4),))
    value_attend = normal_values(arg_keys[4], (D, MIXER_HEADS, DV_A), D ** -0.5, 0.125, ((1, 4),))
    query_linear = normal_values(arg_keys[5], (D, MIXER_HEADS, HDK), D ** -0.5, 0.125, ((1, 4),))
    key_linear = normal_values(arg_keys[6], (D, MIXER_HEADS, HDK), D ** -0.5, 0.125, ((1, 4),))
    value_linear = normal_values(arg_keys[7], (D, MIXER_HEADS, HDV), D ** -0.5, 0.125, ((1, 4),))
    decay_down = normal_values(arg_keys[8], (D, RANK), D ** -0.5, 0.125)
    decay_up = normal_values(arg_keys[9], (RANK, MIXER_HEADS, HDK), (2.0 / RANK ** 0.5), 2.109375)
    decay_bias = draw_decay_bias(jax.random.fold_in(arg_keys[20], 71), part)
    log_retain = draw_log_retain(jax.random.fold_in(jax.random.fold_in(arg_keys[20], part), 71), part)
    query_gain = draw_query_gain(jax.random.fold_in(arg_keys[20], 71), part)
    key_gain = draw_key_gain(jax.random.fold_in(arg_keys[20], 71), part)
    diff_lambda = jnp.clip(jax.random.uniform(arg_keys[14], (MIXER_HEADS,), jnp.float32, 0.3, 0.8), 0.3, 0.8)
    mix_gain = jnp.clip(1.0 + 0.18 * jax.random.normal(arg_keys[15], (DV_A,), jnp.float32), 0.1, 1.9)
    state_gain = jnp.clip(1.0 + 0.18 * jax.random.normal(arg_keys[16], (HDV,), jnp.float32), 0.1, 1.9)
    init_state = normal_values(part_splits[17], (SEQUENCE_COUNT, MIXER_HEADS, HDK, HDV), (0.6 * (TOK_DEV * N_SP) ** 0.5), 80.0, ((1, 4),), jnp.float32)
    output_attend = normal_values(arg_keys[18], (MIXER_HEADS * DV_A, D), (MIXER_HEADS * (DV_A + HDV)) ** -0.5, 0.109375, ((1, 2),))
    output_linear = normal_values(arg_keys[19], (MIXER_HEADS * HDV, D), (MIXER_HEADS * (DV_A + HDV)) ** -0.5, 0.109375, ((1, 2),))
    return dict(tokens=tokens, norm_gain=norm_gain, query_attend=query_attend, key_attend=key_attend, value_attend=value_attend, query_linear=query_linear, key_linear=key_linear, value_linear=value_linear, decay_down=decay_down, decay_up=decay_up, decay_bias=decay_bias, log_retain=log_retain, query_gain=query_gain, key_gain=key_gain, diff_lambda=diff_lambda, mix_gain=mix_gain, state_gain=state_gain, init_state=init_state, output_attend=output_attend, output_linear=output_linear)


norm_eps = 1e-06
decay_tau = 16.0

def rms_scale(values, gain):
    widened = values.astype(jnp.float32)
    return widened * lax.rsqrt(lax.optimization_barrier(jnp.mean(widened * widened, axis=-1, keepdims=True)) + norm_eps) * gain

def widen(values):
    return lax.optimization_barrier(values).astype(jnp.float32)

def gated_linear(queries, keys_in, values_in, log_decay, first_state):
    length, head_count, key_dim = queries.shape
    block_count = length // BLK
    highest_precision = lax.Precision.HIGHEST

    def split_blocks(source):
        return source.reshape(block_count, BLK, head_count, source.shape[-1])
    causal = (jnp.arange(BLK, dtype=jnp.int32)[:, None] >= jnp.arange(BLK, dtype=jnp.int32)[None, :])[None]

    def advance(recurrent_state, inputs_now):
        question_patch_lines, block_k, value_tile_width, block_log = inputs_now
        running_state = jnp.cumsum(block_log, axis=0)
        pivot = running_state[BLK // 2]
        q_scaled = question_patch_lines * jnp.exp(running_state - pivot[None])
        k_scaled = block_k * jnp.exp(pivot[None] - running_state)
        scores = jnp.einsum('thk,shk->hts', q_scaled, k_scaled, precision=highest_precision)
        scores = jnp.where(causal, scores, 0.0)
        inside_block = jnp.einsum('hts,shv->thv', scores, value_tile_width, precision=highest_precision)
        inside_block = inside_block + jnp.einsum('jwo,wos->jws', question_patch_lines * jnp.exp(running_state), recurrent_state, precision=highest_precision)
        final_state = running_state[-1]
        faded_memory_matrix = block_k * jnp.exp(final_state[None] - running_state)
        recurrent_state = recurrent_state * jnp.exp(final_state)[:, :, None] + jnp.einsum('zcb,zcw->cbw', faded_memory_matrix, value_tile_width, precision=highest_precision)
        return (recurrent_state, inside_block)
    _, outputs = lax.scan(advance, first_state, (split_blocks(queries), split_blocks(keys_in), split_blocks(values_in), split_blocks(log_decay)))
    return outputs.reshape(length, head_count, values_in.shape[-1])

def reference(tokens, norm_gain, query_attend, key_attend, value_attend, query_linear, key_linear, value_linear, decay_down, decay_up, decay_bias, log_retain, query_gain, key_gain, diff_lambda, mix_gain, state_gain, init_state, output_attend, output_linear):

    def one_sequence(inputs_now):
        seq_tokens, seq_retain, seq_state = inputs_now
        seq_len = seq_tokens.shape[0]
        normed = rms_scale(seq_tokens, norm_gain).astype(jnp.bfloat16)

        def project(weight):
            return jnp.dot(normed, weight.reshape(weight.shape[0], -1), preferred_element_type=jnp.float32).astype(jnp.bfloat16)
        q_unit = rms_scale(project(query_attend).reshape(seq_len, MIXER_HEADS, 2, HD_A), query_gain).astype(jnp.bfloat16)
        k_unit = rms_scale(project(key_attend).reshape(seq_len, MIXER_HEADS, 2, HD_A), key_gain).astype(jnp.bfloat16)
        v_attend = project(value_attend).reshape(seq_len, MIXER_HEADS, DV_A)
        key_wide = widen(k_unit)
        value_wide = widen(v_attend)
        position_block = jnp.arange(seq_len, dtype=jnp.int32) // BLK

        def attend(block_index):
            first_row = (block_index * TOK_DEV).astype(jnp.int32)
            query_rows = widen(lax.dynamic_slice_in_dim(q_unit, first_row, TOK_DEV, 0))
            query_block = lax.dynamic_slice_in_dim(position_block, first_row, TOK_DEV, 0)
            scores = jnp.einsum('qhmd,khmd->hmqk', query_rows, key_wide) * HD_A ** (-0.5)
            allowed = query_block[:, None] >= position_block[None, :]
            scores = jnp.where(allowed, scores, -jnp.inf)
            top = lax.optimization_barrier(jnp.max(scores, axis=-1, keepdims=True))
            raised = jnp.exp(scores - top)
            totals = lax.optimization_barrier(jnp.sum(raised, axis=-1))
            sums = jnp.einsum('hmqk,khv->hmqv', widen(raised.astype(jnp.bfloat16)), value_wide)
            return sums[:, 0] / totals[:, 0, :, None] - diff_lambda[:, None, None] * sums[:, 1] / totals[:, 1, :, None]
        diff_raw = lax.map(attend, jnp.arange(seq_len // TOK_DEV, dtype=jnp.int32))
        diff_raw = jnp.transpose(diff_raw, (0, 2, 1, 3)).reshape(seq_len, MIXER_HEADS, DV_A)
        attend_out = rms_scale(diff_raw, mix_gain).astype(jnp.bfloat16)
        q_lin = project(query_linear).reshape(seq_len, MIXER_HEADS, HDK)
        k_lin = project(key_linear).reshape(seq_len, MIXER_HEADS, HDK)
        v_lin = project(value_linear).reshape(seq_len, MIXER_HEADS, HDV)
        low_rank = jnp.dot(normed, decay_down, preferred_element_type=jnp.float32).astype(jnp.bfloat16)
        pre_act = jnp.dot(low_rank, decay_up.reshape(RANK, -1), preferred_element_type=jnp.float32).reshape(seq_len, MIXER_HEADS, HDK) + decay_bias
        log_decay = jax.nn.log_sigmoid(pre_act) / decay_tau + seq_retain[:, :, None]
        linear_raw = gated_linear(widen(q_lin) * HDK ** (-0.5), widen(k_lin), widen(v_lin), log_decay, seq_state)
        linear_out = rms_scale(linear_raw, state_gain).astype(jnp.bfloat16)
        total = jnp.dot(attend_out.reshape(seq_len, -1), output_attend, preferred_element_type=jnp.float32)
        total = total + jnp.dot(linear_out.reshape(seq_len, -1), output_linear, preferred_element_type=jnp.float32)
        return total.astype(jnp.bfloat16)
    return lax.map(one_sequence, (tokens, log_retain, init_state))
```

```python
import functools

import jax
import jax.numpy as jnp
from jax import lax
from jax.experimental import pallas as pl
from jax.experimental.pallas import tpu as pltpu
from jax.sharding import PartitionSpec as P

MIXER_HEADS = 8
HD_A = 64
DV_A = 128
HDK = 128
HDV = 256
BLK = 64


norm_eps = 1e-06
decay_tau = 16.0


def entering(part, axis, combine, identity):
    place = lax.axis_index(axis)
    gathered = jax.tree.map(lambda a: lax.all_gather(a, axis), part)
    state = jax.tree.map(lambda a, e: jnp.zeros_like(a) + jnp.asarray(e, a.dtype), part, identity)

    def one(hop, state):
        return combine(
            state, jax.tree.map(lambda a: lax.dynamic_index_in_dim(a, hop, 0, False), gathered)
        )

    return lax.fori_loop(0, place, one, state)


def rms_scale(values, gain):
    widened = values.astype(jnp.float32)
    return (
        widened * lax.rsqrt(jnp.mean(widened * widened, axis=-1, keepdims=True) + norm_eps) * gain
    )


def head_order(fs_size, tp_size, tp_rank):
    per_device = MIXER_HEADS // (fs_size * tp_size)
    owners = jnp.arange(fs_size, dtype=jnp.int32)[:, None] * tp_size + tp_rank
    return (owners * per_device + jnp.arange(per_device, dtype=jnp.int32)[None, :]).reshape(-1)


def linear_blocks(queries, keys_in, values_in, log_decay):
    tok_rows, head_count, key_dim = queries.shape
    value_dim = values_in.shape[-1]
    block_count = tok_rows // BLK
    highest_precision = lax.Precision.HIGHEST

    def split_blocks(source):
        return source.reshape(block_count, BLK, head_count, source.shape[-1])

    causal = (
        jnp.arange(BLK, dtype=jnp.int32)[:, None] >= jnp.arange(BLK, dtype=jnp.int32)[None, :]
    )[None]

    def advance(carry, inputs_now):
        recurrent_state, offset = carry
        question_patch_lines, block_k, value_tile_width, block_log = inputs_now
        running_state = jnp.cumsum(block_log, axis=0)
        pivot = running_state[BLK // 2]
        q_scaled = question_patch_lines * jnp.exp(running_state - pivot[None])
        k_scaled = block_k * jnp.exp(pivot[None] - running_state)
        scores = jnp.einsum("thk,shk->hts", q_scaled, k_scaled, precision=highest_precision)
        scores = jnp.where(causal, scores, 0.0)
        inside_block = jnp.einsum(
            "hts,shv->thv", scores, value_tile_width, precision=highest_precision
        )
        inside_block = inside_block + jnp.einsum(
            "jwo,wos->jws",
            question_patch_lines * jnp.exp(running_state),
            recurrent_state,
            precision=highest_precision,
        )
        final_state = running_state[-1]
        faded_memory_matrix = block_k * jnp.exp(final_state[None] - running_state)
        recurrent_state = recurrent_state * jnp.exp(final_state)[:, :, None] + jnp.einsum(
            "zcb,zcw->cbw", faded_memory_matrix, value_tile_width, precision=highest_precision
        )
        reaching_keys = question_patch_lines * jnp.exp(offset[None] + running_state)
        return ((recurrent_state, offset + final_state), (inside_block, reaching_keys))

    start_carry = (
        jnp.zeros((head_count, key_dim, value_dim), jnp.float32),
        jnp.zeros((head_count, key_dim), jnp.float32),
    )
    (recurrent_state, total_decay), (inside_block, reaching_keys) = lax.scan(
        advance,
        start_carry,
        (
            split_blocks(queries),
            split_blocks(keys_in),
            split_blocks(values_in),
            split_blocks(log_decay),
        ),
    )
    return (
        recurrent_state,
        total_decay,
        inside_block.reshape(tok_rows, head_count, value_dim),
        reaching_keys.reshape(tok_rows, head_count, key_dim),
    )


def body(
    tokens,
    norm_gain,
    query_attend,
    key_attend,
    value_attend,
    query_linear,
    key_linear,
    value_linear,
    decay_down,
    decay_up,
    decay_bias,
    log_retain,
    query_gain,
    key_gain,
    diff_lambda,
    mix_gain,
    state_gain,
    init_state,
    output_attend,
    output_linear,
):
    fs_size = lax.axis_size("fs")
    tp_size = lax.axis_size("tp")
    tp_rank = lax.axis_index("tp")
    tok_rows = tokens.shape[1]
    normed = rms_scale(tokens, norm_gain).astype(jnp.bfloat16)
    normed_rows = normed[0]
    local_weights = (query_attend, key_attend, value_attend, query_linear, key_linear, value_linear)
    widths = [weight.shape[1] * weight.shape[2] for weight in local_weights]
    packed = jnp.concatenate(
        [weight.reshape(weight.shape[0], -1) for weight in local_weights], axis=1
    )
    computed = jnp.einsum(
        "std,dp->stp",
        lax.all_gather(normed, "fs", axis=0, tiled=True),
        packed,
        preferred_element_type=jnp.float32,
    ).astype(jnp.bfloat16)
    arrived = lax.all_to_all(computed, "fs", split_axis=0, concat_axis=2, tiled=True).reshape(
        tok_rows, fs_size, -1
    )
    sections = []
    column_at = 0
    for weight, width_now in zip(local_weights, widths):
        section = arrived[:, :, column_at : column_at + width_now]
        sections.append(section.reshape(tok_rows, fs_size * weight.shape[1], weight.shape[2]))
        column_at = column_at + width_now
    projected = tuple(sections)
    q_pair, k_pair, v_attend, q_lin, k_lin, v_lin = projected
    head_ids = head_order(fs_size, tp_size, tp_rank)
    head_count = head_ids.shape[0]
    q_unit = rms_scale(q_pair.reshape(tok_rows, head_count, 2, HD_A), query_gain).astype(
        jnp.bfloat16
    )
    k_unit = rms_scale(
        k_pair.reshape(tok_rows, head_count, 2, HD_A), jnp.take(key_gain, head_ids, axis=0)
    ).astype(jnp.bfloat16)
    sp_start = lax.axis_index("sp") * tok_rows
    query_block = (sp_start + jnp.arange(tok_rows, dtype=jnp.int32)) // BLK
    score_scale = HD_A ** (-0.5)
    blank_attend = (
        jnp.full((head_count, 2, tok_rows), -jnp.inf, jnp.float32),
        jnp.zeros((head_count, 2, tok_rows), jnp.float32),
        jnp.zeros((head_count, 2, tok_rows, DV_A), jnp.float32),
    )
    carry = blank_attend
    seg_keys = lax.all_gather(k_unit, "sp", axis=0, tiled=True)
    seg_values = lax.all_gather(v_attend, "sp", axis=0, tiled=True)
    span = seg_keys.shape[0]
    stride_token_lines = 2 * tok_rows
    step_count = span // stride_token_lines
    key_steps = seg_keys.reshape(step_count, stride_token_lines, head_count, 2, HD_A)
    value_steps = seg_values.reshape(step_count, stride_token_lines, head_count, DV_A)

    def one_step(running_state, inputs_now):
        step_index, key_step, value_step = inputs_now
        key_start = step_index * stride_token_lines

        def compute(current):
            run_max, run_total, run_acc = current
            scores = (
                jnp.einsum("qhmd,khmd->hmqk", q_unit, key_step, preferred_element_type=jnp.float32)
                * score_scale
            )
            key_block = (key_start + jnp.arange(stride_token_lines, dtype=jnp.int32)) // BLK
            allowed = query_block[:, None] >= key_block[None, :]
            scores = jnp.where(allowed, scores, -jnp.inf)
            new_max = jnp.maximum(run_max, jnp.max(scores, axis=-1))
            factor = jnp.exp(run_max - new_max)
            raised = jnp.exp(scores - new_max[..., None])
            run_total = run_total * factor + jnp.sum(raised, axis=-1)
            run_acc = run_acc * factor[..., None] + jnp.einsum(
                "hmqk,khv->hmqv",
                raised.astype(jnp.bfloat16),
                value_step,
                preferred_element_type=jnp.float32,
            )
            return (new_max, run_total, run_acc)

        def unchanged(current):
            return current

        return (lax.cond(key_start <= sp_start, compute, unchanged, running_state), None)

    carry, _ = lax.scan(
        one_step, carry, (jnp.arange(step_count, dtype=jnp.int32), key_steps, value_steps)
    )
    run_max, run_total, run_acc = carry
    lambda_heads = jnp.take(diff_lambda, head_ids, axis=0)
    diff_raw = (
        run_acc[:, 0] / run_total[:, 0, :, None]
        - lambda_heads[:, None, None] * run_acc[:, 1] / run_total[:, 1, :, None]
    )
    attend_out = rms_scale(jnp.transpose(diff_raw, (1, 0, 2)), mix_gain).astype(jnp.bfloat16)
    low_rank = jnp.dot(normed_rows, decay_down, preferred_element_type=jnp.float32).astype(
        jnp.bfloat16
    )
    up_columns = jnp.take(decay_up, head_ids, axis=1)
    pre_act = jnp.einsum(
        "tr,rhk->thk", low_rank, up_columns, preferred_element_type=jnp.float32
    ) + jnp.take(decay_bias, head_ids, axis=0)
    retain_heads = jnp.take(log_retain[0], head_ids, axis=1)
    log_decay = jax.nn.log_sigmoid(pre_act) / decay_tau + retain_heads[:, :, None]
    local_state, local_decay, inside_block, reaching_keys = linear_blocks(
        q_lin.astype(jnp.float32) * HDK ** (-0.5),
        k_lin.astype(jnp.float32),
        v_lin.astype(jnp.float32),
        log_decay,
    )

    def chain(earlier, later):
        return (earlier[0] + later[0], earlier[1] * jnp.exp(later[0])[:, :, None] + later[1])

    zero_chain = (jnp.zeros_like(local_decay), jnp.zeros_like(local_state))
    prior_decay, prior_state = entering((local_decay, local_state), "sp", chain, zero_chain)
    start_state = lax.all_to_all(init_state, "fs", split_axis=0, concat_axis=1, tiled=True)[0]
    incoming_state = start_state * jnp.exp(prior_decay)[:, :, None] + prior_state
    linear_raw = inside_block + jnp.einsum(
        "jwo,wos->jws", reaching_keys, incoming_state, precision=lax.Precision.HIGHEST
    )
    linear_out = rms_scale(linear_raw, state_gain).astype(jnp.bfloat16)
    out_cols = output_attend.shape[1]
    per_device = MIXER_HEADS // (fs_size * tp_size)
    attend_view = output_attend.reshape(fs_size, tp_size, per_device * DV_A, out_cols)
    linear_view = output_linear.reshape(fs_size, tp_size, per_device * HDV, out_cols)
    blank_out = jnp.zeros((tok_rows, out_cols), jnp.float32)
    running_out = blank_out
    seg_attend = lax.all_gather(attend_out, "tp", axis=1, tiled=True)
    seg_linear = lax.all_gather(linear_out, "tp", axis=1, tiled=True)
    shard_count = seg_attend.shape[1] // head_count
    first_rank = jnp.int32(0) // head_count
    for shard_step in range(shard_count):
        owner_rank = first_rank + shard_step
        rows_attend = lax.dynamic_index_in_dim(attend_view, owner_rank, 1, keepdims=False).reshape(
            -1, out_cols
        )
        rows_linear = lax.dynamic_index_in_dim(linear_view, owner_rank, 1, keepdims=False).reshape(
            -1, out_cols
        )
        part_attend = seg_attend[
            :, shard_step * head_count : (shard_step + 1) * head_count
        ].reshape(tok_rows, -1)
        part_linear = seg_linear[
            :, shard_step * head_count : (shard_step + 1) * head_count
        ].reshape(tok_rows, -1)
        running_out = running_out + jnp.dot(
            part_attend, rows_attend, preferred_element_type=jnp.float32
        )
        running_out = running_out + jnp.dot(
            part_linear, rows_linear, preferred_element_type=jnp.float32
        )
    return running_out.astype(jnp.bfloat16).reshape(1, tok_rows, out_cols)


MESH = pl.DeviceIdType.MESH


def group_barrier(n, fs_size, tp_size):
    z, f, c = lax.axis_index("sp"), lax.axis_index("fs"), lax.axis_index("tp")
    barrier = pltpu.get_barrier_semaphore()
    total = n * fs_size * tp_size
    me = (z * fs_size + f) * tp_size + c
    for k in range(1, total):
        other = lax.rem(me + k, total)
        oz = other // (fs_size * tp_size)
        of = lax.rem(other // tp_size, fs_size)
        oc = lax.rem(other, tp_size)
        pl.semaphore_signal(
            barrier, inc=1, device_id={"sp": oz, "fs": of, "tp": oc}, device_id_type=MESH
        )
    pl.semaphore_wait(barrier, total - 1)


def remote(src, dst, send, recv, **where):
    return pltpu.make_async_remote_copy(
        src_ref=src,
        dst_ref=dst,
        send_sem=send,
        recv_sem=recv,
        device_id=where,
        device_id_type=MESH,
    )


def gather_kernel(
    n,
    fs_size,
    tp_size,
    hpd,
    tok_ref,
    ret_ref,
    out_ref,
    rout_ref,
    recv_a,
    recv_b,
    recv_r,
    send_a,
    send_up,
    send_down,
    send_sib,
    send_r,
    loc,
):
    z, f, c = lax.axis_index("sp"), lax.axis_index("fs"), lax.axis_index("tp")
    rows = tok_ref.shape[0]
    half = rows // tp_size
    group_barrier(n, fs_size, tp_size)
    lo = f * hpd
    hi = lo + hpd - 1
    near = jnp.minimum(jnp.maximum(z, lo), hi)
    own = near == z

    def piece(zc):
        return pl.ds(pl.multiple_of(zc * rows + c * half, half), half)

    mine = pl.ds(pl.multiple_of(c * half, half), half)
    sends = []
    for k in range(fs_size):
        x = lax.rem(f + k, fs_size)
        copy = remote(
            tok_ref.at[mine], out_ref.at[piece(z)], send_a.at[k], recv_a.at[z], sp=near, fs=x
        )
        if k == 0:
            pl.when(jnp.logical_not(own))(copy.start)
        else:
            copy.start()
        sends.append(copy)
    full = pl.ds(pl.multiple_of(z * rows, rows), rows)
    local = pltpu.make_async_copy(tok_ref, out_ref.at[full], loc.at[0])
    local_r = pltpu.make_async_copy(ret_ref, rout_ref.at[z], loc.at[1])
    pl.when(own)(local.start)
    pl.when(own)(local_r.start)
    rsends = []
    for j in range(hpd):
        for k in range(fs_size):
            x = lax.rem(f + k, fs_size)
            there = lo + j
            copy = remote(
                ret_ref,
                rout_ref.at[z],
                send_r.at[j * fs_size + k],
                recv_r.at[z],
                sp=there,
                fs=x,
            )
            go = jnp.logical_not((there == z) & (x == f))
            pl.when(go)(copy.start)
            rsends.append((go, copy))

    s = z // hpd
    mlo = s * hpd
    mhi = mlo + hpd - 1
    pending = []
    for k in range(n):
        zc = jnp.where(2 * z < n, k, n - 1 - k)
        here = (zc == z) & (s == f)
        away = jnp.logical_not(here)
        block = out_ref.at[piece(zc)]
        arrive = remote(block, block, send_sib.at[k], recv_a.at[zc], tp=1 - c)
        pl.when(away)(arrive.wait_recv)
        pl.when(here)(local.wait)
        up = remote(block, block, send_up.at[k], recv_a.at[zc], sp=jnp.minimum(z + 1, n - 1))
        go_up = (zc <= z) & (z + 1 <= mhi)
        pl.when(go_up)(up.start)
        down = remote(block, block, send_down.at[k], recv_a.at[zc], sp=jnp.maximum(z - 1, 0))
        go_down = (zc >= z) & (z - 1 >= mlo)
        pl.when(go_down)(down.start)
        sib = remote(block, block, send_sib.at[k], recv_b.at[zc], tp=1 - c)
        pl.when(away)(sib.start)
        pending.append((zc, away, sib, go_up, up, go_down, down))
    pl.when(own)(local_r.wait)
    for k, copy in enumerate(sends):
        if k == 0:
            pl.when(jnp.logical_not(own))(copy.wait_send)
        else:
            copy.wait_send()
    for go, copy in rsends:
        pl.when(go)(copy.wait_send)
    for zc, away, sib, go_up, up, go_down, down in pending:
        pl.when(go_up)(up.wait_send)
        pl.when(go_down)(down.wait_send)
        other = out_ref.at[pl.ds(pl.multiple_of(zc * rows + (1 - c) * half, half), half)]
        came = remote(other, other, send_sib.at[0], recv_b.at[zc], tp=1 - c)
        pl.when(away)(came.wait_recv)
        pl.when(away)(sib.wait_send)
        came_r = remote(ret_ref, rout_ref.at[zc], send_r.at[0], recv_r.at[zc], tp=1 - c)
        pl.when(away)(came_r.wait_recv)


def gather_positions(tokens, retain, n, fs_size, tp_size, hpd):
    rows, width = tokens.shape
    dma = pltpu.SemaphoreType.DMA
    return pl.pallas_call(
        functools.partial(gather_kernel, n, fs_size, tp_size, hpd),
        out_shape=(
            jax.ShapeDtypeStruct((n * rows, width), tokens.dtype),
            jax.ShapeDtypeStruct((n,) + retain.shape, retain.dtype),
        ),
        in_specs=[pl.BlockSpec(memory_space=pltpu.VMEM)] * 2,
        out_specs=(pl.BlockSpec(memory_space=pl.ANY), pl.BlockSpec(memory_space=pl.ANY)),
        scratch_shapes=[
            dma((n,)),
            dma((n,)),
            dma((n,)),
            dma((fs_size,)),
            dma((n,)),
            dma((n,)),
            dma((n,)),
            dma((hpd * fs_size,)),
            dma((2,)),
        ],
        compiler_params=pltpu.CompilerParams(collective_id=0, has_side_effects=True),
    )(tokens, retain)


def exchange_kernel(
    n,
    fs_size,
    tp_size,
    hpd,
    mix_ref,
    out_ref,
    stage,
    recv_row,
    recv_x,
    recv_s,
    send_row,
    send_x,
    send_s,
    loc,
):
    z, f, c = lax.axis_index("sp"), lax.axis_index("fs"), lax.axis_index("tp")
    rows = out_ref.shape[1]
    group_barrier(n, fs_size, tp_size)
    s = z // hpd
    keep = s == f
    cross = jnp.logical_not(keep)

    def head(x, core, zs):
        return (x * tp_size + core) * hpd + lax.rem(zs, hpd)

    def chunk(zt):
        return mix_ref.at[pl.ds(pl.multiple_of(zt * rows, rows), rows)]

    my_head = head(f, c, z)
    waits = []
    for k in range(1, n):
        zt = lax.rem(z + k, n)
        kept = remote(chunk(zt), out_ref.at[my_head], send_row.at[k], recv_row.at[z], sp=zt)
        moved = remote(chunk(zt), stage.at[z], send_row.at[k], recv_row.at[z], sp=zt)
        pl.when(keep)(kept.start)
        pl.when(cross)(moved.start)
        waits.append((None, kept))
    local = pltpu.make_async_copy(chunk(z), out_ref.at[my_head], loc)
    pl.when(keep)(local.start)
    sib0 = remote(chunk(z), out_ref.at[my_head], send_s.at[my_head], recv_s.at[my_head], tp=1 - c)
    pl.when(keep)(sib0.start)
    waits.append((keep, sib0))
    x0 = remote(chunk(z), out_ref.at[my_head], send_x.at[0], recv_x.at[my_head], fs=s)
    pl.when(cross)(x0.start)
    waits.append((cross, x0))
    for k in range(1, n):
        zs = lax.rem(z + k, n)
        sq = zs // hpd
        hd = head(f, c, zs)
        final = sq == f
        onward = jnp.logical_not(final)
        landed = remote(stage.at[zs], stage.at[zs], send_x.at[k], recv_row.at[zs], tp=1 - c)
        landed.wait_recv()
        sib = remote(out_ref.at[hd], out_ref.at[hd], send_s.at[hd], recv_s.at[hd], tp=1 - c)
        pl.when(final)(sib.start)
        waits.append((final, sib))
        xs = remote(stage.at[zs], out_ref.at[hd], send_x.at[k], recv_x.at[hd], fs=sq)
        pl.when(onward)(xs.start)
        waits.append((onward, xs))
    for k in range(1, fs_size):
        x = lax.rem(f + k, fs_size)
        for j in range(hpd):
            hd = head(x, c, j)
            block = out_ref.at[hd]
            came = remote(block, block, send_s.at[hd], recv_x.at[hd], tp=1 - c)
            came.wait_recv()
            sib = remote(block, block, send_s.at[hd], recv_s.at[hd], tp=1 - c)
            sib.start()
            waits.append((None, sib))
    for x in range(fs_size):
        for j in range(hpd):
            hd = head(x, 1 - c, j)
            block = out_ref.at[hd]
            remote(block, block, send_s.at[hd], recv_s.at[hd], tp=1 - c).wait_recv()
    pl.when(keep)(local.wait)
    for go, copy in waits:
        if go is None:
            copy.wait_send()
        else:
            pl.when(go)(copy.wait_send)


def exchange_heads(mixed, n, fs_size, tp_size, hpd):
    rows, width = mixed.shape[0] // n, mixed.shape[1]
    heads = fs_size * tp_size * hpd
    dma = pltpu.SemaphoreType.DMA
    return pl.pallas_call(
        functools.partial(exchange_kernel, n, fs_size, tp_size, hpd),
        out_shape=jax.ShapeDtypeStruct((heads, rows, width), mixed.dtype),
        in_specs=[pl.BlockSpec(memory_space=pltpu.VMEM)],
        out_specs=pl.BlockSpec(memory_space=pl.ANY),
        scratch_shapes=[
            pltpu.VMEM((n, rows, width), mixed.dtype),
            dma((n,)),
            dma((heads,)),
            dma((heads,)),
            dma((n,)),
            dma((n,)),
            dma((heads,)),
            dma,
        ],
        compiler_params=pltpu.CompilerParams(collective_id=1, has_side_effects=True),
    )(mixed)


def pair_body(
    tokens,
    norm_gain,
    query_attend,
    key_attend,
    value_attend,
    query_linear,
    key_linear,
    value_linear,
    decay_down,
    decay_up,
    decay_bias,
    log_retain,
    query_gain,
    key_gain,
    diff_lambda,
    mix_gain,
    state_gain,
    init_state,
    output_attend,
    output_linear,
):
    n, fs_size, tp_size = lax.axis_size("sp"), lax.axis_size("fs"), lax.axis_size("tp")
    hpd = query_attend.shape[1]
    z = lax.axis_index("sp")
    slot = lax.rem(z, hpd)
    seq = z // hpd
    head = (lax.axis_index("fs") * tp_size + lax.axis_index("tp")) * hpd + slot
    rows = tokens.shape[1]
    positions, retained = gather_positions(
        tokens[0], jnp.transpose(log_retain[0]), n, fs_size, tp_size, hpd
    )
    retain = lax.dynamic_index_in_dim(retained, head, 1, False).reshape(n * rows)
    normed = rms_scale(positions, norm_gain).astype(jnp.bfloat16)

    def project(weight):
        return jnp.dot(
            normed,
            lax.dynamic_index_in_dim(weight, slot, 1, False),
            preferred_element_type=jnp.float32,
        ).astype(jnp.bfloat16)

    length = n * rows
    q_unit = rms_scale(project(query_attend).reshape(length, 2, HD_A), query_gain)
    k_unit = rms_scale(
        project(key_attend).reshape(length, 2, HD_A), lax.dynamic_index_in_dim(key_gain, head, 0, False)
    )
    v_attend = project(value_attend)
    scores = jnp.einsum(
        "qmd,kmd->mqk",
        q_unit.astype(jnp.bfloat16),
        k_unit.astype(jnp.bfloat16),
        preferred_element_type=jnp.float32,
    ) * HD_A ** (-0.5)
    blocks = jnp.arange(length, dtype=jnp.int32) // BLK
    scores = jnp.where(blocks[:, None] >= blocks[None, :], scores, -jnp.inf)
    raised = jnp.exp(scores - jnp.max(scores, axis=-1, keepdims=True))
    totals = jnp.sum(raised, axis=-1, keepdims=True)
    sums = jnp.einsum(
        "mqk,kv->mqv", raised.astype(jnp.bfloat16), v_attend, preferred_element_type=jnp.float32
    )
    lam = lax.dynamic_index_in_dim(diff_lambda, head, 0, False)
    diff_raw = sums[0] / totals[0] - lam * sums[1] / totals[1]
    attend_out = rms_scale(diff_raw, mix_gain).astype(jnp.bfloat16)
    low_rank = jnp.dot(normed, decay_down, preferred_element_type=jnp.float32).astype(jnp.bfloat16)
    pre_act = jnp.dot(
        low_rank,
        lax.dynamic_index_in_dim(decay_up, head, 1, False),
        preferred_element_type=jnp.float32,
    ) + lax.dynamic_index_in_dim(decay_bias, head, 0, False)
    log_decay = jax.nn.log_sigmoid(pre_act) / decay_tau + retain[:, None]
    start = lax.dynamic_index_in_dim(
        lax.dynamic_index_in_dim(init_state, seq, 0, False), slot, 0, False
    )
    _, _, inside, reaching = linear_blocks(
        project(query_linear).astype(jnp.float32)[:, None] * HDK ** (-0.5),
        project(key_linear).astype(jnp.float32)[:, None],
        project(value_linear).astype(jnp.float32)[:, None],
        log_decay[:, None],
    )
    linear_raw = inside[:, 0] + jnp.dot(reaching[:, 0], start, precision=lax.Precision.HIGHEST)
    linear_out = rms_scale(linear_raw, state_gain).astype(jnp.bfloat16)
    mixed = jnp.concatenate([attend_out, linear_out], axis=1)
    arrived = exchange_heads(mixed, n, fs_size, tp_size, hpd)
    heads = arrived.shape[0]
    out = jnp.einsum(
        "htw,hwo->to",
        arrived[:, :, :DV_A],
        output_attend.reshape(heads, DV_A, -1),
        preferred_element_type=jnp.float32,
    ) + jnp.einsum(
        "htw,hwo->to",
        arrived[:, :, DV_A:],
        output_linear.reshape(heads, HDV, -1),
        preferred_element_type=jnp.float32,
    )
    return out.astype(jnp.bfloat16)[None]


def solution(mesh):
    in_specs = (
        P(("grp", "fs"), "sp", None),
        P(),
        P(None, ("fs", "tp"), None),
        P(None, ("fs", "tp"), None),
        P(None, ("fs", "tp"), None),
        P(None, ("fs", "tp"), None),
        P(None, ("fs", "tp"), None),
        P(None, ("fs", "tp"), None),
        P(),
        P(),
        P(),
        P(("grp", "fs"), "sp", None),
        P(),
        P(),
        P(),
        P(),
        P(),
        P("grp", ("fs", "tp"), None, None),
        P(None, "tp"),
        P(None, "tp"),
    )
    out_specs = P(("grp", "fs"), "sp", "tp")
    fs_size, tp_size, sp_size = mesh.shape["fs"], mesh.shape["tp"], mesh.shape["sp"]
    pairs = MIXER_HEADS // tp_size
    chosen = pair_body if pairs == sp_size and tp_size == 2 else body
    return jax.shard_map(chosen, mesh=mesh, in_specs=in_specs, out_specs=out_specs, check_vma=False)
```

```python
import functools

import jax
import jax.numpy as jnp
from jax import lax
from jax.experimental import pallas as pl
from jax.experimental.pallas import tpu as pltpu
from jax.sharding import PartitionSpec as P

MIXER_HEADS = 8
HD_A = 64
DV_A = 128
HDK = 128
HDV = 256
BLK = 64


norm_eps = 1e-06
decay_tau = 16.0


def entering(part, axis, combine, identity):
    place = lax.axis_index(axis)
    gathered = jax.tree.map(lambda a: lax.all_gather(a, axis), part)
    state = jax.tree.map(lambda a, e: jnp.zeros_like(a) + jnp.asarray(e, a.dtype), part, identity)

    def one(hop, state):
        return combine(
            state, jax.tree.map(lambda a: lax.dynamic_index_in_dim(a, hop, 0, False), gathered)
        )

    return lax.fori_loop(0, place, one, state)


def rms_scale(values, gain):
    widened = values.astype(jnp.float32)
    return (
        widened * lax.rsqrt(jnp.mean(widened * widened, axis=-1, keepdims=True) + norm_eps) * gain
    )


def head_order(fs_size, tp_size, tp_rank):
    per_device = MIXER_HEADS // (fs_size * tp_size)
    owners = jnp.arange(fs_size, dtype=jnp.int32)[:, None] * tp_size + tp_rank
    return (owners * per_device + jnp.arange(per_device, dtype=jnp.int32)[None, :]).reshape(-1)


def linear_blocks(queries, keys_in, values_in, log_decay):
    tok_rows, head_count, key_dim = queries.shape
    value_dim = values_in.shape[-1]
    block_count = tok_rows // BLK
    highest_precision = lax.Precision.HIGHEST

    def split_blocks(source):
        return source.reshape(block_count, BLK, head_count, source.shape[-1])

    causal = (
        jnp.arange(BLK, dtype=jnp.int32)[:, None] >= jnp.arange(BLK, dtype=jnp.int32)[None, :]
    )[None]

    def advance(carry, inputs_now):
        recurrent_state, offset = carry
        question_patch_lines, block_k, value_tile_width, block_log = inputs_now
        running_state = jnp.cumsum(block_log, axis=0)
        pivot = running_state[BLK // 2]
        q_scaled = question_patch_lines * jnp.exp(running_state - pivot[None])
        k_scaled = block_k * jnp.exp(pivot[None] - running_state)
        scores = jnp.einsum("thk,shk->hts", q_scaled, k_scaled, precision=highest_precision)
        scores = jnp.where(causal, scores, 0.0)
        inside_block = jnp.einsum(
            "hts,shv->thv", scores, value_tile_width, precision=highest_precision
        )
        inside_block = inside_block + jnp.einsum(
            "jwo,wos->jws",
            question_patch_lines * jnp.exp(running_state),
            recurrent_state,
            precision=highest_precision,
        )
        final_state = running_state[-1]
        faded_memory_matrix = block_k * jnp.exp(final_state[None] - running_state)
        recurrent_state = recurrent_state * jnp.exp(final_state)[:, :, None] + jnp.einsum(
            "zcb,zcw->cbw", faded_memory_matrix, value_tile_width, precision=highest_precision
        )
        reaching_keys = question_patch_lines * jnp.exp(offset[None] + running_state)
        return ((recurrent_state, offset + final_state), (inside_block, reaching_keys))

    start_carry = (
        jnp.zeros((head_count, key_dim, value_dim), jnp.float32),
        jnp.zeros((head_count, key_dim), jnp.float32),
    )
    (recurrent_state, total_decay), (inside_block, reaching_keys) = lax.scan(
        advance,
        start_carry,
        (
            split_blocks(queries),
            split_blocks(keys_in),
            split_blocks(values_in),
            split_blocks(log_decay),
        ),
    )
    return (
        recurrent_state,
        total_decay,
        inside_block.reshape(tok_rows, head_count, value_dim),
        reaching_keys.reshape(tok_rows, head_count, key_dim),
    )


def body(
    tokens,
    norm_gain,
    query_attend,
    key_attend,
    value_attend,
    query_linear,
    key_linear,
    value_linear,
    decay_down,
    decay_up,
    decay_bias,
    log_retain,
    query_gain,
    key_gain,
    diff_lambda,
    mix_gain,
    state_gain,
    init_state,
    output_attend,
    output_linear,
):
    fs_size = lax.axis_size("fs")
    tp_size = lax.axis_size("tp")
    tp_rank = lax.axis_index("tp")
    tok_rows = tokens.shape[1]
    normed = rms_scale(tokens, norm_gain).astype(jnp.bfloat16)
    normed_rows = normed[0]
    local_weights = (query_attend, key_attend, value_attend, query_linear, key_linear, value_linear)
    widths = [weight.shape[1] * weight.shape[2] for weight in local_weights]
    packed = jnp.concatenate(
        [weight.reshape(weight.shape[0], -1) for weight in local_weights], axis=1
    )
    computed = jnp.einsum(
        "std,dp->stp",
        lax.all_gather(normed, "fs", axis=0, tiled=True),
        packed,
        preferred_element_type=jnp.float32,
    ).astype(jnp.bfloat16)
    arrived = lax.all_to_all(computed, "fs", split_axis=0, concat_axis=2, tiled=True).reshape(
        tok_rows, fs_size, -1
    )
    sections = []
    column_at = 0
    for weight, width_now in zip(local_weights, widths):
        section = arrived[:, :, column_at : column_at + width_now]
        sections.append(section.reshape(tok_rows, fs_size * weight.shape[1], weight.shape[2]))
        column_at = column_at + width_now
    projected = tuple(sections)
    q_pair, k_pair, v_attend, q_lin, k_lin, v_lin = projected
    head_ids = head_order(fs_size, tp_size, tp_rank)
    head_count = head_ids.shape[0]
    q_unit = rms_scale(q_pair.reshape(tok_rows, head_count, 2, HD_A), query_gain).astype(
        jnp.bfloat16
    )
    k_unit = rms_scale(
        k_pair.reshape(tok_rows, head_count, 2, HD_A), jnp.take(key_gain, head_ids, axis=0)
    ).astype(jnp.bfloat16)
    sp_start = lax.axis_index("sp") * tok_rows
    query_block = (sp_start + jnp.arange(tok_rows, dtype=jnp.int32)) // BLK
    score_scale = HD_A ** (-0.5)
    blank_attend = (
        jnp.full((head_count, 2, tok_rows), -jnp.inf, jnp.float32),
        jnp.zeros((head_count, 2, tok_rows), jnp.float32),
        jnp.zeros((head_count, 2, tok_rows, DV_A), jnp.float32),
    )
    carry = blank_attend
    seg_keys = lax.all_gather(k_unit, "sp", axis=0, tiled=True)
    seg_values = lax.all_gather(v_attend, "sp", axis=0, tiled=True)
    span = seg_keys.shape[0]
    stride_token_lines = 2 * tok_rows
    step_count = span // stride_token_lines
    key_steps = seg_keys.reshape(step_count, stride_token_lines, head_count, 2, HD_A)
    value_steps = seg_values.reshape(step_count, stride_token_lines, head_count, DV_A)

    def one_step(running_state, inputs_now):
        step_index, key_step, value_step = inputs_now
        key_start = step_index * stride_token_lines

        def compute(current):
            run_max, run_total, run_acc = current
            scores = (
                jnp.einsum("qhmd,khmd->hmqk", q_unit, key_step, preferred_element_type=jnp.float32)
                * score_scale
            )
            key_block = (key_start + jnp.arange(stride_token_lines, dtype=jnp.int32)) // BLK
            allowed = query_block[:, None] >= key_block[None, :]
            scores = jnp.where(allowed, scores, -jnp.inf)
            new_max = jnp.maximum(run_max, jnp.max(scores, axis=-1))
            factor = jnp.exp(run_max - new_max)
            raised = jnp.exp(scores - new_max[..., None])
            run_total = run_total * factor + jnp.sum(raised, axis=-1)
            run_acc = run_acc * factor[..., None] + jnp.einsum(
                "hmqk,khv->hmqv",
                raised.astype(jnp.bfloat16),
                value_step,
                preferred_element_type=jnp.float32,
            )
            return (new_max, run_total, run_acc)

        def unchanged(current):
            return current

        return (lax.cond(key_start <= sp_start, compute, unchanged, running_state), None)

    carry, _ = lax.scan(
        one_step, carry, (jnp.arange(step_count, dtype=jnp.int32), key_steps, value_steps)
    )
    run_max, run_total, run_acc = carry
    lambda_heads = jnp.take(diff_lambda, head_ids, axis=0)
    diff_raw = (
        run_acc[:, 0] / run_total[:, 0, :, None]
        - lambda_heads[:, None, None] * run_acc[:, 1] / run_total[:, 1, :, None]
    )
    attend_out = rms_scale(jnp.transpose(diff_raw, (1, 0, 2)), mix_gain).astype(jnp.bfloat16)
    low_rank = jnp.dot(normed_rows, decay_down, preferred_element_type=jnp.float32).astype(
        jnp.bfloat16
    )
    up_columns = jnp.take(decay_up, head_ids, axis=1)
    pre_act = jnp.einsum(
        "tr,rhk->thk", low_rank, up_columns, preferred_element_type=jnp.float32
    ) + jnp.take(decay_bias, head_ids, axis=0)
    retain_heads = jnp.take(log_retain[0], head_ids, axis=1)
    log_decay = jax.nn.log_sigmoid(pre_act) / decay_tau + retain_heads[:, :, None]
    local_state, local_decay, inside_block, reaching_keys = linear_blocks(
        q_lin.astype(jnp.float32) * HDK ** (-0.5),
        k_lin.astype(jnp.float32),
        v_lin.astype(jnp.float32),
        log_decay,
    )

    def chain(earlier, later):
        return (earlier[0] + later[0], earlier[1] * jnp.exp(later[0])[:, :, None] + later[1])

    zero_chain = (jnp.zeros_like(local_decay), jnp.zeros_like(local_state))
    prior_decay, prior_state = entering((local_decay, local_state), "sp", chain, zero_chain)
    start_state = lax.all_to_all(init_state, "fs", split_axis=0, concat_axis=1, tiled=True)[0]
    incoming_state = start_state * jnp.exp(prior_decay)[:, :, None] + prior_state
    linear_raw = inside_block + jnp.einsum(
        "jwo,wos->jws", reaching_keys, incoming_state, precision=lax.Precision.HIGHEST
    )
    linear_out = rms_scale(linear_raw, state_gain).astype(jnp.bfloat16)
    out_cols = output_attend.shape[1]
    per_device = MIXER_HEADS // (fs_size * tp_size)
    attend_view = output_attend.reshape(fs_size, tp_size, per_device * DV_A, out_cols)
    linear_view = output_linear.reshape(fs_size, tp_size, per_device * HDV, out_cols)
    blank_out = jnp.zeros((tok_rows, out_cols), jnp.float32)
    running_out = blank_out
    seg_attend = lax.all_gather(attend_out, "tp", axis=1, tiled=True)
    seg_linear = lax.all_gather(linear_out, "tp", axis=1, tiled=True)
    shard_count = seg_attend.shape[1] // head_count
    first_rank = jnp.int32(0) // head_count
    for shard_step in range(shard_count):
        owner_rank = first_rank + shard_step
        rows_attend = lax.dynamic_index_in_dim(attend_view, owner_rank, 1, keepdims=False).reshape(
            -1, out_cols
        )
        rows_linear = lax.dynamic_index_in_dim(linear_view, owner_rank, 1, keepdims=False).reshape(
            -1, out_cols
        )
        part_attend = seg_attend[
            :, shard_step * head_count : (shard_step + 1) * head_count
        ].reshape(tok_rows, -1)
        part_linear = seg_linear[
            :, shard_step * head_count : (shard_step + 1) * head_count
        ].reshape(tok_rows, -1)
        running_out = running_out + jnp.dot(
            part_attend, rows_attend, preferred_element_type=jnp.float32
        )
        running_out = running_out + jnp.dot(
            part_linear, rows_linear, preferred_element_type=jnp.float32
        )
    return running_out.astype(jnp.bfloat16).reshape(1, tok_rows, out_cols)


MESH = pl.DeviceIdType.MESH


def group_barrier(n, fs_size, tp_size):
    z, f, c = lax.axis_index("sp"), lax.axis_index("fs"), lax.axis_index("tp")
    barrier = pltpu.get_barrier_semaphore()
    total = n * fs_size * tp_size
    me = (z * fs_size + f) * tp_size + c
    for k in range(1, total):
        other = lax.rem(me + k, total)
        oz = other // (fs_size * tp_size)
        of = lax.rem(other // tp_size, fs_size)
        oc = lax.rem(other, tp_size)
        pl.semaphore_signal(
            barrier, inc=1, device_id={"sp": oz, "fs": of, "tp": oc}, device_id_type=MESH
        )
    pl.semaphore_wait(barrier, total - 1)


def remote(src, dst, send, recv, **where):
    return pltpu.make_async_remote_copy(
        src_ref=src,
        dst_ref=dst,
        send_sem=send,
        recv_sem=recv,
        device_id=where,
        device_id_type=MESH,
    )


def gather_kernel(
    n,
    fs_size,
    tp_size,
    hpd,
    tok_ref,
    ret_ref,
    gain_ref,
    down_ref,
    wq_ref,
    wk_ref,
    wv_ref,
    lq_ref,
    lk_ref,
    lv_ref,
    proj_ref,
    low_ref,
    rout_ref,
    seq_ref,
    raw_ref,
    raw_v_ref,
    w_ref,
    recv_a,
    recv_b,
    recv_r,
    send_a,
    send_up,
    send_down,
    send_sib,
    send_r,
    loc,
    wsem,
):
    z, f, c = lax.axis_index("sp"), lax.axis_index("fs"), lax.axis_index("tp")
    rows, width = tok_ref.shape
    half = rows // tp_size
    loads = [
        pltpu.make_async_copy(ref, raw_ref.at[i], wsem.at[i])
        for i, ref in enumerate((wq_ref, wk_ref, wv_ref, lq_ref, lk_ref))
    ]
    loads.append(pltpu.make_async_copy(lv_ref, raw_v_ref, wsem.at[5]))
    for load in loads:
        load.start()
    group_barrier(n, fs_size, tp_size)
    lo = f * hpd
    hi = lo + hpd - 1
    near = jnp.minimum(jnp.maximum(z, lo), hi)
    own = near == z

    def piece(zc):
        return pl.ds(pl.multiple_of(zc * rows + c * half, half), half)

    mine = pl.ds(pl.multiple_of(c * half, half), half)
    sends = []
    for k in range(fs_size):
        x = lax.rem(f + k, fs_size)
        copy = remote(
            tok_ref.at[mine], seq_ref.at[piece(z)], send_a.at[k], recv_a.at[z], sp=near, fs=x
        )
        if k == 0:
            pl.when(jnp.logical_not(own))(copy.start)
        else:
            copy.start()
        sends.append(copy)
    full = pl.ds(pl.multiple_of(z * rows, rows), rows)
    local = pltpu.make_async_copy(tok_ref, seq_ref.at[full], loc.at[0])
    local_r = pltpu.make_async_copy(ret_ref, rout_ref.at[z], loc.at[1])
    pl.when(own)(local.start)
    pl.when(own)(local_r.start)
    rsends = []
    for j in range(hpd):
        for k in range(fs_size):
            x = lax.rem(f + k, fs_size)
            there = lo + j
            copy = remote(
                ret_ref,
                rout_ref.at[z],
                send_r.at[j * fs_size + k],
                recv_r.at[z],
                sp=there,
                fs=x,
            )
            go = jnp.logical_not((there == z) & (x == f))
            pl.when(go)(copy.start)
            rsends.append((go, copy))

    slot = lax.rem(z, hpd)
    step = 128

    def pick(source, target_cols, parts, part):
        span = step * parts * hpd
        sel = (
            lax.broadcasted_iota(jnp.int32, (step, span), 1)
            == (lax.broadcasted_iota(jnp.int32, (step, span), 0) * parts + part) * hpd + slot
        ).astype(jnp.bfloat16)

        def one(i, carry):
            block = source[pl.ds(pl.multiple_of(i * span, span), span), :]
            w_ref[pl.ds(pl.multiple_of(i * step, step), step), target_cols] = jnp.dot(
                sel, block, preferred_element_type=jnp.float32
            ).astype(jnp.bfloat16)
            return carry

        lax.fori_loop(0, width // step, one, 0)

    for i in range(5):
        loads[i].wait()
        pick(raw_ref.at[i], slice(i * 128, (i + 1) * 128), 1, 0)
    loads[5].wait()
    for part in range(2):
        pick(raw_v_ref, slice((5 + part) * 128, (6 + part) * 128), 2, part)

    s = z // hpd
    mlo = s * hpd
    mhi = mlo + hpd - 1
    pending = []

    def order(k):
        return jnp.where(2 * z < n, k, n - 1 - k)

    def finish(k):
        zc = order(k)
        away = jnp.logical_not((zc == z) & (s == f))
        other = seq_ref.at[pl.ds(pl.multiple_of(zc * rows + (1 - c) * half, half), half)]
        came = remote(other, other, send_sib.at[0], recv_b.at[zc], tp=1 - c)
        pl.when(away)(came.wait_recv)
        at = pl.ds(pl.multiple_of(zc * rows, rows), rows)
        x = seq_ref[at, :].astype(jnp.float32)
        scale = lax.rsqrt(jnp.mean(x * x, axis=-1, keepdims=True) + norm_eps)
        normed = (x * scale * gain_ref[...]).astype(jnp.bfloat16)
        proj_ref[at, :] = jnp.dot(
            normed, w_ref[...], preferred_element_type=jnp.float32
        ).astype(jnp.bfloat16)
        low_ref[at, :] = lax.dot_general(
            normed, down_ref[...], (((1,), (1,)), ((), ())), preferred_element_type=jnp.float32
        ).astype(jnp.bfloat16)

    for k in range(n):
        zc = order(k)
        here = (zc == z) & (s == f)
        away = jnp.logical_not(here)
        block = seq_ref.at[piece(zc)]
        arrive = remote(block, block, send_sib.at[k], recv_a.at[zc], tp=1 - c)
        pl.when(away)(arrive.wait_recv)
        pl.when(here)(local.wait)
        up = remote(block, block, send_up.at[k], recv_a.at[zc], sp=jnp.minimum(z + 1, n - 1))
        go_up = (zc <= z) & (z + 1 <= mhi)
        pl.when(go_up)(up.start)
        down = remote(block, block, send_down.at[k], recv_a.at[zc], sp=jnp.maximum(z - 1, 0))
        go_down = (zc >= z) & (z - 1 >= mlo)
        pl.when(go_down)(down.start)
        sib = remote(block, block, send_sib.at[k], recv_b.at[zc], tp=1 - c)
        pl.when(away)(sib.start)
        pending.append((zc, away, sib, go_up, up, go_down, down))
        if k > 0:
            finish(k - 1)
    finish(n - 1)
    pl.when(own)(local_r.wait)
    for k, copy in enumerate(sends):
        if k == 0:
            pl.when(jnp.logical_not(own))(copy.wait_send)
        else:
            copy.wait_send()
    for go, copy in rsends:
        pl.when(go)(copy.wait_send)
    for zc, away, sib, go_up, up, go_down, down in pending:
        pl.when(go_up)(up.wait_send)
        pl.when(go_down)(down.wait_send)
        pl.when(away)(sib.wait_send)
        came_r = remote(ret_ref, rout_ref.at[zc], send_r.at[0], recv_r.at[zc], tp=1 - c)
        pl.when(away)(came_r.wait_recv)


def interleaved(weight):
    width, hpd, columns = weight.shape
    parts = columns // 128
    return jnp.swapaxes(weight.reshape(width, hpd, parts, 128), 1, 2).reshape(-1, 128)


def gather_positions(tokens, retain, gain, down, weights, n, fs_size, tp_size, hpd):
    rows, width = tokens.shape
    dma = pltpu.SemaphoreType.DMA
    flat = [interleaved(weight) for weight in weights]
    columns = sum(weight.shape[2] for weight in weights)
    vmem = pl.BlockSpec(memory_space=pltpu.VMEM)
    anywhere = pl.BlockSpec(memory_space=pl.ANY)
    return pl.pallas_call(
        functools.partial(gather_kernel, n, fs_size, tp_size, hpd),
        out_shape=(
            jax.ShapeDtypeStruct((n * rows, columns), jnp.bfloat16),
            jax.ShapeDtypeStruct((n * rows, down.shape[0]), jnp.bfloat16),
            jax.ShapeDtypeStruct((n,) + retain.shape, retain.dtype),
        ),
        in_specs=[vmem] * 4 + [anywhere] * 6,
        out_specs=(vmem, vmem, anywhere),
        scratch_shapes=[
            pltpu.VMEM((n * rows, width), jnp.bfloat16),
            pltpu.VMEM((5,) + flat[0].shape, jnp.bfloat16),
            pltpu.VMEM(flat[5].shape, jnp.bfloat16),
            pltpu.VMEM((width, columns), jnp.bfloat16),
            dma((n,)),
            dma((n,)),
            dma((n,)),
            dma((fs_size,)),
            dma((n,)),
            dma((n,)),
            dma((n,)),
            dma((hpd * fs_size,)),
            dma((2,)),
            dma((6,)),
        ],
        compiler_params=pltpu.CompilerParams(collective_id=0, has_side_effects=True),
    )(tokens, retain, gain, down, *flat)


def mix_kernel(
    hpd,
    tp_size,
    lam_ref,
    proj_ref,
    low_ref,
    ret_ref,
    up_ref,
    bias_ref,
    qg_ref,
    kg_ref,
    mg_ref,
    sg_ref,
    init_ref,
    out_ref,
):
    z, f, c = lax.axis_index("sp"), lax.axis_index("fs"), lax.axis_index("tp")
    slot = lax.rem(z, hpd)
    seq = z // hpd
    head = (f * tp_size + c) * hpd + slot
    f32, bf16 = jnp.float32, jnp.bfloat16
    length = proj_ref.shape[0]
    lane = lax.broadcasted_iota(jnp.int32, (1, 2 * HD_A), 1)
    first = lane < HD_A

    def unit(cols, gain):
        x = proj_ref[:, cols].astype(f32)
        sq = x * x
        m0 = jnp.sum(jnp.where(first, sq, 0.0), axis=-1, keepdims=True) / HD_A
        m1 = jnp.sum(jnp.where(first, 0.0, sq), axis=-1, keepdims=True) / HD_A
        r = jnp.where(first, lax.rsqrt(m0 + norm_eps), lax.rsqrt(m1 + norm_eps))
        return (x * r * gain).astype(bf16)

    q_gain = jnp.concatenate([qg_ref[...], qg_ref[...]], axis=1)
    k_pair = kg_ref[pl.ds(head, 1)]
    k_gain = jnp.concatenate([k_pair[:, 0], k_pair[:, 1]], axis=1)
    q_unit = unit(slice(0, 128), q_gain)
    k_unit = unit(slice(128, 256), k_gain)
    zero = jnp.zeros_like(q_unit)
    q_maps = (jnp.where(first, q_unit, zero), jnp.where(first, zero, q_unit))
    tile = 2 * BLK
    key_b = lax.broadcasted_iota(jnp.int32, (tile, tile), 1) // BLK
    query_b = lax.broadcasted_iota(jnp.int32, (tile, tile), 0) // BLK
    allowed = query_b >= key_b
    lam = lam_ref[head]
    for i in range(length // tile):
        at = slice(i * tile, (i + 1) * tile)
        parts = []
        for m in range(2):
            q = q_maps[m][at]
            diag = (
                lax.dot_general(
                    q, k_unit[at], (((1,), (1,)), ((), ())), preferred_element_type=f32
                )
                * HD_A ** (-0.5)
            )
            diag = jnp.where(allowed, diag, -jnp.inf)
            top = jnp.max(diag, axis=-1, keepdims=True)
            if i > 0:
                past = (
                    lax.dot_general(
                        q,
                        k_unit[: i * tile],
                        (((1,), (1,)), ((), ())),
                        preferred_element_type=f32,
                    )
                    * HD_A ** (-0.5)
                )
                top = jnp.maximum(top, jnp.max(past, axis=-1, keepdims=True))
            raised = jnp.exp(diag - top)
            total = jnp.sum(raised, axis=-1, keepdims=True)
            acc = jnp.dot(raised.astype(bf16), proj_ref[at, 256:384], preferred_element_type=f32)
            if i > 0:
                raised = jnp.exp(past - top)
                total = total + jnp.sum(raised, axis=-1, keepdims=True)
                acc = acc + jnp.dot(
                    raised.astype(bf16), proj_ref[: i * tile, 256:384], preferred_element_type=f32
                )
            parts.append(acc / total)
        diff = parts[0] - lam * parts[1]
        scale = lax.rsqrt(jnp.mean(diff * diff, axis=-1, keepdims=True) + norm_eps)
        out_ref[at, :DV_A] = (diff * scale * mg_ref[...]).astype(bf16)

    up = up_ref[:, pl.ds(pl.multiple_of(head * HDK, HDK), HDK)]
    bias = bias_ref[pl.ds(head, 1), :]
    r64 = lax.broadcasted_iota(jnp.int32, (BLK, BLK), 0)
    c64 = lax.broadcasted_iota(jnp.int32, (BLK, BLK), 1)
    causal = r64 >= c64
    lower = causal.astype(f32)
    eye_k = lax.broadcasted_iota(jnp.int32, (HDK, HDK), 0) == lax.broadcasted_iota(
        jnp.int32, (HDK, HDK), 1
    )
    pre = jnp.dot(low_ref[...], up, preferred_element_type=f32) + bias
    log_sig = jnp.minimum(pre, 0.0) - jnp.log1p(jnp.exp(-jnp.abs(pre)))
    log_sig = log_sig / decay_tau
    state = init_ref[pl.ds(seq, 1), pl.ds(slot, 1)].reshape(HDK, HDV)
    rows = ret_ref.shape[2]
    per = rows // BLK
    for b in range(length // BLK):
        at = slice(b * BLK, (b + 1) * BLK)
        ret = ret_ref[b // per, pl.ds(head, 1), :][:, (b % per) * BLK : (b % per + 1) * BLK]
        column = jnp.sum(jnp.where(r64 == c64, ret, 0.0), axis=-1, keepdims=True)
        logs = log_sig[at] + column
        run = jnp.dot(
            lower, logs, preferred_element_type=f32, precision=lax.Precision.HIGHEST
        )
        pivot = run[BLK // 2 : BLK // 2 + 1]
        last = run[BLK - 1 : BLK]
        q = proj_ref[at, 384:512].astype(f32) * HDK ** (-0.5)
        k = proj_ref[at, 512:640].astype(f32)
        v = proj_ref[at, 640:896]
        qs = (q * jnp.exp(run - pivot)).astype(bf16)
        ks = (k * jnp.exp(pivot - run)).astype(bf16)
        inner = lax.dot_general(qs, ks, (((1,), (1,)), ((), ())), preferred_element_type=f32)
        inner = jnp.where(causal, inner, 0.0).astype(bf16)
        raw = jnp.dot(inner, v, preferred_element_type=f32) + jnp.dot(
            (q * jnp.exp(run)).astype(bf16), state.astype(bf16), preferred_element_type=f32
        )
        faded = (k * jnp.exp(last - run)).astype(bf16)
        keep = jnp.sum(jnp.where(eye_k, jnp.exp(last), 0.0), axis=-1, keepdims=True)
        state = state * keep + lax.dot_general(
            faded, v, (((0,), (0,)), ((), ())), preferred_element_type=f32
        )
        scale = lax.rsqrt(jnp.mean(raw * raw, axis=-1, keepdims=True) + norm_eps)
        out_ref[at, DV_A:] = (raw * scale * sg_ref[...]).astype(bf16)


def exchange_kernel(
    n,
    fs_size,
    tp_size,
    hpd,
    mix_ref,
    out_ref,
    stage,
    recv_row,
    recv_x,
    recv_s,
    send_row,
    send_x,
    send_s,
    loc,
):
    z, f, c = lax.axis_index("sp"), lax.axis_index("fs"), lax.axis_index("tp")
    rows = out_ref.shape[1]
    group_barrier(n, fs_size, tp_size)
    s = z // hpd
    keep = s == f
    cross = jnp.logical_not(keep)

    def head(x, core, zs):
        return (x * tp_size + core) * hpd + lax.rem(zs, hpd)

    def chunk(zt):
        return mix_ref.at[pl.ds(pl.multiple_of(zt * rows, rows), rows)]

    my_head = head(f, c, z)
    waits = []
    for k in range(1, n):
        zt = lax.rem(z + k, n)
        kept = remote(chunk(zt), out_ref.at[my_head], send_row.at[k], recv_row.at[z], sp=zt)
        moved = remote(chunk(zt), stage.at[z], send_row.at[k], recv_row.at[z], sp=zt)
        pl.when(keep)(kept.start)
        pl.when(cross)(moved.start)
        waits.append((None, kept))
    local = pltpu.make_async_copy(chunk(z), out_ref.at[my_head], loc)
    pl.when(keep)(local.start)
    sib0 = remote(chunk(z), out_ref.at[my_head], send_s.at[my_head], recv_s.at[my_head], tp=1 - c)
    pl.when(keep)(sib0.start)
    waits.append((keep, sib0))
    x0 = remote(chunk(z), out_ref.at[my_head], send_x.at[0], recv_x.at[my_head], fs=s)
    pl.when(cross)(x0.start)
    waits.append((cross, x0))
    for k in range(1, n):
        zs = lax.rem(z + k, n)
        sq = zs // hpd
        hd = head(f, c, zs)
        final = sq == f
        onward = jnp.logical_not(final)
        landed = remote(stage.at[zs], stage.at[zs], send_x.at[k], recv_row.at[zs], tp=1 - c)
        landed.wait_recv()
        sib = remote(out_ref.at[hd], out_ref.at[hd], send_s.at[hd], recv_s.at[hd], tp=1 - c)
        pl.when(final)(sib.start)
        waits.append((final, sib))
        xs = remote(stage.at[zs], out_ref.at[hd], send_x.at[k], recv_x.at[hd], fs=sq)
        pl.when(onward)(xs.start)
        waits.append((onward, xs))
    for k in range(1, fs_size):
        x = lax.rem(f + k, fs_size)
        for j in range(hpd):
            hd = head(x, c, j)
            block = out_ref.at[hd]
            came = remote(block, block, send_s.at[hd], recv_x.at[hd], tp=1 - c)
            came.wait_recv()
            sib = remote(block, block, send_s.at[hd], recv_s.at[hd], tp=1 - c)
            sib.start()
            waits.append((None, sib))
    for x in range(fs_size):
        for j in range(hpd):
            hd = head(x, 1 - c, j)
            block = out_ref.at[hd]
            remote(block, block, send_s.at[hd], recv_s.at[hd], tp=1 - c).wait_recv()
    pl.when(keep)(local.wait)
    for go, copy in waits:
        if go is None:
            copy.wait_send()
        else:
            pl.when(go)(copy.wait_send)


def exchange_heads(mixed, n, fs_size, tp_size, hpd):
    rows, width = mixed.shape[0] // n, mixed.shape[1]
    heads = fs_size * tp_size * hpd
    dma = pltpu.SemaphoreType.DMA
    return pl.pallas_call(
        functools.partial(exchange_kernel, n, fs_size, tp_size, hpd),
        out_shape=jax.ShapeDtypeStruct((heads, rows, width), mixed.dtype),
        in_specs=[pl.BlockSpec(memory_space=pltpu.VMEM)],
        out_specs=pl.BlockSpec(memory_space=pl.ANY),
        scratch_shapes=[
            pltpu.VMEM((n, rows, width), mixed.dtype),
            dma((n,)),
            dma((heads,)),
            dma((heads,)),
            dma((n,)),
            dma((n,)),
            dma((heads,)),
            dma,
        ],
        compiler_params=pltpu.CompilerParams(collective_id=1, has_side_effects=True),
    )(mixed)


def pair_body(
    tokens,
    norm_gain,
    query_attend,
    key_attend,
    value_attend,
    query_linear,
    key_linear,
    value_linear,
    decay_down,
    decay_up,
    decay_bias,
    log_retain,
    query_gain,
    key_gain,
    diff_lambda,
    mix_gain,
    state_gain,
    init_state,
    output_attend,
    output_linear,
):
    n, fs_size, tp_size = lax.axis_size("sp"), lax.axis_size("fs"), lax.axis_size("tp")
    hpd = query_attend.shape[1]
    weights = (query_attend, key_attend, value_attend, query_linear, key_linear, value_linear)
    projected, low_rank, retained = gather_positions(
        tokens[0],
        jnp.transpose(log_retain[0]),
        norm_gain[None],
        jnp.transpose(decay_down),
        weights,
        n,
        fs_size,
        tp_size,
        hpd,
    )
    vmem = pl.BlockSpec(memory_space=pltpu.VMEM)
    mixed = pl.pallas_call(
        functools.partial(mix_kernel, hpd, tp_size),
        out_shape=jax.ShapeDtypeStruct((projected.shape[0], DV_A + HDV), jnp.bfloat16),
        in_specs=[pl.BlockSpec(memory_space=pltpu.SMEM)] + [vmem] * 10,
        out_specs=vmem,
    )(
        diff_lambda,
        projected,
        low_rank,
        retained,
        decay_up.reshape(decay_up.shape[0], -1),
        decay_bias,
        query_gain[None],
        key_gain,
        mix_gain[None],
        state_gain[None],
        init_state,
    )
    arrived = exchange_heads(mixed, n, fs_size, tp_size, hpd)
    heads = arrived.shape[0]
    out = jnp.einsum(
        "htw,hwo->to",
        arrived[:, :, :DV_A],
        output_attend.reshape(heads, DV_A, -1),
        preferred_element_type=jnp.float32,
    ) + jnp.einsum(
        "htw,hwo->to",
        arrived[:, :, DV_A:],
        output_linear.reshape(heads, HDV, -1),
        preferred_element_type=jnp.float32,
    )
    return out.astype(jnp.bfloat16)[None]


def solution(mesh):
    in_specs = (
        P(("grp", "fs"), "sp", None),
        P(),
        P(None, ("fs", "tp"), None),
        P(None, ("fs", "tp"), None),
        P(None, ("fs", "tp"), None),
        P(None, ("fs", "tp"), None),
        P(None, ("fs", "tp"), None),
        P(None, ("fs", "tp"), None),
        P(),
        P(),
        P(),
        P(("grp", "fs"), "sp", None),
        P(),
        P(),
        P(),
        P(),
        P(),
        P("grp", ("fs", "tp"), None, None),
        P(None, "tp"),
        P(None, "tp"),
    )
    out_specs = P(("grp", "fs"), "sp", "tp")
    fs_size, tp_size, sp_size = mesh.shape["fs"], mesh.shape["tp"], mesh.shape["sp"]
    pairs = MIXER_HEADS // tp_size
    chosen = pair_body if pairs == sp_size and tp_size == 2 else body
    return jax.shard_map(chosen, mesh=mesh, in_specs=in_specs, out_specs=out_specs, check_vma=False)
```

```python
import functools

import jax
import jax.numpy as jnp
from jax import lax
from jax.experimental import pallas as pl
from jax.experimental.pallas import tpu as pltpu
from jax.sharding import PartitionSpec as P

MIXER_HEADS = 8
HD_A = 64
DV_A = 128
HDK = 128
HDV = 256
BLK = 64


norm_eps = 1e-06
decay_tau = 16.0


def entering(part, axis, combine, identity):
    place = lax.axis_index(axis)
    gathered = jax.tree.map(lambda a: lax.all_gather(a, axis), part)
    state = jax.tree.map(lambda a, e: jnp.zeros_like(a) + jnp.asarray(e, a.dtype), part, identity)

    def one(hop, state):
        return combine(
            state, jax.tree.map(lambda a: lax.dynamic_index_in_dim(a, hop, 0, False), gathered)
        )

    return lax.fori_loop(0, place, one, state)


def rms_scale(values, gain):
    widened = values.astype(jnp.float32)
    return (
        widened * lax.rsqrt(jnp.mean(widened * widened, axis=-1, keepdims=True) + norm_eps) * gain
    )


def head_order(fs_size, tp_size, tp_rank):
    per_device = MIXER_HEADS // (fs_size * tp_size)
    owners = jnp.arange(fs_size, dtype=jnp.int32)[:, None] * tp_size + tp_rank
    return (owners * per_device + jnp.arange(per_device, dtype=jnp.int32)[None, :]).reshape(-1)


def linear_blocks(queries, keys_in, values_in, log_decay):
    tok_rows, head_count, key_dim = queries.shape
    value_dim = values_in.shape[-1]
    block_count = tok_rows // BLK
    highest_precision = lax.Precision.HIGHEST

    def split_blocks(source):
        return source.reshape(block_count, BLK, head_count, source.shape[-1])

    causal = (
        jnp.arange(BLK, dtype=jnp.int32)[:, None] >= jnp.arange(BLK, dtype=jnp.int32)[None, :]
    )[None]

    def advance(carry, inputs_now):
        recurrent_state, offset = carry
        question_patch_lines, block_k, value_tile_width, block_log = inputs_now
        running_state = jnp.cumsum(block_log, axis=0)
        pivot = running_state[BLK // 2]
        q_scaled = question_patch_lines * jnp.exp(running_state - pivot[None])
        k_scaled = block_k * jnp.exp(pivot[None] - running_state)
        scores = jnp.einsum("thk,shk->hts", q_scaled, k_scaled, precision=highest_precision)
        scores = jnp.where(causal, scores, 0.0)
        inside_block = jnp.einsum(
            "hts,shv->thv", scores, value_tile_width, precision=highest_precision
        )
        inside_block = inside_block + jnp.einsum(
            "jwo,wos->jws",
            question_patch_lines * jnp.exp(running_state),
            recurrent_state,
            precision=highest_precision,
        )
        final_state = running_state[-1]
        faded_memory_matrix = block_k * jnp.exp(final_state[None] - running_state)
        recurrent_state = recurrent_state * jnp.exp(final_state)[:, :, None] + jnp.einsum(
            "zcb,zcw->cbw", faded_memory_matrix, value_tile_width, precision=highest_precision
        )
        reaching_keys = question_patch_lines * jnp.exp(offset[None] + running_state)
        return ((recurrent_state, offset + final_state), (inside_block, reaching_keys))

    start_carry = (
        jnp.zeros((head_count, key_dim, value_dim), jnp.float32),
        jnp.zeros((head_count, key_dim), jnp.float32),
    )
    (recurrent_state, total_decay), (inside_block, reaching_keys) = lax.scan(
        advance,
        start_carry,
        (
            split_blocks(queries),
            split_blocks(keys_in),
            split_blocks(values_in),
            split_blocks(log_decay),
        ),
    )
    return (
        recurrent_state,
        total_decay,
        inside_block.reshape(tok_rows, head_count, value_dim),
        reaching_keys.reshape(tok_rows, head_count, key_dim),
    )


def body(
    tokens,
    norm_gain,
    query_attend,
    key_attend,
    value_attend,
    query_linear,
    key_linear,
    value_linear,
    decay_down,
    decay_up,
    decay_bias,
    log_retain,
    query_gain,
    key_gain,
    diff_lambda,
    mix_gain,
    state_gain,
    init_state,
    output_attend,
    output_linear,
):
    fs_size = lax.axis_size("fs")
    tp_size = lax.axis_size("tp")
    tp_rank = lax.axis_index("tp")
    tok_rows = tokens.shape[1]
    normed = rms_scale(tokens, norm_gain).astype(jnp.bfloat16)
    normed_rows = normed[0]
    local_weights = (query_attend, key_attend, value_attend, query_linear, key_linear, value_linear)
    widths = [weight.shape[1] * weight.shape[2] for weight in local_weights]
    packed = jnp.concatenate(
        [weight.reshape(weight.shape[0], -1) for weight in local_weights], axis=1
    )
    computed = jnp.einsum(
        "std,dp->stp",
        lax.all_gather(normed, "fs", axis=0, tiled=True),
        packed,
        preferred_element_type=jnp.float32,
    ).astype(jnp.bfloat16)
    arrived = lax.all_to_all(computed, "fs", split_axis=0, concat_axis=2, tiled=True).reshape(
        tok_rows, fs_size, -1
    )
    sections = []
    column_at = 0
    for weight, width_now in zip(local_weights, widths):
        section = arrived[:, :, column_at : column_at + width_now]
        sections.append(section.reshape(tok_rows, fs_size * weight.shape[1], weight.shape[2]))
        column_at = column_at + width_now
    projected = tuple(sections)
    q_pair, k_pair, v_attend, q_lin, k_lin, v_lin = projected
    head_ids = head_order(fs_size, tp_size, tp_rank)
    head_count = head_ids.shape[0]
    q_unit = rms_scale(q_pair.reshape(tok_rows, head_count, 2, HD_A), query_gain).astype(
        jnp.bfloat16
    )
    k_unit = rms_scale(
        k_pair.reshape(tok_rows, head_count, 2, HD_A), jnp.take(key_gain, head_ids, axis=0)
    ).astype(jnp.bfloat16)
    sp_start = lax.axis_index("sp") * tok_rows
    query_block = (sp_start + jnp.arange(tok_rows, dtype=jnp.int32)) // BLK
    score_scale = HD_A ** (-0.5)
    blank_attend = (
        jnp.full((head_count, 2, tok_rows), -jnp.inf, jnp.float32),
        jnp.zeros((head_count, 2, tok_rows), jnp.float32),
        jnp.zeros((head_count, 2, tok_rows, DV_A), jnp.float32),
    )
    carry = blank_attend
    seg_keys = lax.all_gather(k_unit, "sp", axis=0, tiled=True)
    seg_values = lax.all_gather(v_attend, "sp", axis=0, tiled=True)
    span = seg_keys.shape[0]
    stride_token_lines = 2 * tok_rows
    step_count = span // stride_token_lines
    key_steps = seg_keys.reshape(step_count, stride_token_lines, head_count, 2, HD_A)
    value_steps = seg_values.reshape(step_count, stride_token_lines, head_count, DV_A)

    def one_step(running_state, inputs_now):
        step_index, key_step, value_step = inputs_now
        key_start = step_index * stride_token_lines

        def compute(current):
            run_max, run_total, run_acc = current
            scores = (
                jnp.einsum("qhmd,khmd->hmqk", q_unit, key_step, preferred_element_type=jnp.float32)
                * score_scale
            )
            key_block = (key_start + jnp.arange(stride_token_lines, dtype=jnp.int32)) // BLK
            allowed = query_block[:, None] >= key_block[None, :]
            scores = jnp.where(allowed, scores, -jnp.inf)
            new_max = jnp.maximum(run_max, jnp.max(scores, axis=-1))
            factor = jnp.exp(run_max - new_max)
            raised = jnp.exp(scores - new_max[..., None])
            run_total = run_total * factor + jnp.sum(raised, axis=-1)
            run_acc = run_acc * factor[..., None] + jnp.einsum(
                "hmqk,khv->hmqv",
                raised.astype(jnp.bfloat16),
                value_step,
                preferred_element_type=jnp.float32,
            )
            return (new_max, run_total, run_acc)

        def unchanged(current):
            return current

        return (lax.cond(key_start <= sp_start, compute, unchanged, running_state), None)

    carry, _ = lax.scan(
        one_step, carry, (jnp.arange(step_count, dtype=jnp.int32), key_steps, value_steps)
    )
    run_max, run_total, run_acc = carry
    lambda_heads = jnp.take(diff_lambda, head_ids, axis=0)
    diff_raw = (
        run_acc[:, 0] / run_total[:, 0, :, None]
        - lambda_heads[:, None, None] * run_acc[:, 1] / run_total[:, 1, :, None]
    )
    attend_out = rms_scale(jnp.transpose(diff_raw, (1, 0, 2)), mix_gain).astype(jnp.bfloat16)
    low_rank = jnp.dot(normed_rows, decay_down, preferred_element_type=jnp.float32).astype(
        jnp.bfloat16
    )
    up_columns = jnp.take(decay_up, head_ids, axis=1)
    pre_act = jnp.einsum(
        "tr,rhk->thk", low_rank, up_columns, preferred_element_type=jnp.float32
    ) + jnp.take(decay_bias, head_ids, axis=0)
    retain_heads = jnp.take(log_retain[0], head_ids, axis=1)
    log_decay = jax.nn.log_sigmoid(pre_act) / decay_tau + retain_heads[:, :, None]
    local_state, local_decay, inside_block, reaching_keys = linear_blocks(
        q_lin.astype(jnp.float32) * HDK ** (-0.5),
        k_lin.astype(jnp.float32),
        v_lin.astype(jnp.float32),
        log_decay,
    )

    def chain(earlier, later):
        return (earlier[0] + later[0], earlier[1] * jnp.exp(later[0])[:, :, None] + later[1])

    zero_chain = (jnp.zeros_like(local_decay), jnp.zeros_like(local_state))
    prior_decay, prior_state = entering((local_decay, local_state), "sp", chain, zero_chain)
    start_state = lax.all_to_all(init_state, "fs", split_axis=0, concat_axis=1, tiled=True)[0]
    incoming_state = start_state * jnp.exp(prior_decay)[:, :, None] + prior_state
    linear_raw = inside_block + jnp.einsum(
        "jwo,wos->jws", reaching_keys, incoming_state, precision=lax.Precision.HIGHEST
    )
    linear_out = rms_scale(linear_raw, state_gain).astype(jnp.bfloat16)
    out_cols = output_attend.shape[1]
    per_device = MIXER_HEADS // (fs_size * tp_size)
    attend_view = output_attend.reshape(fs_size, tp_size, per_device * DV_A, out_cols)
    linear_view = output_linear.reshape(fs_size, tp_size, per_device * HDV, out_cols)
    blank_out = jnp.zeros((tok_rows, out_cols), jnp.float32)
    running_out = blank_out
    seg_attend = lax.all_gather(attend_out, "tp", axis=1, tiled=True)
    seg_linear = lax.all_gather(linear_out, "tp", axis=1, tiled=True)
    shard_count = seg_attend.shape[1] // head_count
    first_rank = jnp.int32(0) // head_count
    for shard_step in range(shard_count):
        owner_rank = first_rank + shard_step
        rows_attend = lax.dynamic_index_in_dim(attend_view, owner_rank, 1, keepdims=False).reshape(
            -1, out_cols
        )
        rows_linear = lax.dynamic_index_in_dim(linear_view, owner_rank, 1, keepdims=False).reshape(
            -1, out_cols
        )
        part_attend = seg_attend[
            :, shard_step * head_count : (shard_step + 1) * head_count
        ].reshape(tok_rows, -1)
        part_linear = seg_linear[
            :, shard_step * head_count : (shard_step + 1) * head_count
        ].reshape(tok_rows, -1)
        running_out = running_out + jnp.dot(
            part_attend, rows_attend, preferred_element_type=jnp.float32
        )
        running_out = running_out + jnp.dot(
            part_linear, rows_linear, preferred_element_type=jnp.float32
        )
    return running_out.astype(jnp.bfloat16).reshape(1, tok_rows, out_cols)


MESH = pl.DeviceIdType.MESH


def group_barrier(n, fs_size, tp_size):
    z, f, c = lax.axis_index("sp"), lax.axis_index("fs"), lax.axis_index("tp")
    barrier = pltpu.get_barrier_semaphore()
    total = n * fs_size * tp_size
    me = (z * fs_size + f) * tp_size + c
    for k in range(1, total):
        other = lax.rem(me + k, total)
        oz = other // (fs_size * tp_size)
        of = lax.rem(other // tp_size, fs_size)
        oc = lax.rem(other, tp_size)
        pl.semaphore_signal(
            barrier, inc=1, device_id={"sp": oz, "fs": of, "tp": oc}, device_id_type=MESH
        )
    pl.semaphore_wait(barrier, total - 1)


def remote(src, dst, send, recv, **where):
    return pltpu.make_async_remote_copy(
        src_ref=src,
        dst_ref=dst,
        send_sem=send,
        recv_sem=recv,
        device_id=where,
        device_id_type=MESH,
    )


def gather_kernel(
    n,
    fs_size,
    tp_size,
    hpd,
    tok_ref,
    ret_ref,
    gain_ref,
    down_ref,
    wq_ref,
    wk_ref,
    wv_ref,
    lq_ref,
    lk_ref,
    lv_ref,
    proj_ref,
    low_ref,
    rout_ref,
    seq_ref,
    relay_ref,
    raw_ref,
    raw_v_ref,
    w_ref,
    recv_a,
    recv_b,
    recv_l,
    recv_r,
    send_x,
    send_row,
    send_rl,
    send_up,
    send_down,
    send_sib,
    send_r,
    loc,
    wsem,
):
    z, f, c = lax.axis_index("sp"), lax.axis_index("fs"), lax.axis_index("tp")
    rows, width = tok_ref.shape
    half = rows // tp_size
    pieces = recv_l.shape[0]
    prow = half // pieces
    loads = [
        pltpu.make_async_copy(ref, raw_ref.at[i], wsem.at[i])
        for i, ref in enumerate((wq_ref, wk_ref, wv_ref, lq_ref, lk_ref))
    ]
    loads.append(pltpu.make_async_copy(lv_ref, raw_v_ref, wsem.at[5]))
    for load in loads:
        load.start()
    group_barrier(n, fs_size, tp_size)
    s = z // hpd
    own = s == f
    strange = jnp.logical_not(own)

    def nearest(seq):
        return jnp.minimum(jnp.maximum(z, seq * hpd), seq * hpd + hpd - 1)

    def piece(zc, core, p):
        return seq_ref.at[pl.ds(pl.multiple_of(zc * rows + core * half + p * prow, prow), prow)]

    lo = f * hpd
    rsends = []
    for j in range(hpd):
        for k in range(fs_size):
            x = lax.rem(f + k, fs_size)
            there = lo + j
            copy = remote(
                ret_ref,
                rout_ref.at[z],
                send_r.at[j * fs_size + k],
                recv_r.at[z],
                sp=there,
                fs=x,
            )
            go = jnp.logical_not((there == z) & (x == f))
            pl.when(go)(copy.start)
            rsends.append((go, copy))
    sends = []
    for p in range(pieces):
        mine = tok_ref.at[pl.ds(pl.multiple_of(c * half + p * prow, prow), prow)]
        there = relay_ref.at[pl.ds(p * prow, prow)]
        over = remote(mine, piece(z, c, p), send_x.at[p], recv_a.at[z, p], fs=1 - f)
        pl.when(own)(over.start)
        lent = remote(mine, there, send_x.at[p], recv_l.at[p], fs=1 - f)
        pl.when(strange)(lent.start)
        along = remote(mine, piece(z, c, p), send_row.at[p], recv_a.at[z, p], sp=nearest(f))
        pl.when(strange)(along.start)
        sends += [(own, over), (strange, lent), (strange, along)]
    full = pl.ds(pl.multiple_of(z * rows, rows), rows)
    local = pltpu.make_async_copy(tok_ref, seq_ref.at[full], loc.at[0])
    local_r = pltpu.make_async_copy(ret_ref, rout_ref.at[z], loc.at[1])
    pl.when(own)(local.start)
    pl.when(own)(local_r.start)

    slot = lax.rem(z, hpd)
    step = 128

    def pick(source, target_cols, parts, part):
        span = step * parts * hpd
        sel = (
            lax.broadcasted_iota(jnp.int32, (step, span), 1)
            == (lax.broadcasted_iota(jnp.int32, (step, span), 0) * parts + part) * hpd + slot
        ).astype(jnp.bfloat16)

        def one(i, carry):
            block = source[pl.ds(pl.multiple_of(i * span, span), span), :]
            w_ref[pl.ds(pl.multiple_of(i * step, step), step), target_cols] = jnp.dot(
                sel, block, preferred_element_type=jnp.float32
            ).astype(jnp.bfloat16)
            return carry

        lax.fori_loop(0, width // step, one, 0)

    def pick_all(first, last):
        for i in range(first, min(last, 5)):
            loads[i].wait()
            pick(raw_ref.at[i], slice(i * 128, (i + 1) * 128), 1, 0)
        if last > 5:
            loads[5].wait()
            for part in range(2):
                pick(raw_v_ref, slice((5 + part) * 128, (6 + part) * 128), 2, part)

    mlo = s * hpd
    mhi = mlo + hpd - 1

    def pass_on(p):
        held = relay_ref.at[pl.ds(p * prow, prow)]
        lent = remote(held, piece(z, c, p), send_rl.at[p], recv_l.at[p], sp=nearest(1 - f))
        pl.when(own)(lent.wait_recv)
        along = remote(held, piece(z, c, p), send_rl.at[p], recv_a.at[z, p], sp=nearest(1 - f))
        pl.when(own)(along.start)
        sends.append((own, along))
        for k in range(n):
            zc = jnp.where(2 * z < n, n - 1 - k, k)
            away = jnp.logical_not((zc == z) & own)
            block = piece(zc, c, p)
            arrive = remote(block, block, send_sib.at[k, p], recv_a.at[zc, p], tp=1 - c)
            pl.when(away)(arrive.wait_recv)
            up = remote(
                block, block, send_up.at[k, p], recv_a.at[zc, p], sp=jnp.minimum(z + 1, n - 1)
            )
            go_up = (zc <= z) & (z + 1 <= mhi)
            pl.when(go_up)(up.start)
            down = remote(
                block, block, send_down.at[k, p], recv_a.at[zc, p], sp=jnp.maximum(z - 1, 0)
            )
            go_down = (zc >= z) & (z - 1 >= mlo)
            pl.when(go_down)(down.start)
            sib = remote(block, block, send_sib.at[k, p], recv_b.at[zc, p], tp=1 - c)
            pl.when(away)(sib.start)
            sends.extend([(go_up, up), (go_down, down), (away, sib)])

    def finish(p):
        for zc in range(n):
            away = jnp.logical_not((zc == z) & own)
            other = piece(zc, 1 - c, p)
            came = remote(other, other, send_sib.at[zc, p], recv_b.at[zc, p], tp=1 - c)
            pl.when(away)(came.wait_recv)
        spots = [
            slice(zc * rows + core * half + p * prow, zc * rows + core * half + (p + 1) * prow)
            for zc in range(n)
            for core in range(tp_size)
        ]
        x = jnp.concatenate([seq_ref[spot, :] for spot in spots], axis=0).astype(jnp.float32)
        scale = lax.rsqrt(jnp.mean(x * x, axis=-1, keepdims=True) + norm_eps)
        normed = (x * scale * gain_ref[...]).astype(jnp.bfloat16)
        made = jnp.dot(normed, w_ref[...], preferred_element_type=jnp.float32).astype(jnp.bfloat16)
        low = lax.dot_general(
            normed, down_ref[...], (((1,), (1,)), ((), ())), preferred_element_type=jnp.float32
        ).astype(jnp.bfloat16)
        for i, spot in enumerate(spots):
            proj_ref[spot, :] = made[i * prow : (i + 1) * prow]
            low_ref[spot, :] = low[i * prow : (i + 1) * prow]

    pl.when(own)(local.wait)
    pass_on(0)
    pick_all(0, 3)
    for p in range(1, pieces):
        pass_on(p)
        if p == 1:
            pick_all(3, 6)
        finish(p - 1)
    finish(pieces - 1)
    pl.when(own)(local_r.wait)
    for go, copy in rsends + sends:
        pl.when(go)(copy.wait_send)
    for zc in range(n):
        away = jnp.logical_not((zc == z) & own)
        came_r = remote(ret_ref, rout_ref.at[zc], send_r.at[0], recv_r.at[zc], tp=1 - c)
        pl.when(away)(came_r.wait_recv)


def interleaved(weight):
    width, hpd, columns = weight.shape
    parts = columns // 128
    return jnp.swapaxes(weight.reshape(width, hpd, parts, 128), 1, 2).reshape(-1, 128)


def gather_positions(tokens, retain, gain, down, weights, n, fs_size, tp_size, hpd):
    rows, width = tokens.shape
    dma = pltpu.SemaphoreType.DMA
    flat = [interleaved(weight) for weight in weights]
    pieces = max(1, rows // tp_size // 16)
    columns = sum(weight.shape[2] for weight in weights)
    vmem = pl.BlockSpec(memory_space=pltpu.VMEM)
    anywhere = pl.BlockSpec(memory_space=pl.ANY)
    return pl.pallas_call(
        functools.partial(gather_kernel, n, fs_size, tp_size, hpd),
        out_shape=(
            jax.ShapeDtypeStruct((n * rows, columns), jnp.bfloat16),
            jax.ShapeDtypeStruct((n * rows, down.shape[0]), jnp.bfloat16),
            jax.ShapeDtypeStruct((n,) + retain.shape, retain.dtype),
        ),
        in_specs=[vmem] * 4 + [anywhere] * 6,
        out_specs=(vmem, vmem, anywhere),
        scratch_shapes=[
            pltpu.VMEM((n * rows, width), jnp.bfloat16),
            pltpu.VMEM((rows // tp_size, width), jnp.bfloat16),
            pltpu.VMEM((5,) + flat[0].shape, jnp.bfloat16),
            pltpu.VMEM(flat[5].shape, jnp.bfloat16),
            pltpu.VMEM((width, columns), jnp.bfloat16),
            dma((n, pieces)),
            dma((n, pieces)),
            dma((pieces,)),
            dma((n,)),
            dma((pieces,)),
            dma((pieces,)),
            dma((pieces,)),
            dma((n, pieces)),
            dma((n, pieces)),
            dma((n, pieces)),
            dma((hpd * fs_size,)),
            dma((2,)),
            dma((6,)),
        ],
        compiler_params=pltpu.CompilerParams(collective_id=0, has_side_effects=True),
    )(tokens, retain, gain, down, *flat)


def mix_kernel(
    hpd,
    tp_size,
    lam_ref,
    proj_ref,
    low_ref,
    ret_ref,
    up_ref,
    bias_ref,
    qg_ref,
    kg_ref,
    mg_ref,
    sg_ref,
    init_ref,
    out_ref,
):
    z, f, c = lax.axis_index("sp"), lax.axis_index("fs"), lax.axis_index("tp")
    slot = lax.rem(z, hpd)
    seq = z // hpd
    head = (f * tp_size + c) * hpd + slot
    f32, bf16 = jnp.float32, jnp.bfloat16
    length = proj_ref.shape[0]
    lane = lax.broadcasted_iota(jnp.int32, (1, 2 * HD_A), 1)
    first = lane < HD_A

    def unit(cols, gain):
        x = proj_ref[:, cols].astype(f32)
        sq = x * x
        m0 = jnp.sum(jnp.where(first, sq, 0.0), axis=-1, keepdims=True) / HD_A
        m1 = jnp.sum(jnp.where(first, 0.0, sq), axis=-1, keepdims=True) / HD_A
        r = jnp.where(first, lax.rsqrt(m0 + norm_eps), lax.rsqrt(m1 + norm_eps))
        return (x * r * gain).astype(bf16)

    q_gain = jnp.concatenate([qg_ref[...], qg_ref[...]], axis=1)
    k_pair = kg_ref[pl.ds(head, 1)]
    k_gain = jnp.concatenate([k_pair[:, 0], k_pair[:, 1]], axis=1)
    q_unit = unit(slice(0, 128), q_gain)
    k_unit = unit(slice(128, 256), k_gain)
    zero = jnp.zeros_like(q_unit)
    q_maps = (jnp.where(first, q_unit, zero), jnp.where(first, zero, q_unit))
    tile = 2 * BLK
    key_b = lax.broadcasted_iota(jnp.int32, (tile, tile), 1) // BLK
    query_b = lax.broadcasted_iota(jnp.int32, (tile, tile), 0) // BLK
    allowed = query_b >= key_b
    lam = lam_ref[head]
    for i in range(length // tile):
        at = slice(i * tile, (i + 1) * tile)
        parts = []
        for m in range(2):
            q = q_maps[m][at]
            diag = (
                lax.dot_general(
                    q, k_unit[at], (((1,), (1,)), ((), ())), preferred_element_type=f32
                )
                * HD_A ** (-0.5)
            )
            diag = jnp.where(allowed, diag, -jnp.inf)
            top = jnp.max(diag, axis=-1, keepdims=True)
            if i > 0:
                past = (
                    lax.dot_general(
                        q,
                        k_unit[: i * tile],
                        (((1,), (1,)), ((), ())),
                        preferred_element_type=f32,
                    )
                    * HD_A ** (-0.5)
                )
                top = jnp.maximum(top, jnp.max(past, axis=-1, keepdims=True))
            raised = jnp.exp(diag - top)
            total = jnp.sum(raised, axis=-1, keepdims=True)
            acc = jnp.dot(raised.astype(bf16), proj_ref[at, 256:384], preferred_element_type=f32)
            if i > 0:
                raised = jnp.exp(past - top)
                total = total + jnp.sum(raised, axis=-1, keepdims=True)
                acc = acc + jnp.dot(
                    raised.astype(bf16), proj_ref[: i * tile, 256:384], preferred_element_type=f32
                )
            parts.append(acc / total)
        diff = parts[0] - lam * parts[1]
        scale = lax.rsqrt(jnp.mean(diff * diff, axis=-1, keepdims=True) + norm_eps)
        out_ref[at, :DV_A] = (diff * scale * mg_ref[...]).astype(bf16)

    up = up_ref[:, pl.ds(pl.multiple_of(head * HDK, HDK), HDK)]
    bias = bias_ref[pl.ds(head, 1), :]
    r64 = lax.broadcasted_iota(jnp.int32, (BLK, BLK), 0)
    c64 = lax.broadcasted_iota(jnp.int32, (BLK, BLK), 1)
    causal = r64 >= c64
    lower = causal.astype(f32)
    eye_k = lax.broadcasted_iota(jnp.int32, (HDK, HDK), 0) == lax.broadcasted_iota(
        jnp.int32, (HDK, HDK), 1
    )
    pre = jnp.dot(low_ref[...], up, preferred_element_type=f32) + bias
    log_sig = jnp.minimum(pre, 0.0) - jnp.log1p(jnp.exp(-jnp.abs(pre)))
    log_sig = log_sig / decay_tau
    state = init_ref[pl.ds(seq, 1), pl.ds(slot, 1)].reshape(HDK, HDV)
    rows = ret_ref.shape[2]
    per = rows // BLK
    for b in range(length // BLK):
        at = slice(b * BLK, (b + 1) * BLK)
        ret = ret_ref[b // per, pl.ds(head, 1), :][:, (b % per) * BLK : (b % per + 1) * BLK]
        column = jnp.sum(jnp.where(r64 == c64, ret, 0.0), axis=-1, keepdims=True)
        logs = log_sig[at] + column
        run = jnp.dot(
            lower, logs, preferred_element_type=f32, precision=lax.Precision.HIGHEST
        )
        pivot = run[BLK // 2 : BLK // 2 + 1]
        last = run[BLK - 1 : BLK]
        q = proj_ref[at, 384:512].astype(f32) * HDK ** (-0.5)
        k = proj_ref[at, 512:640].astype(f32)
        v = proj_ref[at, 640:896]
        qs = (q * jnp.exp(run - pivot)).astype(bf16)
        ks = (k * jnp.exp(pivot - run)).astype(bf16)
        inner = lax.dot_general(qs, ks, (((1,), (1,)), ((), ())), preferred_element_type=f32)
        inner = jnp.where(causal, inner, 0.0).astype(bf16)
        raw = jnp.dot(inner, v, preferred_element_type=f32) + jnp.dot(
            (q * jnp.exp(run)).astype(bf16), state.astype(bf16), preferred_element_type=f32
        )
        faded = (k * jnp.exp(last - run)).astype(bf16)
        keep = jnp.sum(jnp.where(eye_k, jnp.exp(last), 0.0), axis=-1, keepdims=True)
        state = state * keep + lax.dot_general(
            faded, v, (((0,), (0,)), ((), ())), preferred_element_type=f32
        )
        scale = lax.rsqrt(jnp.mean(raw * raw, axis=-1, keepdims=True) + norm_eps)
        out_ref[at, DV_A:] = (raw * scale * sg_ref[...]).astype(bf16)


def exchange_kernel(
    n,
    fs_size,
    tp_size,
    hpd,
    mix_ref,
    out_ref,
    stage,
    recv_row,
    recv_x,
    recv_s,
    send_row,
    send_x,
    send_s,
    loc,
):
    z, f, c = lax.axis_index("sp"), lax.axis_index("fs"), lax.axis_index("tp")
    rows = out_ref.shape[1]
    group_barrier(n, fs_size, tp_size)
    s = z // hpd
    keep = s == f
    cross = jnp.logical_not(keep)

    def head(x, core, zs):
        return (x * tp_size + core) * hpd + lax.rem(zs, hpd)

    def chunk(zt):
        return mix_ref.at[pl.ds(pl.multiple_of(zt * rows, rows), rows)]

    my_head = head(f, c, z)
    waits = []
    for k in range(1, n):
        zt = lax.rem(z + k, n)
        kept = remote(chunk(zt), out_ref.at[my_head], send_row.at[k], recv_row.at[z], sp=zt)
        moved = remote(chunk(zt), stage.at[z], send_row.at[k], recv_row.at[z], sp=zt)
        pl.when(keep)(kept.start)
        pl.when(cross)(moved.start)
        waits.append((None, kept))
    local = pltpu.make_async_copy(chunk(z), out_ref.at[my_head], loc)
    pl.when(keep)(local.start)
    sib0 = remote(chunk(z), out_ref.at[my_head], send_s.at[my_head], recv_s.at[my_head], tp=1 - c)
    pl.when(keep)(sib0.start)
    waits.append((keep, sib0))
    x0 = remote(chunk(z), out_ref.at[my_head], send_x.at[0], recv_x.at[my_head], fs=s)
    pl.when(cross)(x0.start)
    waits.append((cross, x0))
    for k in range(1, n):
        zs = lax.rem(z + k, n)
        sq = zs // hpd
        hd = head(f, c, zs)
        final = sq == f
        onward = jnp.logical_not(final)
        landed = remote(stage.at[zs], stage.at[zs], send_x.at[k], recv_row.at[zs], tp=1 - c)
        landed.wait_recv()
        sib = remote(out_ref.at[hd], out_ref.at[hd], send_s.at[hd], recv_s.at[hd], tp=1 - c)
        pl.when(final)(sib.start)
        waits.append((final, sib))
        xs = remote(stage.at[zs], out_ref.at[hd], send_x.at[k], recv_x.at[hd], fs=sq)
        pl.when(onward)(xs.start)
        waits.append((onward, xs))
    for k in range(1, fs_size):
        x = lax.rem(f + k, fs_size)
        for j in range(hpd):
            hd = head(x, c, j)
            block = out_ref.at[hd]
            came = remote(block, block, send_s.at[hd], recv_x.at[hd], tp=1 - c)
            came.wait_recv()
            sib = remote(block, block, send_s.at[hd], recv_s.at[hd], tp=1 - c)
            sib.start()
            waits.append((None, sib))
    for x in range(fs_size):
        for j in range(hpd):
            hd = head(x, 1 - c, j)
            block = out_ref.at[hd]
            remote(block, block, send_s.at[hd], recv_s.at[hd], tp=1 - c).wait_recv()
    pl.when(keep)(local.wait)
    for go, copy in waits:
        if go is None:
            copy.wait_send()
        else:
            pl.when(go)(copy.wait_send)


def exchange_heads(mixed, n, fs_size, tp_size, hpd):
    rows, width = mixed.shape[0] // n, mixed.shape[1]
    heads = fs_size * tp_size * hpd
    dma = pltpu.SemaphoreType.DMA
    return pl.pallas_call(
        functools.partial(exchange_kernel, n, fs_size, tp_size, hpd),
        out_shape=jax.ShapeDtypeStruct((heads, rows, width), mixed.dtype),
        in_specs=[pl.BlockSpec(memory_space=pltpu.VMEM)],
        out_specs=pl.BlockSpec(memory_space=pl.ANY),
        scratch_shapes=[
            pltpu.VMEM((n, rows, width), mixed.dtype),
            dma((n,)),
            dma((heads,)),
            dma((heads,)),
            dma((n,)),
            dma((n,)),
            dma((heads,)),
            dma,
        ],
        compiler_params=pltpu.CompilerParams(collective_id=1, has_side_effects=True),
    )(mixed)


def pair_body(
    tokens,
    norm_gain,
    query_attend,
    key_attend,
    value_attend,
    query_linear,
    key_linear,
    value_linear,
    decay_down,
    decay_up,
    decay_bias,
    log_retain,
    query_gain,
    key_gain,
    diff_lambda,
    mix_gain,
    state_gain,
    init_state,
    output_attend,
    output_linear,
):
    n, fs_size, tp_size = lax.axis_size("sp"), lax.axis_size("fs"), lax.axis_size("tp")
    hpd = query_attend.shape[1]
    weights = (query_attend, key_attend, value_attend, query_linear, key_linear, value_linear)
    projected, low_rank, retained = gather_positions(
        tokens[0],
        jnp.transpose(log_retain[0]),
        norm_gain[None],
        jnp.transpose(decay_down),
        weights,
        n,
        fs_size,
        tp_size,
        hpd,
    )
    vmem = pl.BlockSpec(memory_space=pltpu.VMEM)
    mixed = pl.pallas_call(
        functools.partial(mix_kernel, hpd, tp_size),
        out_shape=jax.ShapeDtypeStruct((projected.shape[0], DV_A + HDV), jnp.bfloat16),
        in_specs=[pl.BlockSpec(memory_space=pltpu.SMEM)] + [vmem] * 10,
        out_specs=vmem,
    )(
        diff_lambda,
        projected,
        low_rank,
        retained,
        decay_up.reshape(decay_up.shape[0], -1),
        decay_bias,
        query_gain[None],
        key_gain,
        mix_gain[None],
        state_gain[None],
        init_state,
    )
    arrived = exchange_heads(mixed, n, fs_size, tp_size, hpd)
    heads = arrived.shape[0]
    out = jnp.einsum(
        "htw,hwo->to",
        arrived[:, :, :DV_A],
        output_attend.reshape(heads, DV_A, -1),
        preferred_element_type=jnp.float32,
    ) + jnp.einsum(
        "htw,hwo->to",
        arrived[:, :, DV_A:],
        output_linear.reshape(heads, HDV, -1),
        preferred_element_type=jnp.float32,
    )
    return out.astype(jnp.bfloat16)[None]


def solution(mesh):
    in_specs = (
        P(("grp", "fs"), "sp", None),
        P(),
        P(None, ("fs", "tp"), None),
        P(None, ("fs", "tp"), None),
        P(None, ("fs", "tp"), None),
        P(None, ("fs", "tp"), None),
        P(None, ("fs", "tp"), None),
        P(None, ("fs", "tp"), None),
        P(),
        P(),
        P(),
        P(("grp", "fs"), "sp", None),
        P(),
        P(),
        P(),
        P(),
        P(),
        P("grp", ("fs", "tp"), None, None),
        P(None, "tp"),
        P(None, "tp"),
    )
    out_specs = P(("grp", "fs"), "sp", "tp")
    fs_size, tp_size, sp_size = mesh.shape["fs"], mesh.shape["tp"], mesh.shape["sp"]
    pairs = MIXER_HEADS // tp_size
    chosen = pair_body if pairs == sp_size and tp_size == 2 and fs_size == 2 else body
    return jax.shard_map(chosen, mesh=mesh, in_specs=in_specs, out_specs=out_specs, check_vma=False)
```

```python
import functools

import jax
import jax.numpy as jnp
from jax import lax
from jax.experimental import pallas as pl
from jax.experimental.pallas import tpu as pltpu
from jax.sharding import PartitionSpec as P

MIXER_HEADS = 8
HD_A = 64
DV_A = 128
HDK = 128
HDV = 256
BLK = 64


norm_eps = 1e-06
decay_tau = 16.0


def entering(part, axis, combine, identity):
    place = lax.axis_index(axis)
    gathered = jax.tree.map(lambda a: lax.all_gather(a, axis), part)
    state = jax.tree.map(lambda a, e: jnp.zeros_like(a) + jnp.asarray(e, a.dtype), part, identity)

    def one(hop, state):
        return combine(
            state, jax.tree.map(lambda a: lax.dynamic_index_in_dim(a, hop, 0, False), gathered)
        )

    return lax.fori_loop(0, place, one, state)


def rms_scale(values, gain):
    widened = values.astype(jnp.float32)
    return (
        widened * lax.rsqrt(jnp.mean(widened * widened, axis=-1, keepdims=True) + norm_eps) * gain
    )


def head_order(fs_size, tp_size, tp_rank):
    per_device = MIXER_HEADS // (fs_size * tp_size)
    owners = jnp.arange(fs_size, dtype=jnp.int32)[:, None] * tp_size + tp_rank
    return (owners * per_device + jnp.arange(per_device, dtype=jnp.int32)[None, :]).reshape(-1)


def linear_blocks(queries, keys_in, values_in, log_decay):
    tok_rows, head_count, key_dim = queries.shape
    value_dim = values_in.shape[-1]
    block_count = tok_rows // BLK
    highest_precision = lax.Precision.HIGHEST

    def split_blocks(source):
        return source.reshape(block_count, BLK, head_count, source.shape[-1])

    causal = (
        jnp.arange(BLK, dtype=jnp.int32)[:, None] >= jnp.arange(BLK, dtype=jnp.int32)[None, :]
    )[None]

    def advance(carry, inputs_now):
        recurrent_state, offset = carry
        question_patch_lines, block_k, value_tile_width, block_log = inputs_now
        running_state = jnp.cumsum(block_log, axis=0)
        pivot = running_state[BLK // 2]
        q_scaled = question_patch_lines * jnp.exp(running_state - pivot[None])
        k_scaled = block_k * jnp.exp(pivot[None] - running_state)
        scores = jnp.einsum("thk,shk->hts", q_scaled, k_scaled, precision=highest_precision)
        scores = jnp.where(causal, scores, 0.0)
        inside_block = jnp.einsum(
            "hts,shv->thv", scores, value_tile_width, precision=highest_precision
        )
        inside_block = inside_block + jnp.einsum(
            "jwo,wos->jws",
            question_patch_lines * jnp.exp(running_state),
            recurrent_state,
            precision=highest_precision,
        )
        final_state = running_state[-1]
        faded_memory_matrix = block_k * jnp.exp(final_state[None] - running_state)
        recurrent_state = recurrent_state * jnp.exp(final_state)[:, :, None] + jnp.einsum(
            "zcb,zcw->cbw", faded_memory_matrix, value_tile_width, precision=highest_precision
        )
        reaching_keys = question_patch_lines * jnp.exp(offset[None] + running_state)
        return ((recurrent_state, offset + final_state), (inside_block, reaching_keys))

    start_carry = (
        jnp.zeros((head_count, key_dim, value_dim), jnp.float32),
        jnp.zeros((head_count, key_dim), jnp.float32),
    )
    (recurrent_state, total_decay), (inside_block, reaching_keys) = lax.scan(
        advance,
        start_carry,
        (
            split_blocks(queries),
            split_blocks(keys_in),
            split_blocks(values_in),
            split_blocks(log_decay),
        ),
    )
    return (
        recurrent_state,
        total_decay,
        inside_block.reshape(tok_rows, head_count, value_dim),
        reaching_keys.reshape(tok_rows, head_count, key_dim),
    )


def body(
    tokens,
    norm_gain,
    query_attend,
    key_attend,
    value_attend,
    query_linear,
    key_linear,
    value_linear,
    decay_down,
    decay_up,
    decay_bias,
    log_retain,
    query_gain,
    key_gain,
    diff_lambda,
    mix_gain,
    state_gain,
    init_state,
    output_attend,
    output_linear,
):
    fs_size = lax.axis_size("fs")
    tp_size = lax.axis_size("tp")
    tp_rank = lax.axis_index("tp")
    tok_rows = tokens.shape[1]
    normed = rms_scale(tokens, norm_gain).astype(jnp.bfloat16)
    normed_rows = normed[0]
    local_weights = (query_attend, key_attend, value_attend, query_linear, key_linear, value_linear)
    widths = [weight.shape[1] * weight.shape[2] for weight in local_weights]
    packed = jnp.concatenate(
        [weight.reshape(weight.shape[0], -1) for weight in local_weights], axis=1
    )
    computed = jnp.einsum(
        "std,dp->stp",
        lax.all_gather(normed, "fs", axis=0, tiled=True),
        packed,
        preferred_element_type=jnp.float32,
    ).astype(jnp.bfloat16)
    arrived = lax.all_to_all(computed, "fs", split_axis=0, concat_axis=2, tiled=True).reshape(
        tok_rows, fs_size, -1
    )
    sections = []
    column_at = 0
    for weight, width_now in zip(local_weights, widths):
        section = arrived[:, :, column_at : column_at + width_now]
        sections.append(section.reshape(tok_rows, fs_size * weight.shape[1], weight.shape[2]))
        column_at = column_at + width_now
    projected = tuple(sections)
    q_pair, k_pair, v_attend, q_lin, k_lin, v_lin = projected
    head_ids = head_order(fs_size, tp_size, tp_rank)
    head_count = head_ids.shape[0]
    q_unit = rms_scale(q_pair.reshape(tok_rows, head_count, 2, HD_A), query_gain).astype(
        jnp.bfloat16
    )
    k_unit = rms_scale(
        k_pair.reshape(tok_rows, head_count, 2, HD_A), jnp.take(key_gain, head_ids, axis=0)
    ).astype(jnp.bfloat16)
    sp_start = lax.axis_index("sp") * tok_rows
    query_block = (sp_start + jnp.arange(tok_rows, dtype=jnp.int32)) // BLK
    score_scale = HD_A ** (-0.5)
    blank_attend = (
        jnp.full((head_count, 2, tok_rows), -jnp.inf, jnp.float32),
        jnp.zeros((head_count, 2, tok_rows), jnp.float32),
        jnp.zeros((head_count, 2, tok_rows, DV_A), jnp.float32),
    )
    carry = blank_attend
    seg_keys = lax.all_gather(k_unit, "sp", axis=0, tiled=True)
    seg_values = lax.all_gather(v_attend, "sp", axis=0, tiled=True)
    span = seg_keys.shape[0]
    stride_token_lines = 2 * tok_rows
    step_count = span // stride_token_lines
    key_steps = seg_keys.reshape(step_count, stride_token_lines, head_count, 2, HD_A)
    value_steps = seg_values.reshape(step_count, stride_token_lines, head_count, DV_A)

    def one_step(running_state, inputs_now):
        step_index, key_step, value_step = inputs_now
        key_start = step_index * stride_token_lines

        def compute(current):
            run_max, run_total, run_acc = current
            scores = (
                jnp.einsum("qhmd,khmd->hmqk", q_unit, key_step, preferred_element_type=jnp.float32)
                * score_scale
            )
            key_block = (key_start + jnp.arange(stride_token_lines, dtype=jnp.int32)) // BLK
            allowed = query_block[:, None] >= key_block[None, :]
            scores = jnp.where(allowed, scores, -jnp.inf)
            new_max = jnp.maximum(run_max, jnp.max(scores, axis=-1))
            factor = jnp.exp(run_max - new_max)
            raised = jnp.exp(scores - new_max[..., None])
            run_total = run_total * factor + jnp.sum(raised, axis=-1)
            run_acc = run_acc * factor[..., None] + jnp.einsum(
                "hmqk,khv->hmqv",
                raised.astype(jnp.bfloat16),
                value_step,
                preferred_element_type=jnp.float32,
            )
            return (new_max, run_total, run_acc)

        def unchanged(current):
            return current

        return (lax.cond(key_start <= sp_start, compute, unchanged, running_state), None)

    carry, _ = lax.scan(
        one_step, carry, (jnp.arange(step_count, dtype=jnp.int32), key_steps, value_steps)
    )
    run_max, run_total, run_acc = carry
    lambda_heads = jnp.take(diff_lambda, head_ids, axis=0)
    diff_raw = (
        run_acc[:, 0] / run_total[:, 0, :, None]
        - lambda_heads[:, None, None] * run_acc[:, 1] / run_total[:, 1, :, None]
    )
    attend_out = rms_scale(jnp.transpose(diff_raw, (1, 0, 2)), mix_gain).astype(jnp.bfloat16)
    low_rank = jnp.dot(normed_rows, decay_down, preferred_element_type=jnp.float32).astype(
        jnp.bfloat16
    )
    up_columns = jnp.take(decay_up, head_ids, axis=1)
    pre_act = jnp.einsum(
        "tr,rhk->thk", low_rank, up_columns, preferred_element_type=jnp.float32
    ) + jnp.take(decay_bias, head_ids, axis=0)
    retain_heads = jnp.take(log_retain[0], head_ids, axis=1)
    log_decay = jax.nn.log_sigmoid(pre_act) / decay_tau + retain_heads[:, :, None]
    local_state, local_decay, inside_block, reaching_keys = linear_blocks(
        q_lin.astype(jnp.float32) * HDK ** (-0.5),
        k_lin.astype(jnp.float32),
        v_lin.astype(jnp.float32),
        log_decay,
    )

    def chain(earlier, later):
        return (earlier[0] + later[0], earlier[1] * jnp.exp(later[0])[:, :, None] + later[1])

    zero_chain = (jnp.zeros_like(local_decay), jnp.zeros_like(local_state))
    prior_decay, prior_state = entering((local_decay, local_state), "sp", chain, zero_chain)
    start_state = lax.all_to_all(init_state, "fs", split_axis=0, concat_axis=1, tiled=True)[0]
    incoming_state = start_state * jnp.exp(prior_decay)[:, :, None] + prior_state
    linear_raw = inside_block + jnp.einsum(
        "jwo,wos->jws", reaching_keys, incoming_state, precision=lax.Precision.HIGHEST
    )
    linear_out = rms_scale(linear_raw, state_gain).astype(jnp.bfloat16)
    out_cols = output_attend.shape[1]
    per_device = MIXER_HEADS // (fs_size * tp_size)
    attend_view = output_attend.reshape(fs_size, tp_size, per_device * DV_A, out_cols)
    linear_view = output_linear.reshape(fs_size, tp_size, per_device * HDV, out_cols)
    blank_out = jnp.zeros((tok_rows, out_cols), jnp.float32)
    running_out = blank_out
    seg_attend = lax.all_gather(attend_out, "tp", axis=1, tiled=True)
    seg_linear = lax.all_gather(linear_out, "tp", axis=1, tiled=True)
    shard_count = seg_attend.shape[1] // head_count
    first_rank = jnp.int32(0) // head_count
    for shard_step in range(shard_count):
        owner_rank = first_rank + shard_step
        rows_attend = lax.dynamic_index_in_dim(attend_view, owner_rank, 1, keepdims=False).reshape(
            -1, out_cols
        )
        rows_linear = lax.dynamic_index_in_dim(linear_view, owner_rank, 1, keepdims=False).reshape(
            -1, out_cols
        )
        part_attend = seg_attend[
            :, shard_step * head_count : (shard_step + 1) * head_count
        ].reshape(tok_rows, -1)
        part_linear = seg_linear[
            :, shard_step * head_count : (shard_step + 1) * head_count
        ].reshape(tok_rows, -1)
        running_out = running_out + jnp.dot(
            part_attend, rows_attend, preferred_element_type=jnp.float32
        )
        running_out = running_out + jnp.dot(
            part_linear, rows_linear, preferred_element_type=jnp.float32
        )
    return running_out.astype(jnp.bfloat16).reshape(1, tok_rows, out_cols)


MESH = pl.DeviceIdType.MESH


def group_barrier(n, fs_size, tp_size):
    z, f, c = lax.axis_index("sp"), lax.axis_index("fs"), lax.axis_index("tp")
    barrier = pltpu.get_barrier_semaphore()
    total = n * fs_size * tp_size
    me = (z * fs_size + f) * tp_size + c
    for k in range(1, total):
        other = lax.rem(me + k, total)
        oz = other // (fs_size * tp_size)
        of = lax.rem(other // tp_size, fs_size)
        oc = lax.rem(other, tp_size)
        pl.semaphore_signal(
            barrier, inc=1, device_id={"sp": oz, "fs": of, "tp": oc}, device_id_type=MESH
        )
    pl.semaphore_wait(barrier, total - 1)


def remote(src, dst, send, recv, **where):
    return pltpu.make_async_remote_copy(
        src_ref=src,
        dst_ref=dst,
        send_sem=send,
        recv_sem=recv,
        device_id=where,
        device_id_type=MESH,
    )


def gather_kernel(
    n,
    fs_size,
    tp_size,
    hpd,
    tok_ref,
    ret_ref,
    gain_ref,
    down_ref,
    wq_ref,
    wk_ref,
    wv_ref,
    lq_ref,
    lk_ref,
    lv_ref,
    proj_ref,
    low_ref,
    rout_ref,
    seq_ref,
    relay_ref,
    raw_ref,
    raw_v_ref,
    w_ref,
    recv_a,
    recv_b,
    recv_l,
    recv_r,
    send_x,
    send_row,
    send_rl,
    send_up,
    send_down,
    send_sib,
    send_r,
    loc,
    wsem,
):
    z, f, c = lax.axis_index("sp"), lax.axis_index("fs"), lax.axis_index("tp")
    rows, width = tok_ref.shape
    half = rows // tp_size
    pieces = recv_l.shape[0]
    prow = half // pieces
    loads = [
        pltpu.make_async_copy(ref, raw_ref.at[i], wsem.at[i])
        for i, ref in enumerate((wq_ref, wk_ref, wv_ref, lq_ref, lk_ref))
    ]
    loads.append(pltpu.make_async_copy(lv_ref, raw_v_ref, wsem.at[5]))
    for load in loads:
        load.start()
    group_barrier(n, fs_size, tp_size)
    s = z // hpd
    own = s == f
    strange = jnp.logical_not(own)

    def nearest(seq):
        return jnp.minimum(jnp.maximum(z, seq * hpd), seq * hpd + hpd - 1)

    def piece(zc, core, p):
        return seq_ref.at[pl.ds(pl.multiple_of(zc * rows + core * half + p * prow, prow), prow)]

    lo = f * hpd
    rsends = []
    for j in range(hpd):
        for k in range(fs_size):
            x = lax.rem(f + k, fs_size)
            there = lo + j
            copy = remote(
                ret_ref,
                rout_ref.at[z],
                send_r.at[j * fs_size + k],
                recv_r.at[z],
                sp=there,
                fs=x,
            )
            go = jnp.logical_not((there == z) & (x == f))
            pl.when(go)(copy.start)
            rsends.append((go, copy))
    sends = []
    for p in range(pieces):
        mine = tok_ref.at[pl.ds(pl.multiple_of(c * half + p * prow, prow), prow)]
        there = relay_ref.at[pl.ds(p * prow, prow)]
        over = remote(mine, piece(z, c, p), send_x.at[p], recv_a.at[z, p], fs=1 - f)
        pl.when(own)(over.start)
        lent = remote(mine, there, send_x.at[p], recv_l.at[p], fs=1 - f)
        pl.when(strange)(lent.start)
        along = remote(mine, piece(z, c, p), send_row.at[p], recv_a.at[z, p], sp=nearest(f))
        pl.when(strange)(along.start)
        sends += [(own, over), (strange, lent), (strange, along)]
    full = pl.ds(pl.multiple_of(z * rows, rows), rows)
    local = pltpu.make_async_copy(tok_ref, seq_ref.at[full], loc.at[0])
    local_r = pltpu.make_async_copy(ret_ref, rout_ref.at[z], loc.at[1])
    pl.when(own)(local.start)
    pl.when(own)(local_r.start)

    slot = lax.rem(z, hpd)
    step = 128

    def pick(source, target_cols, parts, part):
        span = step * parts * hpd
        sel = (
            lax.broadcasted_iota(jnp.int32, (step, span), 1)
            == (lax.broadcasted_iota(jnp.int32, (step, span), 0) * parts + part) * hpd + slot
        ).astype(jnp.bfloat16)

        def one(i, carry):
            block = source[pl.ds(pl.multiple_of(i * span, span), span), :]
            w_ref[pl.ds(pl.multiple_of(i * step, step), step), target_cols] = jnp.dot(
                sel, block, preferred_element_type=jnp.float32
            ).astype(jnp.bfloat16)
            return carry

        lax.fori_loop(0, width // step, one, 0)

    def pick_all(first, last):
        for i in range(first, min(last, 5)):
            loads[i].wait()
            pick(raw_ref.at[i], slice(i * 128, (i + 1) * 128), 1, 0)
        if last > 5:
            loads[5].wait()
            for part in range(2):
                pick(raw_v_ref, slice((5 + part) * 128, (6 + part) * 128), 2, part)

    mlo = s * hpd
    mhi = mlo + hpd - 1

    def relay(p):
        held = relay_ref.at[pl.ds(p * prow, prow)]
        lent = remote(held, piece(z, c, p), send_rl.at[p], recv_l.at[p], sp=nearest(1 - f))
        pl.when(own)(lent.wait_recv)
        along = remote(held, piece(z, c, p), send_rl.at[p], recv_a.at[z, p], sp=nearest(1 - f))
        pl.when(own)(along.start)
        sends.append((own, along))

    def handle(zc, p, act, away):
        block = piece(zc, c, p)
        arrive = remote(block, block, send_sib.at[zc, p], recv_a.at[zc, p], tp=1 - c)
        pl.when(away)(arrive.wait_recv)
        up = remote(
            block, block, send_up.at[zc, p], recv_a.at[zc, p], sp=jnp.minimum(z + 1, n - 1)
        )
        go_up = act & (zc <= z) & (z + 1 <= mhi)
        pl.when(go_up)(up.start)
        down = remote(
            block, block, send_down.at[zc, p], recv_a.at[zc, p], sp=jnp.maximum(z - 1, 0)
        )
        go_down = act & (zc >= z) & (z - 1 >= mlo)
        pl.when(go_down)(down.start)
        sib = remote(block, block, send_sib.at[zc, p], recv_b.at[zc, p], tp=1 - c)
        pl.when(away)(sib.start)
        sends.extend([(go_up, up), (go_down, down), (away, sib)])

    def early(p):
        relay(p)
        handle(z, p, z >= 0, strange)

    def rest(p):
        for k in range(n):
            zc = jnp.where(2 * z < n, n - 1 - k, k)
            handle(zc, p, zc != z, zc != z)

    def finish(p):
        for zc in range(n):
            away = jnp.logical_not((zc == z) & own)
            other = piece(zc, 1 - c, p)
            came = remote(other, other, send_sib.at[zc, p], recv_b.at[zc, p], tp=1 - c)
            pl.when(away)(came.wait_recv)
        spots = [
            slice(zc * rows + core * half + p * prow, zc * rows + core * half + (p + 1) * prow)
            for zc in range(n)
            for core in range(tp_size)
        ]
        x = jnp.concatenate([seq_ref[spot, :] for spot in spots], axis=0).astype(jnp.float32)
        scale = lax.rsqrt(jnp.mean(x * x, axis=-1, keepdims=True) + norm_eps)
        normed = (x * scale * gain_ref[...]).astype(jnp.bfloat16)
        made = jnp.dot(normed, w_ref[...], preferred_element_type=jnp.float32).astype(jnp.bfloat16)
        low = lax.dot_general(
            normed, down_ref[...], (((1,), (1,)), ((), ())), preferred_element_type=jnp.float32
        ).astype(jnp.bfloat16)
        for i, spot in enumerate(spots):
            proj_ref[spot, :] = made[i * prow : (i + 1) * prow]
            low_ref[spot, :] = low[i * prow : (i + 1) * prow]

    pl.when(own)(local.wait)
    early(0)
    for p in range(pieces):
        if p + 1 < pieces:
            early(p + 1)
        rest(p)
        if p == 0:
            pick_all(0, 3)
        if p == min(1, pieces - 1):
            pick_all(3, 6)
        if p > 0:
            finish(p - 1)
    finish(pieces - 1)
    pl.when(own)(local_r.wait)
    for go, copy in rsends + sends:
        pl.when(go)(copy.wait_send)
    for zc in range(n):
        away = jnp.logical_not((zc == z) & own)
        came_r = remote(ret_ref, rout_ref.at[zc], send_r.at[0], recv_r.at[zc], tp=1 - c)
        pl.when(away)(came_r.wait_recv)


def interleaved(weight):
    width, hpd, columns = weight.shape
    parts = columns // 128
    return jnp.swapaxes(weight.reshape(width, hpd, parts, 128), 1, 2).reshape(-1, 128)


def gather_positions(tokens, retain, gain, down, weights, n, fs_size, tp_size, hpd):
    rows, width = tokens.shape
    dma = pltpu.SemaphoreType.DMA
    flat = [interleaved(weight) for weight in weights]
    pieces = max(1, rows // tp_size // 16)
    columns = sum(weight.shape[2] for weight in weights)
    vmem = pl.BlockSpec(memory_space=pltpu.VMEM)
    anywhere = pl.BlockSpec(memory_space=pl.ANY)
    return pl.pallas_call(
        functools.partial(gather_kernel, n, fs_size, tp_size, hpd),
        out_shape=(
            jax.ShapeDtypeStruct((n * rows, columns), jnp.bfloat16),
            jax.ShapeDtypeStruct((n * rows, down.shape[0]), jnp.bfloat16),
            jax.ShapeDtypeStruct((n,) + retain.shape, retain.dtype),
        ),
        in_specs=[vmem] * 4 + [anywhere] * 6,
        out_specs=(vmem, vmem, anywhere),
        scratch_shapes=[
            pltpu.VMEM((n * rows, width), jnp.bfloat16),
            pltpu.VMEM((rows // tp_size, width), jnp.bfloat16),
            pltpu.VMEM((5,) + flat[0].shape, jnp.bfloat16),
            pltpu.VMEM(flat[5].shape, jnp.bfloat16),
            pltpu.VMEM((width, columns), jnp.bfloat16),
            dma((n, pieces)),
            dma((n, pieces)),
            dma((pieces,)),
            dma((n,)),
            dma((pieces,)),
            dma((pieces,)),
            dma((pieces,)),
            dma((n, pieces)),
            dma((n, pieces)),
            dma((n, pieces)),
            dma((hpd * fs_size,)),
            dma((2,)),
            dma((6,)),
        ],
        compiler_params=pltpu.CompilerParams(collective_id=0, has_side_effects=True),
    )(tokens, retain, gain, down, *flat)


def mix_kernel(
    hpd,
    tp_size,
    lam_ref,
    proj_ref,
    low_ref,
    ret_ref,
    up_ref,
    bias_ref,
    qg_ref,
    kg_ref,
    mg_ref,
    sg_ref,
    init_ref,
    out_ref,
):
    z, f, c = lax.axis_index("sp"), lax.axis_index("fs"), lax.axis_index("tp")
    slot = lax.rem(z, hpd)
    seq = z // hpd
    head = (f * tp_size + c) * hpd + slot
    f32, bf16 = jnp.float32, jnp.bfloat16
    length = proj_ref.shape[0]
    lane = lax.broadcasted_iota(jnp.int32, (1, 2 * HD_A), 1)
    first = lane < HD_A

    def unit(cols, gain):
        x = proj_ref[:, cols].astype(f32)
        sq = x * x
        m0 = jnp.sum(jnp.where(first, sq, 0.0), axis=-1, keepdims=True) / HD_A
        m1 = jnp.sum(jnp.where(first, 0.0, sq), axis=-1, keepdims=True) / HD_A
        r = jnp.where(first, lax.rsqrt(m0 + norm_eps), lax.rsqrt(m1 + norm_eps))
        return (x * r * gain).astype(bf16)

    q_gain = jnp.concatenate([qg_ref[...], qg_ref[...]], axis=1)
    k_pair = kg_ref[pl.ds(head, 1)]
    k_gain = jnp.concatenate([k_pair[:, 0], k_pair[:, 1]], axis=1)
    q_unit = unit(slice(0, 128), q_gain)
    k_unit = unit(slice(128, 256), k_gain)
    zero = jnp.zeros_like(q_unit)
    q_maps = (jnp.where(first, q_unit, zero), jnp.where(first, zero, q_unit))
    tile = 2 * BLK
    key_b = lax.broadcasted_iota(jnp.int32, (tile, tile), 1) // BLK
    query_b = lax.broadcasted_iota(jnp.int32, (tile, tile), 0) // BLK
    allowed = query_b >= key_b
    lam = lam_ref[head]
    for i in range(length // tile):
        at = slice(i * tile, (i + 1) * tile)
        parts = []
        for m in range(2):
            q = q_maps[m][at]
            diag = (
                lax.dot_general(
                    q, k_unit[at], (((1,), (1,)), ((), ())), preferred_element_type=f32
                )
                * HD_A ** (-0.5)
            )
            diag = jnp.where(allowed, diag, -jnp.inf)
            top = jnp.max(diag, axis=-1, keepdims=True)
            if i > 0:
                past = (
                    lax.dot_general(
                        q,
                        k_unit[: i * tile],
                        (((1,), (1,)), ((), ())),
                        preferred_element_type=f32,
                    )
                    * HD_A ** (-0.5)
                )
                top = jnp.maximum(top, jnp.max(past, axis=-1, keepdims=True))
            raised = jnp.exp(diag - top)
            total = jnp.sum(raised, axis=-1, keepdims=True)
            acc = jnp.dot(raised.astype(bf16), proj_ref[at, 256:384], preferred_element_type=f32)
            if i > 0:
                raised = jnp.exp(past - top)
                total = total + jnp.sum(raised, axis=-1, keepdims=True)
                acc = acc + jnp.dot(
                    raised.astype(bf16), proj_ref[: i * tile, 256:384], preferred_element_type=f32
                )
            parts.append(acc / total)
        diff = parts[0] - lam * parts[1]
        scale = lax.rsqrt(jnp.mean(diff * diff, axis=-1, keepdims=True) + norm_eps)
        out_ref[at, :DV_A] = (diff * scale * mg_ref[...]).astype(bf16)

    up = up_ref[:, pl.ds(pl.multiple_of(head * HDK, HDK), HDK)]
    bias = bias_ref[pl.ds(head, 1), :]
    r64 = lax.broadcasted_iota(jnp.int32, (BLK, BLK), 0)
    c64 = lax.broadcasted_iota(jnp.int32, (BLK, BLK), 1)
    causal = r64 >= c64
    lower = causal.astype(f32)
    eye_k = lax.broadcasted_iota(jnp.int32, (HDK, HDK), 0) == lax.broadcasted_iota(
        jnp.int32, (HDK, HDK), 1
    )
    pre = jnp.dot(low_ref[...], up, preferred_element_type=f32) + bias
    log_sig = jnp.minimum(pre, 0.0) - jnp.log1p(jnp.exp(-jnp.abs(pre)))
    log_sig = log_sig / decay_tau
    state = init_ref[pl.ds(seq, 1), pl.ds(slot, 1)].reshape(HDK, HDV)
    rows = ret_ref.shape[2]
    per = rows // BLK
    for b in range(length // BLK):
        at = slice(b * BLK, (b + 1) * BLK)
        ret = ret_ref[b // per, pl.ds(head, 1), :][:, (b % per) * BLK : (b % per + 1) * BLK]
        column = jnp.sum(jnp.where(r64 == c64, ret, 0.0), axis=-1, keepdims=True)
        logs = log_sig[at] + column
        run = jnp.dot(
            lower, logs, preferred_element_type=f32, precision=lax.Precision.HIGHEST
        )
        pivot = run[BLK // 2 : BLK // 2 + 1]
        last = run[BLK - 1 : BLK]
        q = proj_ref[at, 384:512].astype(f32) * HDK ** (-0.5)
        k = proj_ref[at, 512:640].astype(f32)
        v = proj_ref[at, 640:896]
        qs = (q * jnp.exp(run - pivot)).astype(bf16)
        ks = (k * jnp.exp(pivot - run)).astype(bf16)
        inner = lax.dot_general(qs, ks, (((1,), (1,)), ((), ())), preferred_element_type=f32)
        inner = jnp.where(causal, inner, 0.0).astype(bf16)
        raw = jnp.dot(inner, v, preferred_element_type=f32) + jnp.dot(
            (q * jnp.exp(run)).astype(bf16), state.astype(bf16), preferred_element_type=f32
        )
        faded = (k * jnp.exp(last - run)).astype(bf16)
        keep = jnp.sum(jnp.where(eye_k, jnp.exp(last), 0.0), axis=-1, keepdims=True)
        state = state * keep + lax.dot_general(
            faded, v, (((0,), (0,)), ((), ())), preferred_element_type=f32
        )
        scale = lax.rsqrt(jnp.mean(raw * raw, axis=-1, keepdims=True) + norm_eps)
        out_ref[at, DV_A:] = (raw * scale * sg_ref[...]).astype(bf16)


def exchange_kernel(
    n,
    fs_size,
    tp_size,
    hpd,
    mix_ref,
    out_ref,
    stage,
    recv_row,
    recv_x,
    recv_s,
    send_row,
    send_x,
    send_s,
    loc,
):
    z, f, c = lax.axis_index("sp"), lax.axis_index("fs"), lax.axis_index("tp")
    rows = out_ref.shape[1]
    group_barrier(n, fs_size, tp_size)
    s = z // hpd
    keep = s == f
    cross = jnp.logical_not(keep)

    def head(x, core, zs):
        return (x * tp_size + core) * hpd + lax.rem(zs, hpd)

    def chunk(zt):
        return mix_ref.at[pl.ds(pl.multiple_of(zt * rows, rows), rows)]

    my_head = head(f, c, z)
    waits = []
    for k in range(1, n):
        zt = lax.rem(z + k, n)
        kept = remote(chunk(zt), out_ref.at[my_head], send_row.at[k], recv_row.at[z], sp=zt)
        moved = remote(chunk(zt), stage.at[z], send_row.at[k], recv_row.at[z], sp=zt)
        pl.when(keep)(kept.start)
        pl.when(cross)(moved.start)
        waits.append((None, kept))
    local = pltpu.make_async_copy(chunk(z), out_ref.at[my_head], loc)
    pl.when(keep)(local.start)
    sib0 = remote(chunk(z), out_ref.at[my_head], send_s.at[my_head], recv_s.at[my_head], tp=1 - c)
    pl.when(keep)(sib0.start)
    waits.append((keep, sib0))
    x0 = remote(chunk(z), out_ref.at[my_head], send_x.at[0], recv_x.at[my_head], fs=s)
    pl.when(cross)(x0.start)
    waits.append((cross, x0))
    for k in range(1, n):
        zs = lax.rem(z + k, n)
        sq = zs // hpd
        hd = head(f, c, zs)
        final = sq == f
        onward = jnp.logical_not(final)
        landed = remote(stage.at[zs], stage.at[zs], send_x.at[k], recv_row.at[zs], tp=1 - c)
        landed.wait_recv()
        sib = remote(out_ref.at[hd], out_ref.at[hd], send_s.at[hd], recv_s.at[hd], tp=1 - c)
        pl.when(final)(sib.start)
        waits.append((final, sib))
        xs = remote(stage.at[zs], out_ref.at[hd], send_x.at[k], recv_x.at[hd], fs=sq)
        pl.when(onward)(xs.start)
        waits.append((onward, xs))
    for k in range(1, fs_size):
        x = lax.rem(f + k, fs_size)
        for j in range(hpd):
            hd = head(x, c, j)
            block = out_ref.at[hd]
            came = remote(block, block, send_s.at[hd], recv_x.at[hd], tp=1 - c)
            came.wait_recv()
            sib = remote(block, block, send_s.at[hd], recv_s.at[hd], tp=1 - c)
            sib.start()
            waits.append((None, sib))
    for x in range(fs_size):
        for j in range(hpd):
            hd = head(x, 1 - c, j)
            block = out_ref.at[hd]
            remote(block, block, send_s.at[hd], recv_s.at[hd], tp=1 - c).wait_recv()
    pl.when(keep)(local.wait)
    for go, copy in waits:
        if go is None:
            copy.wait_send()
        else:
            pl.when(go)(copy.wait_send)


def exchange_heads(mixed, n, fs_size, tp_size, hpd):
    rows, width = mixed.shape[0] // n, mixed.shape[1]
    heads = fs_size * tp_size * hpd
    dma = pltpu.SemaphoreType.DMA
    return pl.pallas_call(
        functools.partial(exchange_kernel, n, fs_size, tp_size, hpd),
        out_shape=jax.ShapeDtypeStruct((heads, rows, width), mixed.dtype),
        in_specs=[pl.BlockSpec(memory_space=pltpu.VMEM)],
        out_specs=pl.BlockSpec(memory_space=pl.ANY),
        scratch_shapes=[
            pltpu.VMEM((n, rows, width), mixed.dtype),
            dma((n,)),
            dma((heads,)),
            dma((heads,)),
            dma((n,)),
            dma((n,)),
            dma((heads,)),
            dma,
        ],
        compiler_params=pltpu.CompilerParams(collective_id=1, has_side_effects=True),
    )(mixed)


def pair_body(
    tokens,
    norm_gain,
    query_attend,
    key_attend,
    value_attend,
    query_linear,
    key_linear,
    value_linear,
    decay_down,
    decay_up,
    decay_bias,
    log_retain,
    query_gain,
    key_gain,
    diff_lambda,
    mix_gain,
    state_gain,
    init_state,
    output_attend,
    output_linear,
):
    n, fs_size, tp_size = lax.axis_size("sp"), lax.axis_size("fs"), lax.axis_size("tp")
    hpd = query_attend.shape[1]
    weights = (query_attend, key_attend, value_attend, query_linear, key_linear, value_linear)
    projected, low_rank, retained = gather_positions(
        tokens[0],
        jnp.transpose(log_retain[0]),
        norm_gain[None],
        jnp.transpose(decay_down),
        weights,
        n,
        fs_size,
        tp_size,
        hpd,
    )
    vmem = pl.BlockSpec(memory_space=pltpu.VMEM)
    mixed = pl.pallas_call(
        functools.partial(mix_kernel, hpd, tp_size),
        out_shape=jax.ShapeDtypeStruct((projected.shape[0], DV_A + HDV), jnp.bfloat16),
        in_specs=[pl.BlockSpec(memory_space=pltpu.SMEM)] + [vmem] * 10,
        out_specs=vmem,
    )(
        diff_lambda,
        projected,
        low_rank,
        retained,
        decay_up.reshape(decay_up.shape[0], -1),
        decay_bias,
        query_gain[None],
        key_gain,
        mix_gain[None],
        state_gain[None],
        init_state,
    )
    arrived = exchange_heads(mixed, n, fs_size, tp_size, hpd)
    heads = arrived.shape[0]
    out = jnp.einsum(
        "htw,hwo->to",
        arrived[:, :, :DV_A],
        output_attend.reshape(heads, DV_A, -1),
        preferred_element_type=jnp.float32,
    ) + jnp.einsum(
        "htw,hwo->to",
        arrived[:, :, DV_A:],
        output_linear.reshape(heads, HDV, -1),
        preferred_element_type=jnp.float32,
    )
    return out.astype(jnp.bfloat16)[None]


def solution(mesh):
    in_specs = (
        P(("grp", "fs"), "sp", None),
        P(),
        P(None, ("fs", "tp"), None),
        P(None, ("fs", "tp"), None),
        P(None, ("fs", "tp"), None),
        P(None, ("fs", "tp"), None),
        P(None, ("fs", "tp"), None),
        P(None, ("fs", "tp"), None),
        P(),
        P(),
        P(),
        P(("grp", "fs"), "sp", None),
        P(),
        P(),
        P(),
        P(),
        P(),
        P("grp", ("fs", "tp"), None, None),
        P(None, "tp"),
        P(None, "tp"),
    )
    out_specs = P(("grp", "fs"), "sp", "tp")
    fs_size, tp_size, sp_size = mesh.shape["fs"], mesh.shape["tp"], mesh.shape["sp"]
    pairs = MIXER_HEADS // tp_size
    chosen = pair_body if pairs == sp_size and tp_size == 2 and fs_size == 2 else body
    return jax.shard_map(chosen, mesh=mesh, in_specs=in_specs, out_specs=out_specs, check_vma=False)
```

```python
import functools

import jax
import jax.numpy as jnp
from jax import lax
from jax.experimental import pallas as pl
from jax.experimental.pallas import tpu as pltpu
from jax.sharding import PartitionSpec as P

MIXER_HEADS = 8
HD_A = 64
DV_A = 128
HDK = 128
HDV = 256
BLK = 64


norm_eps = 1e-06
decay_tau = 16.0


def entering(part, axis, combine, identity):
    place = lax.axis_index(axis)
    gathered = jax.tree.map(lambda a: lax.all_gather(a, axis), part)
    state = jax.tree.map(lambda a, e: jnp.zeros_like(a) + jnp.asarray(e, a.dtype), part, identity)

    def one(hop, state):
        return combine(
            state, jax.tree.map(lambda a: lax.dynamic_index_in_dim(a, hop, 0, False), gathered)
        )

    return lax.fori_loop(0, place, one, state)


def rms_scale(values, gain):
    widened = values.astype(jnp.float32)
    return (
        widened * lax.rsqrt(jnp.mean(widened * widened, axis=-1, keepdims=True) + norm_eps) * gain
    )


def head_order(fs_size, tp_size, tp_rank):
    per_device = MIXER_HEADS // (fs_size * tp_size)
    owners = jnp.arange(fs_size, dtype=jnp.int32)[:, None] * tp_size + tp_rank
    return (owners * per_device + jnp.arange(per_device, dtype=jnp.int32)[None, :]).reshape(-1)


def linear_blocks(queries, keys_in, values_in, log_decay):
    tok_rows, head_count, key_dim = queries.shape
    value_dim = values_in.shape[-1]
    block_count = tok_rows // BLK
    highest_precision = lax.Precision.HIGHEST

    def split_blocks(source):
        return source.reshape(block_count, BLK, head_count, source.shape[-1])

    causal = (
        jnp.arange(BLK, dtype=jnp.int32)[:, None] >= jnp.arange(BLK, dtype=jnp.int32)[None, :]
    )[None]

    def advance(carry, inputs_now):
        recurrent_state, offset = carry
        question_patch_lines, block_k, value_tile_width, block_log = inputs_now
        running_state = jnp.cumsum(block_log, axis=0)
        pivot = running_state[BLK // 2]
        q_scaled = question_patch_lines * jnp.exp(running_state - pivot[None])
        k_scaled = block_k * jnp.exp(pivot[None] - running_state)
        scores = jnp.einsum("thk,shk->hts", q_scaled, k_scaled, precision=highest_precision)
        scores = jnp.where(causal, scores, 0.0)
        inside_block = jnp.einsum(
            "hts,shv->thv", scores, value_tile_width, precision=highest_precision
        )
        inside_block = inside_block + jnp.einsum(
            "jwo,wos->jws",
            question_patch_lines * jnp.exp(running_state),
            recurrent_state,
            precision=highest_precision,
        )
        final_state = running_state[-1]
        faded_memory_matrix = block_k * jnp.exp(final_state[None] - running_state)
        recurrent_state = recurrent_state * jnp.exp(final_state)[:, :, None] + jnp.einsum(
            "zcb,zcw->cbw", faded_memory_matrix, value_tile_width, precision=highest_precision
        )
        reaching_keys = question_patch_lines * jnp.exp(offset[None] + running_state)
        return ((recurrent_state, offset + final_state), (inside_block, reaching_keys))

    start_carry = (
        jnp.zeros((head_count, key_dim, value_dim), jnp.float32),
        jnp.zeros((head_count, key_dim), jnp.float32),
    )
    (recurrent_state, total_decay), (inside_block, reaching_keys) = lax.scan(
        advance,
        start_carry,
        (
            split_blocks(queries),
            split_blocks(keys_in),
            split_blocks(values_in),
            split_blocks(log_decay),
        ),
    )
    return (
        recurrent_state,
        total_decay,
        inside_block.reshape(tok_rows, head_count, value_dim),
        reaching_keys.reshape(tok_rows, head_count, key_dim),
    )


def body(
    tokens,
    norm_gain,
    query_attend,
    key_attend,
    value_attend,
    query_linear,
    key_linear,
    value_linear,
    decay_down,
    decay_up,
    decay_bias,
    log_retain,
    query_gain,
    key_gain,
    diff_lambda,
    mix_gain,
    state_gain,
    init_state,
    output_attend,
    output_linear,
):
    fs_size = lax.axis_size("fs")
    tp_size = lax.axis_size("tp")
    tp_rank = lax.axis_index("tp")
    tok_rows = tokens.shape[1]
    normed = rms_scale(tokens, norm_gain).astype(jnp.bfloat16)
    normed_rows = normed[0]
    local_weights = (query_attend, key_attend, value_attend, query_linear, key_linear, value_linear)
    widths = [weight.shape[1] * weight.shape[2] for weight in local_weights]
    packed = jnp.concatenate(
        [weight.reshape(weight.shape[0], -1) for weight in local_weights], axis=1
    )
    computed = jnp.einsum(
        "std,dp->stp",
        lax.all_gather(normed, "fs", axis=0, tiled=True),
        packed,
        preferred_element_type=jnp.float32,
    ).astype(jnp.bfloat16)
    arrived = lax.all_to_all(computed, "fs", split_axis=0, concat_axis=2, tiled=True).reshape(
        tok_rows, fs_size, -1
    )
    sections = []
    column_at = 0
    for weight, width_now in zip(local_weights, widths):
        section = arrived[:, :, column_at : column_at + width_now]
        sections.append(section.reshape(tok_rows, fs_size * weight.shape[1], weight.shape[2]))
        column_at = column_at + width_now
    projected = tuple(sections)
    q_pair, k_pair, v_attend, q_lin, k_lin, v_lin = projected
    head_ids = head_order(fs_size, tp_size, tp_rank)
    head_count = head_ids.shape[0]
    q_unit = rms_scale(q_pair.reshape(tok_rows, head_count, 2, HD_A), query_gain).astype(
        jnp.bfloat16
    )
    k_unit = rms_scale(
        k_pair.reshape(tok_rows, head_count, 2, HD_A), jnp.take(key_gain, head_ids, axis=0)
    ).astype(jnp.bfloat16)
    sp_start = lax.axis_index("sp") * tok_rows
    query_block = (sp_start + jnp.arange(tok_rows, dtype=jnp.int32)) // BLK
    score_scale = HD_A ** (-0.5)
    blank_attend = (
        jnp.full((head_count, 2, tok_rows), -jnp.inf, jnp.float32),
        jnp.zeros((head_count, 2, tok_rows), jnp.float32),
        jnp.zeros((head_count, 2, tok_rows, DV_A), jnp.float32),
    )
    carry = blank_attend
    seg_keys = lax.all_gather(k_unit, "sp", axis=0, tiled=True)
    seg_values = lax.all_gather(v_attend, "sp", axis=0, tiled=True)
    span = seg_keys.shape[0]
    stride_token_lines = 2 * tok_rows
    step_count = span // stride_token_lines
    key_steps = seg_keys.reshape(step_count, stride_token_lines, head_count, 2, HD_A)
    value_steps = seg_values.reshape(step_count, stride_token_lines, head_count, DV_A)

    def one_step(running_state, inputs_now):
        step_index, key_step, value_step = inputs_now
        key_start = step_index * stride_token_lines

        def compute(current):
            run_max, run_total, run_acc = current
            scores = (
                jnp.einsum("qhmd,khmd->hmqk", q_unit, key_step, preferred_element_type=jnp.float32)
                * score_scale
            )
            key_block = (key_start + jnp.arange(stride_token_lines, dtype=jnp.int32)) // BLK
            allowed = query_block[:, None] >= key_block[None, :]
            scores = jnp.where(allowed, scores, -jnp.inf)
            new_max = jnp.maximum(run_max, jnp.max(scores, axis=-1))
            factor = jnp.exp(run_max - new_max)
            raised = jnp.exp(scores - new_max[..., None])
            run_total = run_total * factor + jnp.sum(raised, axis=-1)
            run_acc = run_acc * factor[..., None] + jnp.einsum(
                "hmqk,khv->hmqv",
                raised.astype(jnp.bfloat16),
                value_step,
                preferred_element_type=jnp.float32,
            )
            return (new_max, run_total, run_acc)

        def unchanged(current):
            return current

        return (lax.cond(key_start <= sp_start, compute, unchanged, running_state), None)

    carry, _ = lax.scan(
        one_step, carry, (jnp.arange(step_count, dtype=jnp.int32), key_steps, value_steps)
    )
    run_max, run_total, run_acc = carry
    lambda_heads = jnp.take(diff_lambda, head_ids, axis=0)
    diff_raw = (
        run_acc[:, 0] / run_total[:, 0, :, None]
        - lambda_heads[:, None, None] * run_acc[:, 1] / run_total[:, 1, :, None]
    )
    attend_out = rms_scale(jnp.transpose(diff_raw, (1, 0, 2)), mix_gain).astype(jnp.bfloat16)
    low_rank = jnp.dot(normed_rows, decay_down, preferred_element_type=jnp.float32).astype(
        jnp.bfloat16
    )
    up_columns = jnp.take(decay_up, head_ids, axis=1)
    pre_act = jnp.einsum(
        "tr,rhk->thk", low_rank, up_columns, preferred_element_type=jnp.float32
    ) + jnp.take(decay_bias, head_ids, axis=0)
    retain_heads = jnp.take(log_retain[0], head_ids, axis=1)
    log_decay = jax.nn.log_sigmoid(pre_act) / decay_tau + retain_heads[:, :, None]
    local_state, local_decay, inside_block, reaching_keys = linear_blocks(
        q_lin.astype(jnp.float32) * HDK ** (-0.5),
        k_lin.astype(jnp.float32),
        v_lin.astype(jnp.float32),
        log_decay,
    )

    def chain(earlier, later):
        return (earlier[0] + later[0], earlier[1] * jnp.exp(later[0])[:, :, None] + later[1])

    zero_chain = (jnp.zeros_like(local_decay), jnp.zeros_like(local_state))
    prior_decay, prior_state = entering((local_decay, local_state), "sp", chain, zero_chain)
    start_state = lax.all_to_all(init_state, "fs", split_axis=0, concat_axis=1, tiled=True)[0]
    incoming_state = start_state * jnp.exp(prior_decay)[:, :, None] + prior_state
    linear_raw = inside_block + jnp.einsum(
        "jwo,wos->jws", reaching_keys, incoming_state, precision=lax.Precision.HIGHEST
    )
    linear_out = rms_scale(linear_raw, state_gain).astype(jnp.bfloat16)
    out_cols = output_attend.shape[1]
    per_device = MIXER_HEADS // (fs_size * tp_size)
    attend_view = output_attend.reshape(fs_size, tp_size, per_device * DV_A, out_cols)
    linear_view = output_linear.reshape(fs_size, tp_size, per_device * HDV, out_cols)
    blank_out = jnp.zeros((tok_rows, out_cols), jnp.float32)
    running_out = blank_out
    seg_attend = lax.all_gather(attend_out, "tp", axis=1, tiled=True)
    seg_linear = lax.all_gather(linear_out, "tp", axis=1, tiled=True)
    shard_count = seg_attend.shape[1] // head_count
    first_rank = jnp.int32(0) // head_count
    for shard_step in range(shard_count):
        owner_rank = first_rank + shard_step
        rows_attend = lax.dynamic_index_in_dim(attend_view, owner_rank, 1, keepdims=False).reshape(
            -1, out_cols
        )
        rows_linear = lax.dynamic_index_in_dim(linear_view, owner_rank, 1, keepdims=False).reshape(
            -1, out_cols
        )
        part_attend = seg_attend[
            :, shard_step * head_count : (shard_step + 1) * head_count
        ].reshape(tok_rows, -1)
        part_linear = seg_linear[
            :, shard_step * head_count : (shard_step + 1) * head_count
        ].reshape(tok_rows, -1)
        running_out = running_out + jnp.dot(
            part_attend, rows_attend, preferred_element_type=jnp.float32
        )
        running_out = running_out + jnp.dot(
            part_linear, rows_linear, preferred_element_type=jnp.float32
        )
    return running_out.astype(jnp.bfloat16).reshape(1, tok_rows, out_cols)


MESH = pl.DeviceIdType.MESH


def group_barrier(n, fs_size, tp_size):
    z, f, c = lax.axis_index("sp"), lax.axis_index("fs"), lax.axis_index("tp")
    barrier = pltpu.get_barrier_semaphore()
    total = n * fs_size * tp_size
    me = (z * fs_size + f) * tp_size + c
    for k in range(1, total):
        other = lax.rem(me + k, total)
        oz = other // (fs_size * tp_size)
        of = lax.rem(other // tp_size, fs_size)
        oc = lax.rem(other, tp_size)
        pl.semaphore_signal(
            barrier, inc=1, device_id={"sp": oz, "fs": of, "tp": oc}, device_id_type=MESH
        )
    pl.semaphore_wait(barrier, total - 1)


def remote(src, dst, send, recv, **where):
    return pltpu.make_async_remote_copy(
        src_ref=src,
        dst_ref=dst,
        send_sem=send,
        recv_sem=recv,
        device_id=where,
        device_id_type=MESH,
    )


def gather_kernel(
    n,
    fs_size,
    tp_size,
    hpd,
    tok_ref,
    ret_ref,
    gain_ref,
    down_ref,
    wq_ref,
    wk_ref,
    wv_ref,
    lq_ref,
    lk_ref,
    lv_ref,
    proj_ref,
    low_ref,
    rout_ref,
    seq_ref,
    relay_ref,
    raw_ref,
    raw_v_ref,
    w_ref,
    recv_a,
    recv_b,
    recv_l,
    recv_r,
    send_x,
    send_row,
    send_rl,
    send_up,
    send_down,
    send_sib,
    send_r,
    loc,
    wsem,
):
    z, f, c = lax.axis_index("sp"), lax.axis_index("fs"), lax.axis_index("tp")
    rows, width = tok_ref.shape
    half = rows // tp_size
    pieces = recv_l.shape[0]
    prow = half // pieces
    loads = [
        pltpu.make_async_copy(ref, raw_ref.at[i], wsem.at[i])
        for i, ref in enumerate((wq_ref, wk_ref, wv_ref, lq_ref, lk_ref))
    ]
    loads.append(pltpu.make_async_copy(lv_ref, raw_v_ref, wsem.at[5]))
    for load in loads:
        load.start()
    group_barrier(n, fs_size, tp_size)
    s = z // hpd
    own = s == f
    strange = jnp.logical_not(own)

    def nearest(seq):
        return jnp.minimum(jnp.maximum(z, seq * hpd), seq * hpd + hpd - 1)

    def piece(zc, core, p):
        return seq_ref.at[pl.ds(pl.multiple_of(zc * rows + core * half + p * prow, prow), prow)]

    lo = f * hpd
    rsends = []
    for j in range(hpd):
        for k in range(fs_size):
            x = lax.rem(f + k, fs_size)
            there = lo + j
            copy = remote(
                ret_ref,
                rout_ref.at[z],
                send_r.at[j * fs_size + k],
                recv_r.at[z],
                sp=there,
                fs=x,
            )
            go = jnp.logical_not((there == z) & (x == f))
            pl.when(go)(copy.start)
            rsends.append((go, copy))
    sends = []
    for p in range(pieces):
        mine = tok_ref.at[pl.ds(pl.multiple_of(c * half + p * prow, prow), prow)]
        there = relay_ref.at[pl.ds(p * prow, prow)]
        over = remote(mine, piece(z, c, p), send_x.at[p], recv_a.at[z, p], fs=1 - f)
        pl.when(own)(over.start)
        lent = remote(mine, there, send_x.at[p], recv_l.at[p], fs=1 - f)
        pl.when(strange)(lent.start)
        along = remote(mine, piece(z, c, p), send_row.at[p], recv_a.at[z, p], sp=nearest(f))
        pl.when(strange)(along.start)
        sends += [(own, over), (strange, lent), (strange, along)]
    full = pl.ds(pl.multiple_of(z * rows, rows), rows)
    local = pltpu.make_async_copy(tok_ref, seq_ref.at[full], loc.at[0])
    local_r = pltpu.make_async_copy(ret_ref, rout_ref.at[z], loc.at[1])
    pl.when(own)(local.start)
    pl.when(own)(local_r.start)

    slot = lax.rem(z, hpd)
    step = 128

    def pick(sources, target_cols, parts, part):
        span = step * parts * hpd
        sel = (
            lax.broadcasted_iota(jnp.int32, (step, span), 1)
            == (lax.broadcasted_iota(jnp.int32, (step, span), 0) * parts + part) * hpd + slot
        ).astype(jnp.bfloat16)
        for i in range(width // step):
            blocks = [source[i * span : (i + 1) * span, :] for source in sources]
            block = blocks[0] if len(blocks) == 1 else jnp.concatenate(blocks, axis=1)
            w_ref[i * step : (i + 1) * step, target_cols] = jnp.dot(
                sel, block, preferred_element_type=jnp.float32
            ).astype(jnp.bfloat16)

    def pick_all(first, last):
        for i in range(first, min(last, 5), 2):
            group = range(i, min(i + 2, 5))
            for j in group:
                loads[j].wait()
            pick([raw_ref.at[j] for j in group], slice(i * 128, (group[-1] + 1) * 128), 1, 0)
        if last > 5:
            loads[5].wait()
            for part in range(2):
                pick([raw_v_ref], slice((5 + part) * 128, (6 + part) * 128), 2, part)

    mlo = s * hpd
    mhi = mlo + hpd - 1

    def relay(p):
        held = relay_ref.at[pl.ds(p * prow, prow)]
        lent = remote(held, piece(z, c, p), send_rl.at[p], recv_l.at[p], sp=nearest(1 - f))
        pl.when(own)(lent.wait_recv)
        along = remote(held, piece(z, c, p), send_rl.at[p], recv_a.at[z, p], sp=nearest(1 - f))
        pl.when(own)(along.start)
        sends.append((own, along))

    def handle(zc, p, act, away):
        block = piece(zc, c, p)
        arrive = remote(block, block, send_sib.at[zc, p], recv_a.at[zc, p], tp=1 - c)
        pl.when(away)(arrive.wait_recv)
        up = remote(
            block, block, send_up.at[zc, p], recv_a.at[zc, p], sp=jnp.minimum(z + 1, n - 1)
        )
        go_up = act & (zc <= z) & (z + 1 <= mhi)
        pl.when(go_up)(up.start)
        down = remote(
            block, block, send_down.at[zc, p], recv_a.at[zc, p], sp=jnp.maximum(z - 1, 0)
        )
        go_down = act & (zc >= z) & (z - 1 >= mlo)
        pl.when(go_down)(down.start)
        sib = remote(block, block, send_sib.at[zc, p], recv_b.at[zc, p], tp=1 - c)
        pl.when(away)(sib.start)
        sends.extend([(go_up, up), (go_down, down), (away, sib)])

    def early(p):
        relay(p)
        handle(z, p, z >= 0, strange)

    def rest(p):
        for k in range(n):
            zc = jnp.where(2 * z < n, n - 1 - k, k)
            handle(zc, p, zc != z, zc != z)

    def finish(p):
        for zc in range(n):
            away = jnp.logical_not((zc == z) & own)
            other = piece(zc, 1 - c, p)
            came = remote(other, other, send_sib.at[zc, p], recv_b.at[zc, p], tp=1 - c)
            pl.when(away)(came.wait_recv)
        spots = [
            slice(zc * rows + core * half + p * prow, zc * rows + core * half + (p + 1) * prow)
            for zc in range(n)
            for core in range(tp_size)
        ]
        x = jnp.concatenate([seq_ref[spot, :] for spot in spots], axis=0).astype(jnp.float32)
        scale = lax.rsqrt(jnp.mean(x * x, axis=-1, keepdims=True) + norm_eps)
        normed = (x * scale * gain_ref[...]).astype(jnp.bfloat16)
        made = jnp.dot(normed, w_ref[...], preferred_element_type=jnp.float32).astype(jnp.bfloat16)
        low = lax.dot_general(
            normed, down_ref[...], (((1,), (1,)), ((), ())), preferred_element_type=jnp.float32
        ).astype(jnp.bfloat16)
        for i, spot in enumerate(spots):
            proj_ref[spot, :] = made[i * prow : (i + 1) * prow]
            low_ref[spot, :] = low[i * prow : (i + 1) * prow]

    pl.when(own)(local.wait)
    early(0)
    for p in range(pieces):
        if p + 1 < pieces:
            early(p + 1)
        rest(p)
        if p == 0:
            pick_all(0, 4)
        if p == min(1, pieces - 1):
            pick_all(4, 6)
        if p > 0:
            finish(p - 1)
    finish(pieces - 1)
    pl.when(own)(local_r.wait)
    for go, copy in rsends + sends:
        pl.when(go)(copy.wait_send)
    for zc in range(n):
        away = jnp.logical_not((zc == z) & own)
        came_r = remote(ret_ref, rout_ref.at[zc], send_r.at[0], recv_r.at[zc], tp=1 - c)
        pl.when(away)(came_r.wait_recv)


def interleaved(weight):
    width, hpd, columns = weight.shape
    parts = columns // 128
    return jnp.swapaxes(weight.reshape(width, hpd, parts, 128), 1, 2).reshape(-1, 128)


def gather_positions(tokens, retain, gain, down, weights, n, fs_size, tp_size, hpd):
    rows, width = tokens.shape
    dma = pltpu.SemaphoreType.DMA
    flat = [interleaved(weight) for weight in weights]
    pieces = max(1, rows // tp_size // 16)
    columns = sum(weight.shape[2] for weight in weights)
    vmem = pl.BlockSpec(memory_space=pltpu.VMEM)
    anywhere = pl.BlockSpec(memory_space=pl.ANY)
    return pl.pallas_call(
        functools.partial(gather_kernel, n, fs_size, tp_size, hpd),
        out_shape=(
            jax.ShapeDtypeStruct((n * rows, columns), jnp.bfloat16),
            jax.ShapeDtypeStruct((n * rows, down.shape[0]), jnp.bfloat16),
            jax.ShapeDtypeStruct((n,) + retain.shape, retain.dtype),
        ),
        in_specs=[vmem] * 4 + [anywhere] * 6,
        out_specs=(vmem, vmem, anywhere),
        scratch_shapes=[
            pltpu.VMEM((n * rows, width), jnp.bfloat16),
            pltpu.VMEM((rows // tp_size, width), jnp.bfloat16),
            pltpu.VMEM((5,) + flat[0].shape, jnp.bfloat16),
            pltpu.VMEM(flat[5].shape, jnp.bfloat16),
            pltpu.VMEM((width, columns), jnp.bfloat16),
            dma((n, pieces)),
            dma((n, pieces)),
            dma((pieces,)),
            dma((n,)),
            dma((pieces,)),
            dma((pieces,)),
            dma((pieces,)),
            dma((n, pieces)),
            dma((n, pieces)),
            dma((n, pieces)),
            dma((hpd * fs_size,)),
            dma((2,)),
            dma((6,)),
        ],
        compiler_params=pltpu.CompilerParams(collective_id=0, has_side_effects=True),
    )(tokens, retain, gain, down, *flat)


def mix_kernel(
    hpd,
    tp_size,
    lam_ref,
    proj_ref,
    low_ref,
    ret_ref,
    up_ref,
    bias_ref,
    qg_ref,
    kg_ref,
    mg_ref,
    sg_ref,
    init_ref,
    out_ref,
):
    z, f, c = lax.axis_index("sp"), lax.axis_index("fs"), lax.axis_index("tp")
    slot = lax.rem(z, hpd)
    seq = z // hpd
    head = (f * tp_size + c) * hpd + slot
    f32, bf16 = jnp.float32, jnp.bfloat16
    length = proj_ref.shape[0]
    lane = lax.broadcasted_iota(jnp.int32, (1, 2 * HD_A), 1)
    first = lane < HD_A

    def unit(cols, gain):
        x = proj_ref[:, cols].astype(f32)
        sq = x * x
        m0 = jnp.sum(jnp.where(first, sq, 0.0), axis=-1, keepdims=True) / HD_A
        m1 = jnp.sum(jnp.where(first, 0.0, sq), axis=-1, keepdims=True) / HD_A
        r = jnp.where(first, lax.rsqrt(m0 + norm_eps), lax.rsqrt(m1 + norm_eps))
        return (x * r * gain).astype(bf16)

    q_gain = jnp.concatenate([qg_ref[...], qg_ref[...]], axis=1)
    k_pair = kg_ref[pl.ds(head, 1)]
    k_gain = jnp.concatenate([k_pair[:, 0], k_pair[:, 1]], axis=1)
    q_unit = unit(slice(0, 128), q_gain)
    k_unit = unit(slice(128, 256), k_gain)
    zero = jnp.zeros_like(q_unit)
    q_maps = (jnp.where(first, q_unit, zero), jnp.where(first, zero, q_unit))
    tile = 2 * BLK
    key_b = lax.broadcasted_iota(jnp.int32, (tile, tile), 1) // BLK
    query_b = lax.broadcasted_iota(jnp.int32, (tile, tile), 0) // BLK
    allowed = query_b >= key_b
    lam = lam_ref[head]
    for i in range(length // tile):
        at = slice(i * tile, (i + 1) * tile)
        parts = []
        for m in range(2):
            q = q_maps[m][at]
            diag = (
                lax.dot_general(
                    q, k_unit[at], (((1,), (1,)), ((), ())), preferred_element_type=f32
                )
                * HD_A ** (-0.5)
            )
            diag = jnp.where(allowed, diag, -jnp.inf)
            top = jnp.max(diag, axis=-1, keepdims=True)
            if i > 0:
                past = (
                    lax.dot_general(
                        q,
                        k_unit[: i * tile],
                        (((1,), (1,)), ((), ())),
                        preferred_element_type=f32,
                    )
                    * HD_A ** (-0.5)
                )
                top = jnp.maximum(top, jnp.max(past, axis=-1, keepdims=True))
            raised = jnp.exp(diag - top)
            total = jnp.sum(raised, axis=-1, keepdims=True)
            acc = jnp.dot(raised.astype(bf16), proj_ref[at, 256:384], preferred_element_type=f32)
            if i > 0:
                raised = jnp.exp(past - top)
                total = total + jnp.sum(raised, axis=-1, keepdims=True)
                acc = acc + jnp.dot(
                    raised.astype(bf16), proj_ref[: i * tile, 256:384], preferred_element_type=f32
                )
            parts.append(acc / total)
        diff = parts[0] - lam * parts[1]
        scale = lax.rsqrt(jnp.mean(diff * diff, axis=-1, keepdims=True) + norm_eps)
        out_ref[at, :DV_A] = (diff * scale * mg_ref[...]).astype(bf16)

    up = up_ref[:, pl.ds(pl.multiple_of(head * HDK, HDK), HDK)]
    bias = bias_ref[pl.ds(head, 1), :]
    r64 = lax.broadcasted_iota(jnp.int32, (BLK, BLK), 0)
    c64 = lax.broadcasted_iota(jnp.int32, (BLK, BLK), 1)
    causal = r64 >= c64
    lower = causal.astype(f32)
    eye_k = lax.broadcasted_iota(jnp.int32, (HDK, HDK), 0) == lax.broadcasted_iota(
        jnp.int32, (HDK, HDK), 1
    )
    pre = jnp.dot(low_ref[...], up, preferred_element_type=f32) + bias
    log_sig = jnp.minimum(pre, 0.0) - jnp.log1p(jnp.exp(-jnp.abs(pre)))
    log_sig = log_sig / decay_tau
    state = init_ref[pl.ds(seq, 1), pl.ds(slot, 1)].reshape(HDK, HDV)
    rows = ret_ref.shape[2]
    per = rows // BLK
    for b in range(length // BLK):
        at = slice(b * BLK, (b + 1) * BLK)
        ret = ret_ref[b // per, pl.ds(head, 1), :][:, (b % per) * BLK : (b % per + 1) * BLK]
        column = jnp.sum(jnp.where(r64 == c64, ret, 0.0), axis=-1, keepdims=True)
        logs = log_sig[at] + column
        run = jnp.dot(
            lower, logs, preferred_element_type=f32, precision=lax.Precision.HIGHEST
        )
        pivot = run[BLK // 2 : BLK // 2 + 1]
        last = run[BLK - 1 : BLK]
        q = proj_ref[at, 384:512].astype(f32) * HDK ** (-0.5)
        k = proj_ref[at, 512:640].astype(f32)
        v = proj_ref[at, 640:896]
        qs = (q * jnp.exp(run - pivot)).astype(bf16)
        ks = (k * jnp.exp(pivot - run)).astype(bf16)
        inner = lax.dot_general(qs, ks, (((1,), (1,)), ((), ())), preferred_element_type=f32)
        inner = jnp.where(causal, inner, 0.0).astype(bf16)
        raw = jnp.dot(inner, v, preferred_element_type=f32) + jnp.dot(
            (q * jnp.exp(run)).astype(bf16), state.astype(bf16), preferred_element_type=f32
        )
        faded = (k * jnp.exp(last - run)).astype(bf16)
        keep = jnp.sum(jnp.where(eye_k, jnp.exp(last), 0.0), axis=-1, keepdims=True)
        state = state * keep + lax.dot_general(
            faded, v, (((0,), (0,)), ((), ())), preferred_element_type=f32
        )
        scale = lax.rsqrt(jnp.mean(raw * raw, axis=-1, keepdims=True) + norm_eps)
        out_ref[at, DV_A:] = (raw * scale * sg_ref[...]).astype(bf16)


def exchange_kernel(
    n,
    fs_size,
    tp_size,
    hpd,
    mix_ref,
    out_ref,
    stage,
    recv_row,
    recv_x,
    recv_s,
    send_row,
    send_x,
    send_s,
    loc,
):
    z, f, c = lax.axis_index("sp"), lax.axis_index("fs"), lax.axis_index("tp")
    rows = out_ref.shape[1]
    group_barrier(n, fs_size, tp_size)
    s = z // hpd
    keep = s == f
    cross = jnp.logical_not(keep)

    def head(x, core, zs):
        return (x * tp_size + core) * hpd + lax.rem(zs, hpd)

    def chunk(zt):
        return mix_ref.at[pl.ds(pl.multiple_of(zt * rows, rows), rows)]

    my_head = head(f, c, z)
    waits = []
    for k in range(1, n):
        zt = lax.rem(z + k, n)
        kept = remote(chunk(zt), out_ref.at[my_head], send_row.at[k], recv_row.at[z], sp=zt)
        moved = remote(chunk(zt), stage.at[z], send_row.at[k], recv_row.at[z], sp=zt)
        pl.when(keep)(kept.start)
        pl.when(cross)(moved.start)
        waits.append((None, kept))
    local = pltpu.make_async_copy(chunk(z), out_ref.at[my_head], loc)
    pl.when(keep)(local.start)
    sib0 = remote(chunk(z), out_ref.at[my_head], send_s.at[my_head], recv_s.at[my_head], tp=1 - c)
    pl.when(keep)(sib0.start)
    waits.append((keep, sib0))
    x0 = remote(chunk(z), out_ref.at[my_head], send_x.at[0], recv_x.at[my_head], fs=s)
    pl.when(cross)(x0.start)
    waits.append((cross, x0))
    for k in range(1, n):
        zs = lax.rem(z + k, n)
        sq = zs // hpd
        hd = head(f, c, zs)
        final = sq == f
        onward = jnp.logical_not(final)
        landed = remote(stage.at[zs], stage.at[zs], send_x.at[k], recv_row.at[zs], tp=1 - c)
        landed.wait_recv()
        sib = remote(out_ref.at[hd], out_ref.at[hd], send_s.at[hd], recv_s.at[hd], tp=1 - c)
        pl.when(final)(sib.start)
        waits.append((final, sib))
        xs = remote(stage.at[zs], out_ref.at[hd], send_x.at[k], recv_x.at[hd], fs=sq)
        pl.when(onward)(xs.start)
        waits.append((onward, xs))
    for k in range(1, fs_size):
        x = lax.rem(f + k, fs_size)
        for j in range(hpd):
            hd = head(x, c, j)
            block = out_ref.at[hd]
            came = remote(block, block, send_s.at[hd], recv_x.at[hd], tp=1 - c)
            came.wait_recv()
            sib = remote(block, block, send_s.at[hd], recv_s.at[hd], tp=1 - c)
            sib.start()
            waits.append((None, sib))
    for x in range(fs_size):
        for j in range(hpd):
            hd = head(x, 1 - c, j)
            block = out_ref.at[hd]
            remote(block, block, send_s.at[hd], recv_s.at[hd], tp=1 - c).wait_recv()
    pl.when(keep)(local.wait)
    for go, copy in waits:
        if go is None:
            copy.wait_send()
        else:
            pl.when(go)(copy.wait_send)


def exchange_heads(mixed, n, fs_size, tp_size, hpd):
    rows, width = mixed.shape[0] // n, mixed.shape[1]
    heads = fs_size * tp_size * hpd
    dma = pltpu.SemaphoreType.DMA
    return pl.pallas_call(
        functools.partial(exchange_kernel, n, fs_size, tp_size, hpd),
        out_shape=jax.ShapeDtypeStruct((heads, rows, width), mixed.dtype),
        in_specs=[pl.BlockSpec(memory_space=pltpu.VMEM)],
        out_specs=pl.BlockSpec(memory_space=pl.ANY),
        scratch_shapes=[
            pltpu.VMEM((n, rows, width), mixed.dtype),
            dma((n,)),
            dma((heads,)),
            dma((heads,)),
            dma((n,)),
            dma((n,)),
            dma((heads,)),
            dma,
        ],
        compiler_params=pltpu.CompilerParams(collective_id=1, has_side_effects=True),
    )(mixed)


def pair_body(
    tokens,
    norm_gain,
    query_attend,
    key_attend,
    value_attend,
    query_linear,
    key_linear,
    value_linear,
    decay_down,
    decay_up,
    decay_bias,
    log_retain,
    query_gain,
    key_gain,
    diff_lambda,
    mix_gain,
    state_gain,
    init_state,
    output_attend,
    output_linear,
):
    n, fs_size, tp_size = lax.axis_size("sp"), lax.axis_size("fs"), lax.axis_size("tp")
    hpd = query_attend.shape[1]
    weights = (query_attend, key_attend, value_attend, query_linear, key_linear, value_linear)
    projected, low_rank, retained = gather_positions(
        tokens[0],
        jnp.transpose(log_retain[0]),
        norm_gain[None],
        jnp.transpose(decay_down),
        weights,
        n,
        fs_size,
        tp_size,
        hpd,
    )
    vmem = pl.BlockSpec(memory_space=pltpu.VMEM)
    mixed = pl.pallas_call(
        functools.partial(mix_kernel, hpd, tp_size),
        out_shape=jax.ShapeDtypeStruct((projected.shape[0], DV_A + HDV), jnp.bfloat16),
        in_specs=[pl.BlockSpec(memory_space=pltpu.SMEM)] + [vmem] * 10,
        out_specs=vmem,
    )(
        diff_lambda,
        projected,
        low_rank,
        retained,
        decay_up.reshape(decay_up.shape[0], -1),
        decay_bias,
        query_gain[None],
        key_gain,
        mix_gain[None],
        state_gain[None],
        init_state,
    )
    arrived = exchange_heads(mixed, n, fs_size, tp_size, hpd)
    heads = arrived.shape[0]
    out = jnp.einsum(
        "htw,hwo->to",
        arrived[:, :, :DV_A],
        output_attend.reshape(heads, DV_A, -1),
        preferred_element_type=jnp.float32,
    ) + jnp.einsum(
        "htw,hwo->to",
        arrived[:, :, DV_A:],
        output_linear.reshape(heads, HDV, -1),
        preferred_element_type=jnp.float32,
    )
    return out.astype(jnp.bfloat16)[None]


def solution(mesh):
    in_specs = (
        P(("grp", "fs"), "sp", None),
        P(),
        P(None, ("fs", "tp"), None),
        P(None, ("fs", "tp"), None),
        P(None, ("fs", "tp"), None),
        P(None, ("fs", "tp"), None),
        P(None, ("fs", "tp"), None),
        P(None, ("fs", "tp"), None),
        P(),
        P(),
        P(),
        P(("grp", "fs"), "sp", None),
        P(),
        P(),
        P(),
        P(),
        P(),
        P("grp", ("fs", "tp"), None, None),
        P(None, "tp"),
        P(None, "tp"),
    )
    out_specs = P(("grp", "fs"), "sp", "tp")
    fs_size, tp_size, sp_size = mesh.shape["fs"], mesh.shape["tp"], mesh.shape["sp"]
    pairs = MIXER_HEADS // tp_size
    chosen = pair_body if pairs == sp_size and tp_size == 2 and fs_size == 2 else body
    return jax.shard_map(chosen, mesh=mesh, in_specs=in_specs, out_specs=out_specs, check_vma=False)
```

```python
import functools

import jax
import jax.numpy as jnp
from jax import lax
from jax.experimental import pallas as pl
from jax.experimental.pallas import tpu as pltpu
from jax.sharding import PartitionSpec as P

MIXER_HEADS = 8
HD_A = 64
DV_A = 128
HDK = 128
HDV = 256
BLK = 64


norm_eps = 1e-06
decay_tau = 16.0


def entering(part, axis, combine, identity):
    place = lax.axis_index(axis)
    gathered = jax.tree.map(lambda a: lax.all_gather(a, axis), part)
    state = jax.tree.map(lambda a, e: jnp.zeros_like(a) + jnp.asarray(e, a.dtype), part, identity)

    def one(hop, state):
        return combine(
            state, jax.tree.map(lambda a: lax.dynamic_index_in_dim(a, hop, 0, False), gathered)
        )

    return lax.fori_loop(0, place, one, state)


def rms_scale(values, gain):
    widened = values.astype(jnp.float32)
    return (
        widened * lax.rsqrt(jnp.mean(widened * widened, axis=-1, keepdims=True) + norm_eps) * gain
    )


def head_order(fs_size, tp_size, tp_rank):
    per_device = MIXER_HEADS // (fs_size * tp_size)
    owners = jnp.arange(fs_size, dtype=jnp.int32)[:, None] * tp_size + tp_rank
    return (owners * per_device + jnp.arange(per_device, dtype=jnp.int32)[None, :]).reshape(-1)


def linear_blocks(queries, keys_in, values_in, log_decay):
    tok_rows, head_count, key_dim = queries.shape
    value_dim = values_in.shape[-1]
    block_count = tok_rows // BLK
    highest_precision = lax.Precision.HIGHEST

    def split_blocks(source):
        return source.reshape(block_count, BLK, head_count, source.shape[-1])

    causal = (
        jnp.arange(BLK, dtype=jnp.int32)[:, None] >= jnp.arange(BLK, dtype=jnp.int32)[None, :]
    )[None]

    def advance(carry, inputs_now):
        recurrent_state, offset = carry
        question_patch_lines, block_k, value_tile_width, block_log = inputs_now
        running_state = jnp.cumsum(block_log, axis=0)
        pivot = running_state[BLK // 2]
        q_scaled = question_patch_lines * jnp.exp(running_state - pivot[None])
        k_scaled = block_k * jnp.exp(pivot[None] - running_state)
        scores = jnp.einsum("thk,shk->hts", q_scaled, k_scaled, precision=highest_precision)
        scores = jnp.where(causal, scores, 0.0)
        inside_block = jnp.einsum(
            "hts,shv->thv", scores, value_tile_width, precision=highest_precision
        )
        inside_block = inside_block + jnp.einsum(
            "jwo,wos->jws",
            question_patch_lines * jnp.exp(running_state),
            recurrent_state,
            precision=highest_precision,
        )
        final_state = running_state[-1]
        faded_memory_matrix = block_k * jnp.exp(final_state[None] - running_state)
        recurrent_state = recurrent_state * jnp.exp(final_state)[:, :, None] + jnp.einsum(
            "zcb,zcw->cbw", faded_memory_matrix, value_tile_width, precision=highest_precision
        )
        reaching_keys = question_patch_lines * jnp.exp(offset[None] + running_state)
        return ((recurrent_state, offset + final_state), (inside_block, reaching_keys))

    start_carry = (
        jnp.zeros((head_count, key_dim, value_dim), jnp.float32),
        jnp.zeros((head_count, key_dim), jnp.float32),
    )
    (recurrent_state, total_decay), (inside_block, reaching_keys) = lax.scan(
        advance,
        start_carry,
        (
            split_blocks(queries),
            split_blocks(keys_in),
            split_blocks(values_in),
            split_blocks(log_decay),
        ),
    )
    return (
        recurrent_state,
        total_decay,
        inside_block.reshape(tok_rows, head_count, value_dim),
        reaching_keys.reshape(tok_rows, head_count, key_dim),
    )


def body(
    tokens,
    norm_gain,
    query_attend,
    key_attend,
    value_attend,
    query_linear,
    key_linear,
    value_linear,
    decay_down,
    decay_up,
    decay_bias,
    log_retain,
    query_gain,
    key_gain,
    diff_lambda,
    mix_gain,
    state_gain,
    init_state,
    output_attend,
    output_linear,
):
    fs_size = lax.axis_size("fs")
    tp_size = lax.axis_size("tp")
    tp_rank = lax.axis_index("tp")
    tok_rows = tokens.shape[1]
    normed = rms_scale(tokens, norm_gain).astype(jnp.bfloat16)
    normed_rows = normed[0]
    local_weights = (query_attend, key_attend, value_attend, query_linear, key_linear, value_linear)
    widths = [weight.shape[1] * weight.shape[2] for weight in local_weights]
    packed = jnp.concatenate(
        [weight.reshape(weight.shape[0], -1) for weight in local_weights], axis=1
    )
    computed = jnp.einsum(
        "std,dp->stp",
        lax.all_gather(normed, "fs", axis=0, tiled=True),
        packed,
        preferred_element_type=jnp.float32,
    ).astype(jnp.bfloat16)
    arrived = lax.all_to_all(computed, "fs", split_axis=0, concat_axis=2, tiled=True).reshape(
        tok_rows, fs_size, -1
    )
    sections = []
    column_at = 0
    for weight, width_now in zip(local_weights, widths):
        section = arrived[:, :, column_at : column_at + width_now]
        sections.append(section.reshape(tok_rows, fs_size * weight.shape[1], weight.shape[2]))
        column_at = column_at + width_now
    projected = tuple(sections)
    q_pair, k_pair, v_attend, q_lin, k_lin, v_lin = projected
    head_ids = head_order(fs_size, tp_size, tp_rank)
    head_count = head_ids.shape[0]
    q_unit = rms_scale(q_pair.reshape(tok_rows, head_count, 2, HD_A), query_gain).astype(
        jnp.bfloat16
    )
    k_unit = rms_scale(
        k_pair.reshape(tok_rows, head_count, 2, HD_A), jnp.take(key_gain, head_ids, axis=0)
    ).astype(jnp.bfloat16)
    sp_start = lax.axis_index("sp") * tok_rows
    query_block = (sp_start + jnp.arange(tok_rows, dtype=jnp.int32)) // BLK
    score_scale = HD_A ** (-0.5)
    blank_attend = (
        jnp.full((head_count, 2, tok_rows), -jnp.inf, jnp.float32),
        jnp.zeros((head_count, 2, tok_rows), jnp.float32),
        jnp.zeros((head_count, 2, tok_rows, DV_A), jnp.float32),
    )
    carry = blank_attend
    seg_keys = lax.all_gather(k_unit, "sp", axis=0, tiled=True)
    seg_values = lax.all_gather(v_attend, "sp", axis=0, tiled=True)
    span = seg_keys.shape[0]
    stride_token_lines = 2 * tok_rows
    step_count = span // stride_token_lines
    key_steps = seg_keys.reshape(step_count, stride_token_lines, head_count, 2, HD_A)
    value_steps = seg_values.reshape(step_count, stride_token_lines, head_count, DV_A)

    def one_step(running_state, inputs_now):
        step_index, key_step, value_step = inputs_now
        key_start = step_index * stride_token_lines

        def compute(current):
            run_max, run_total, run_acc = current
            scores = (
                jnp.einsum("qhmd,khmd->hmqk", q_unit, key_step, preferred_element_type=jnp.float32)
                * score_scale
            )
            key_block = (key_start + jnp.arange(stride_token_lines, dtype=jnp.int32)) // BLK
            allowed = query_block[:, None] >= key_block[None, :]
            scores = jnp.where(allowed, scores, -jnp.inf)
            new_max = jnp.maximum(run_max, jnp.max(scores, axis=-1))
            factor = jnp.exp(run_max - new_max)
            raised = jnp.exp(scores - new_max[..., None])
            run_total = run_total * factor + jnp.sum(raised, axis=-1)
            run_acc = run_acc * factor[..., None] + jnp.einsum(
                "hmqk,khv->hmqv",
                raised.astype(jnp.bfloat16),
                value_step,
                preferred_element_type=jnp.float32,
            )
            return (new_max, run_total, run_acc)

        def unchanged(current):
            return current

        return (lax.cond(key_start <= sp_start, compute, unchanged, running_state), None)

    carry, _ = lax.scan(
        one_step, carry, (jnp.arange(step_count, dtype=jnp.int32), key_steps, value_steps)
    )
    run_max, run_total, run_acc = carry
    lambda_heads = jnp.take(diff_lambda, head_ids, axis=0)
    diff_raw = (
        run_acc[:, 0] / run_total[:, 0, :, None]
        - lambda_heads[:, None, None] * run_acc[:, 1] / run_total[:, 1, :, None]
    )
    attend_out = rms_scale(jnp.transpose(diff_raw, (1, 0, 2)), mix_gain).astype(jnp.bfloat16)
    low_rank = jnp.dot(normed_rows, decay_down, preferred_element_type=jnp.float32).astype(
        jnp.bfloat16
    )
    up_columns = jnp.take(decay_up, head_ids, axis=1)
    pre_act = jnp.einsum(
        "tr,rhk->thk", low_rank, up_columns, preferred_element_type=jnp.float32
    ) + jnp.take(decay_bias, head_ids, axis=0)
    retain_heads = jnp.take(log_retain[0], head_ids, axis=1)
    log_decay = jax.nn.log_sigmoid(pre_act) / decay_tau + retain_heads[:, :, None]
    local_state, local_decay, inside_block, reaching_keys = linear_blocks(
        q_lin.astype(jnp.float32) * HDK ** (-0.5),
        k_lin.astype(jnp.float32),
        v_lin.astype(jnp.float32),
        log_decay,
    )

    def chain(earlier, later):
        return (earlier[0] + later[0], earlier[1] * jnp.exp(later[0])[:, :, None] + later[1])

    zero_chain = (jnp.zeros_like(local_decay), jnp.zeros_like(local_state))
    prior_decay, prior_state = entering((local_decay, local_state), "sp", chain, zero_chain)
    start_state = lax.all_to_all(init_state, "fs", split_axis=0, concat_axis=1, tiled=True)[0]
    incoming_state = start_state * jnp.exp(prior_decay)[:, :, None] + prior_state
    linear_raw = inside_block + jnp.einsum(
        "jwo,wos->jws", reaching_keys, incoming_state, precision=lax.Precision.HIGHEST
    )
    linear_out = rms_scale(linear_raw, state_gain).astype(jnp.bfloat16)
    out_cols = output_attend.shape[1]
    per_device = MIXER_HEADS // (fs_size * tp_size)
    attend_view = output_attend.reshape(fs_size, tp_size, per_device * DV_A, out_cols)
    linear_view = output_linear.reshape(fs_size, tp_size, per_device * HDV, out_cols)
    blank_out = jnp.zeros((tok_rows, out_cols), jnp.float32)
    running_out = blank_out
    seg_attend = lax.all_gather(attend_out, "tp", axis=1, tiled=True)
    seg_linear = lax.all_gather(linear_out, "tp", axis=1, tiled=True)
    shard_count = seg_attend.shape[1] // head_count
    first_rank = jnp.int32(0) // head_count
    for shard_step in range(shard_count):
        owner_rank = first_rank + shard_step
        rows_attend = lax.dynamic_index_in_dim(attend_view, owner_rank, 1, keepdims=False).reshape(
            -1, out_cols
        )
        rows_linear = lax.dynamic_index_in_dim(linear_view, owner_rank, 1, keepdims=False).reshape(
            -1, out_cols
        )
        part_attend = seg_attend[
            :, shard_step * head_count : (shard_step + 1) * head_count
        ].reshape(tok_rows, -1)
        part_linear = seg_linear[
            :, shard_step * head_count : (shard_step + 1) * head_count
        ].reshape(tok_rows, -1)
        running_out = running_out + jnp.dot(
            part_attend, rows_attend, preferred_element_type=jnp.float32
        )
        running_out = running_out + jnp.dot(
            part_linear, rows_linear, preferred_element_type=jnp.float32
        )
    return running_out.astype(jnp.bfloat16).reshape(1, tok_rows, out_cols)


MESH = pl.DeviceIdType.MESH


def group_barrier(n, fs_size, tp_size):
    z, f, c = lax.axis_index("sp"), lax.axis_index("fs"), lax.axis_index("tp")
    barrier = pltpu.get_barrier_semaphore()
    total = n * fs_size * tp_size
    me = (z * fs_size + f) * tp_size + c
    for k in range(1, total):
        other = lax.rem(me + k, total)
        oz = other // (fs_size * tp_size)
        of = lax.rem(other // tp_size, fs_size)
        oc = lax.rem(other, tp_size)
        pl.semaphore_signal(
            barrier, inc=1, device_id={"sp": oz, "fs": of, "tp": oc}, device_id_type=MESH
        )
    pl.semaphore_wait(barrier, total - 1)


def remote(src, dst, send, recv, **where):
    return pltpu.make_async_remote_copy(
        src_ref=src,
        dst_ref=dst,
        send_sem=send,
        recv_sem=recv,
        device_id=where,
        device_id_type=MESH,
    )


def gather_kernel(
    n,
    fs_size,
    tp_size,
    hpd,
    tok_ref,
    ret_ref,
    gain_ref,
    down_ref,
    wq_ref,
    wk_ref,
    wv_ref,
    lq_ref,
    lk_ref,
    lv_ref,
    proj_ref,
    low_ref,
    rout_ref,
    seq_ref,
    relay_ref,
    raw_ref,
    raw_v_ref,
    w_ref,
    recv_a,
    recv_b,
    recv_l,
    recv_r,
    send_x,
    send_row,
    send_rl,
    send_up,
    send_down,
    send_sib,
    send_r,
    loc,
    wsem,
):
    z, f, c = lax.axis_index("sp"), lax.axis_index("fs"), lax.axis_index("tp")
    rows, width = tok_ref.shape
    half = rows // tp_size
    pieces = recv_l.shape[0]
    prow = half // pieces
    loads = [
        pltpu.make_async_copy(ref, raw_ref.at[i], wsem.at[i])
        for i, ref in enumerate((wq_ref, wk_ref, wv_ref, lq_ref, lk_ref))
    ]
    loads.append(pltpu.make_async_copy(lv_ref, raw_v_ref, wsem.at[5]))
    for load in loads:
        load.start()
    group_barrier(n, fs_size, tp_size)
    s = z // hpd
    own = s == f
    strange = jnp.logical_not(own)

    def nearest(seq):
        return jnp.minimum(jnp.maximum(z, seq * hpd), seq * hpd + hpd - 1)

    def piece(zc, core, p):
        return seq_ref.at[pl.ds(pl.multiple_of(zc * rows + core * half + p * prow, prow), prow)]

    lo = f * hpd
    rsends = []
    for j in range(hpd):
        for k in range(fs_size):
            x = lax.rem(f + k, fs_size)
            there = lo + j
            copy = remote(
                ret_ref,
                rout_ref.at[z],
                send_r.at[j * fs_size + k],
                recv_r.at[z],
                sp=there,
                fs=x,
            )
            go = jnp.logical_not((there == z) & (x == f))
            pl.when(go)(copy.start)
            rsends.append((go, copy))
    sends = []
    for p in range(pieces):
        mine = tok_ref.at[pl.ds(pl.multiple_of(c * half + p * prow, prow), prow)]
        there = relay_ref.at[pl.ds(p * prow, prow)]
        over = remote(mine, piece(z, c, p), send_x.at[p], recv_a.at[z, p], fs=1 - f)
        pl.when(own)(over.start)
        lent = remote(mine, there, send_x.at[p], recv_l.at[p], fs=1 - f)
        pl.when(strange)(lent.start)
        along = remote(mine, piece(z, c, p), send_row.at[p], recv_a.at[z, p], sp=nearest(f))
        pl.when(strange)(along.start)
        sends += [(own, over), (strange, lent), (strange, along)]
    full = pl.ds(pl.multiple_of(z * rows, rows), rows)
    local = pltpu.make_async_copy(tok_ref, seq_ref.at[full], loc.at[0])
    local_r = pltpu.make_async_copy(ret_ref, rout_ref.at[z], loc.at[1])
    pl.when(own)(local.start)
    pl.when(own)(local_r.start)

    slot = lax.rem(z, hpd)
    step = 128

    def pick(sources, target_cols, parts, part):
        span = step * parts * hpd
        sel = (
            lax.broadcasted_iota(jnp.int32, (step, span), 1)
            == (lax.broadcasted_iota(jnp.int32, (step, span), 0) * parts + part) * hpd + slot
        ).astype(jnp.bfloat16)
        for i in range(width // step):
            blocks = [source[i * span : (i + 1) * span, :] for source in sources]
            block = blocks[0] if len(blocks) == 1 else jnp.concatenate(blocks, axis=1)
            w_ref[i * step : (i + 1) * step, target_cols] = jnp.dot(
                sel, block, preferred_element_type=jnp.float32
            ).astype(jnp.bfloat16)

    def pick_all(first, last):
        for i in range(first, min(last, 5), 2):
            group = range(i, min(i + 2, 5))
            for j in group:
                loads[j].wait()
            pick([raw_ref.at[j] for j in group], slice(i * 128, (group[-1] + 1) * 128), 1, 0)
        if last > 5:
            loads[5].wait()
            for part in range(2):
                pick([raw_v_ref], slice((5 + part) * 128, (6 + part) * 128), 2, part)

    mlo = s * hpd
    mhi = mlo + hpd - 1

    def relay(p):
        held = relay_ref.at[pl.ds(p * prow, prow)]
        lent = remote(held, piece(z, c, p), send_rl.at[p], recv_l.at[p], sp=nearest(1 - f))
        pl.when(own)(lent.wait_recv)
        along = remote(held, piece(z, c, p), send_rl.at[p], recv_a.at[z, p], sp=nearest(1 - f))
        pl.when(own)(along.start)
        sends.append((own, along))

    def handle(zc, p, act, away):
        block = piece(zc, c, p)
        arrive = remote(block, block, send_sib.at[zc, p], recv_a.at[zc, p], tp=1 - c)
        pl.when(away)(arrive.wait_recv)
        up = remote(
            block, block, send_up.at[zc, p], recv_a.at[zc, p], sp=jnp.minimum(z + 1, n - 1)
        )
        go_up = act & (zc <= z) & (z + 1 <= mhi)
        pl.when(go_up)(up.start)
        down = remote(
            block, block, send_down.at[zc, p], recv_a.at[zc, p], sp=jnp.maximum(z - 1, 0)
        )
        go_down = act & (zc >= z) & (z - 1 >= mlo)
        pl.when(go_down)(down.start)
        sib = remote(block, block, send_sib.at[zc, p], recv_b.at[zc, p], tp=1 - c)
        pl.when(away)(sib.start)
        sends.extend([(go_up, up), (go_down, down), (away, sib)])

    def early(p):
        relay(p)
        handle(z, p, z >= 0, strange)

    def rest(p):
        for k in range(n):
            zc = jnp.where(2 * z < n, n - 1 - k, k)
            handle(zc, p, zc != z, zc != z)

    def finish(p):
        for zc in range(n):
            away = jnp.logical_not((zc == z) & own)
            other = piece(zc, 1 - c, p)
            came = remote(other, other, send_sib.at[zc, p], recv_b.at[zc, p], tp=1 - c)
            pl.when(away)(came.wait_recv)
        spots = [
            slice(zc * rows + core * half + p * prow, zc * rows + core * half + (p + 1) * prow)
            for zc in range(n)
            for core in range(tp_size)
        ]
        x = jnp.concatenate([seq_ref[spot, :] for spot in spots], axis=0).astype(jnp.float32)
        scale = lax.rsqrt(jnp.mean(x * x, axis=-1, keepdims=True) + norm_eps)
        normed = (x * scale * gain_ref[...]).astype(jnp.bfloat16)
        made = jnp.dot(normed, w_ref[...], preferred_element_type=jnp.float32).astype(jnp.bfloat16)
        low = lax.dot_general(
            normed, down_ref[...], (((1,), (1,)), ((), ())), preferred_element_type=jnp.float32
        ).astype(jnp.bfloat16)
        for i, spot in enumerate(spots):
            proj_ref[spot, :] = made[i * prow : (i + 1) * prow]
            low_ref[spot, :] = low[i * prow : (i + 1) * prow]

    pl.when(own)(local.wait)
    early(0)
    for p in range(pieces):
        if p + 1 < pieces:
            early(p + 1)
        rest(p)
        if p == 0:
            pick_all(0, 4)
        if p == min(1, pieces - 1):
            pick_all(4, 6)
        if p > 0:
            finish(p - 1)
    finish(pieces - 1)
    pl.when(own)(local_r.wait)
    for go, copy in rsends + sends:
        pl.when(go)(copy.wait_send)
    for zc in range(n):
        away = jnp.logical_not((zc == z) & own)
        came_r = remote(ret_ref, rout_ref.at[zc], send_r.at[0], recv_r.at[zc], tp=1 - c)
        pl.when(away)(came_r.wait_recv)


def interleaved(weight):
    width, hpd, columns = weight.shape
    parts = columns // 128
    return jnp.swapaxes(weight.reshape(width, hpd, parts, 128), 1, 2).reshape(-1, 128)


def gather_positions(tokens, retain, gain, down, weights, n, fs_size, tp_size, hpd):
    rows, width = tokens.shape
    dma = pltpu.SemaphoreType.DMA
    flat = [interleaved(weight) for weight in weights]
    pieces = max(1, rows // tp_size // 16)
    columns = sum(weight.shape[2] for weight in weights)
    vmem = pl.BlockSpec(memory_space=pltpu.VMEM)
    anywhere = pl.BlockSpec(memory_space=pl.ANY)
    return pl.pallas_call(
        functools.partial(gather_kernel, n, fs_size, tp_size, hpd),
        out_shape=(
            jax.ShapeDtypeStruct((n * rows, columns), jnp.bfloat16),
            jax.ShapeDtypeStruct((n * rows, down.shape[0]), jnp.bfloat16),
            jax.ShapeDtypeStruct((n,) + retain.shape, retain.dtype),
        ),
        in_specs=[vmem] * 4 + [anywhere] * 6,
        out_specs=(vmem, vmem, anywhere),
        scratch_shapes=[
            pltpu.VMEM((n * rows, width), jnp.bfloat16),
            pltpu.VMEM((rows // tp_size, width), jnp.bfloat16),
            pltpu.VMEM((5,) + flat[0].shape, jnp.bfloat16),
            pltpu.VMEM(flat[5].shape, jnp.bfloat16),
            pltpu.VMEM((width, columns), jnp.bfloat16),
            dma((n, pieces)),
            dma((n, pieces)),
            dma((pieces,)),
            dma((n,)),
            dma((pieces,)),
            dma((pieces,)),
            dma((pieces,)),
            dma((n, pieces)),
            dma((n, pieces)),
            dma((n, pieces)),
            dma((hpd * fs_size,)),
            dma((2,)),
            dma((6,)),
        ],
        compiler_params=pltpu.CompilerParams(collective_id=0, has_side_effects=True),
    )(tokens, retain, gain, down, *flat)


def mix_kernel(
    hpd,
    tp_size,
    lam_ref,
    proj_ref,
    low_ref,
    ret_ref,
    up_ref,
    bias_ref,
    qg_ref,
    kg_ref,
    mg_ref,
    sg_ref,
    init_ref,
    out_ref,
):
    z, f, c = lax.axis_index("sp"), lax.axis_index("fs"), lax.axis_index("tp")
    slot = lax.rem(z, hpd)
    seq = z // hpd
    head = (f * tp_size + c) * hpd + slot
    f32, bf16 = jnp.float32, jnp.bfloat16
    length = proj_ref.shape[0]
    lane = lax.broadcasted_iota(jnp.int32, (1, 2 * HD_A), 1)
    first = lane < HD_A

    def unit(cols, gain):
        x = proj_ref[:, cols].astype(f32)
        sq = x * x
        m0 = jnp.sum(jnp.where(first, sq, 0.0), axis=-1, keepdims=True) / HD_A
        m1 = jnp.sum(jnp.where(first, 0.0, sq), axis=-1, keepdims=True) / HD_A
        r = jnp.where(first, lax.rsqrt(m0 + norm_eps), lax.rsqrt(m1 + norm_eps))
        return (x * r * gain).astype(bf16)

    q_gain = jnp.concatenate([qg_ref[...], qg_ref[...]], axis=1)
    k_pair = kg_ref[pl.ds(head, 1)]
    k_gain = jnp.concatenate([k_pair[:, 0], k_pair[:, 1]], axis=1)
    q_unit = unit(slice(0, 128), q_gain)
    k_unit = unit(slice(128, 256), k_gain)
    zero = jnp.zeros_like(q_unit)
    q_maps = (jnp.where(first, q_unit, zero), jnp.where(first, zero, q_unit))
    tile = 2 * BLK
    key_b = lax.broadcasted_iota(jnp.int32, (tile, tile), 1) // BLK
    query_b = lax.broadcasted_iota(jnp.int32, (tile, tile), 0) // BLK
    allowed = query_b >= key_b
    lam = lam_ref[head]
    for i in range(length // tile):
        at = slice(i * tile, (i + 1) * tile)
        parts = []
        for m in range(2):
            q = q_maps[m][at]
            diag = (
                lax.dot_general(
                    q, k_unit[at], (((1,), (1,)), ((), ())), preferred_element_type=f32
                )
                * HD_A ** (-0.5)
            )
            diag = jnp.where(allowed, diag, -jnp.inf)
            top = jnp.max(diag, axis=-1, keepdims=True)
            if i > 0:
                past = (
                    lax.dot_general(
                        q,
                        k_unit[: i * tile],
                        (((1,), (1,)), ((), ())),
                        preferred_element_type=f32,
                    )
                    * HD_A ** (-0.5)
                )
                top = jnp.maximum(top, jnp.max(past, axis=-1, keepdims=True))
            raised = jnp.exp(diag - top)
            total = jnp.sum(raised, axis=-1, keepdims=True)
            acc = jnp.dot(raised.astype(bf16), proj_ref[at, 256:384], preferred_element_type=f32)
            if i > 0:
                raised = jnp.exp(past - top)
                total = total + jnp.sum(raised, axis=-1, keepdims=True)
                acc = acc + jnp.dot(
                    raised.astype(bf16), proj_ref[: i * tile, 256:384], preferred_element_type=f32
                )
            parts.append(acc / total)
        diff = parts[0] - lam * parts[1]
        scale = lax.rsqrt(jnp.mean(diff * diff, axis=-1, keepdims=True) + norm_eps)
        out_ref[at, :DV_A] = (diff * scale * mg_ref[...]).astype(bf16)

    ups = up_ref[...].astype(f32)
    chosen_head = lax.broadcasted_iota(jnp.int32, ups.shape, 1) == head
    up = jnp.sum(jnp.where(chosen_head, ups, 0.0), axis=1).astype(bf16)
    bias = bias_ref[pl.ds(head, 1), :]
    r64 = lax.broadcasted_iota(jnp.int32, (BLK, BLK), 0)
    c64 = lax.broadcasted_iota(jnp.int32, (BLK, BLK), 1)
    causal = r64 >= c64
    lower = causal.astype(f32)
    eye_k = lax.broadcasted_iota(jnp.int32, (HDK, HDK), 0) == lax.broadcasted_iota(
        jnp.int32, (HDK, HDK), 1
    )
    pre = jnp.dot(low_ref[...], up, preferred_element_type=f32) + bias
    log_sig = jnp.minimum(pre, 0.0) - jnp.log1p(jnp.exp(-jnp.abs(pre)))
    log_sig = log_sig / decay_tau
    state = init_ref[pl.ds(seq, 1), pl.ds(slot, 1)].reshape(HDK, HDV)
    rows = ret_ref.shape[2]
    per = rows // BLK
    for b in range(length // BLK):
        at = slice(b * BLK, (b + 1) * BLK)
        ret = ret_ref[b // per, pl.ds(head, 1), :][:, (b % per) * BLK : (b % per + 1) * BLK]
        column = jnp.sum(jnp.where(r64 == c64, ret, 0.0), axis=-1, keepdims=True)
        logs = log_sig[at] + column
        run = jnp.dot(
            lower, logs, preferred_element_type=f32, precision=lax.Precision.HIGHEST
        )
        pivot = run[BLK // 2 : BLK // 2 + 1]
        last = run[BLK - 1 : BLK]
        q = proj_ref[at, 384:512].astype(f32) * HDK ** (-0.5)
        k = proj_ref[at, 512:640].astype(f32)
        v = proj_ref[at, 640:896]
        qs = (q * jnp.exp(run - pivot)).astype(bf16)
        ks = (k * jnp.exp(pivot - run)).astype(bf16)
        inner = lax.dot_general(qs, ks, (((1,), (1,)), ((), ())), preferred_element_type=f32)
        inner = jnp.where(causal, inner, 0.0).astype(bf16)
        raw = jnp.dot(inner, v, preferred_element_type=f32) + jnp.dot(
            (q * jnp.exp(run)).astype(bf16), state.astype(bf16), preferred_element_type=f32
        )
        faded = (k * jnp.exp(last - run)).astype(bf16)
        keep = jnp.sum(jnp.where(eye_k, jnp.exp(last), 0.0), axis=-1, keepdims=True)
        state = state * keep + lax.dot_general(
            faded, v, (((0,), (0,)), ((), ())), preferred_element_type=f32
        )
        scale = lax.rsqrt(jnp.mean(raw * raw, axis=-1, keepdims=True) + norm_eps)
        out_ref[at, DV_A:] = (raw * scale * sg_ref[...]).astype(bf16)


def exchange_kernel(
    n,
    fs_size,
    tp_size,
    hpd,
    mix_ref,
    out_ref,
    stage,
    recv_row,
    recv_x,
    recv_s,
    send_row,
    send_x,
    send_s,
    loc,
):
    z, f, c = lax.axis_index("sp"), lax.axis_index("fs"), lax.axis_index("tp")
    rows = out_ref.shape[1]
    group_barrier(n, fs_size, tp_size)
    s = z // hpd
    keep = s == f
    cross = jnp.logical_not(keep)

    def head(x, core, zs):
        return (x * tp_size + core) * hpd + lax.rem(zs, hpd)

    def chunk(zt):
        return mix_ref.at[pl.ds(pl.multiple_of(zt * rows, rows), rows)]

    my_head = head(f, c, z)
    waits = []
    for k in range(1, n):
        zt = lax.rem(z + k, n)
        kept = remote(chunk(zt), out_ref.at[my_head], send_row.at[k], recv_row.at[z], sp=zt)
        moved = remote(chunk(zt), stage.at[z], send_row.at[k], recv_row.at[z], sp=zt)
        pl.when(keep)(kept.start)
        pl.when(cross)(moved.start)
        waits.append((None, kept))
    local = pltpu.make_async_copy(chunk(z), out_ref.at[my_head], loc)
    pl.when(keep)(local.start)
    sib0 = remote(chunk(z), out_ref.at[my_head], send_s.at[my_head], recv_s.at[my_head], tp=1 - c)
    pl.when(keep)(sib0.start)
    waits.append((keep, sib0))
    x0 = remote(chunk(z), out_ref.at[my_head], send_x.at[0], recv_x.at[my_head], fs=s)
    pl.when(cross)(x0.start)
    waits.append((cross, x0))
    for k in range(1, n):
        zs = lax.rem(z + k, n)
        sq = zs // hpd
        hd = head(f, c, zs)
        final = sq == f
        onward = jnp.logical_not(final)
        landed = remote(stage.at[zs], stage.at[zs], send_x.at[k], recv_row.at[zs], tp=1 - c)
        landed.wait_recv()
        sib = remote(out_ref.at[hd], out_ref.at[hd], send_s.at[hd], recv_s.at[hd], tp=1 - c)
        pl.when(final)(sib.start)
        waits.append((final, sib))
        xs = remote(stage.at[zs], out_ref.at[hd], send_x.at[k], recv_x.at[hd], fs=sq)
        pl.when(onward)(xs.start)
        waits.append((onward, xs))
    for k in range(1, fs_size):
        x = lax.rem(f + k, fs_size)
        for j in range(hpd):
            hd = head(x, c, j)
            block = out_ref.at[hd]
            came = remote(block, block, send_s.at[hd], recv_x.at[hd], tp=1 - c)
            came.wait_recv()
            sib = remote(block, block, send_s.at[hd], recv_s.at[hd], tp=1 - c)
            sib.start()
            waits.append((None, sib))
    for x in range(fs_size):
        for j in range(hpd):
            hd = head(x, 1 - c, j)
            block = out_ref.at[hd]
            remote(block, block, send_s.at[hd], recv_s.at[hd], tp=1 - c).wait_recv()
    pl.when(keep)(local.wait)
    for go, copy in waits:
        if go is None:
            copy.wait_send()
        else:
            pl.when(go)(copy.wait_send)


def exchange_heads(mixed, n, fs_size, tp_size, hpd):
    rows, width = mixed.shape[0] // n, mixed.shape[1]
    heads = fs_size * tp_size * hpd
    dma = pltpu.SemaphoreType.DMA
    return pl.pallas_call(
        functools.partial(exchange_kernel, n, fs_size, tp_size, hpd),
        out_shape=jax.ShapeDtypeStruct((heads, rows, width), mixed.dtype),
        in_specs=[pl.BlockSpec(memory_space=pltpu.VMEM)],
        out_specs=pl.BlockSpec(memory_space=pl.ANY),
        scratch_shapes=[
            pltpu.VMEM((n, rows, width), mixed.dtype),
            dma((n,)),
            dma((heads,)),
            dma((heads,)),
            dma((n,)),
            dma((n,)),
            dma((heads,)),
            dma,
        ],
        compiler_params=pltpu.CompilerParams(collective_id=1, has_side_effects=True),
    )(mixed)


def pair_body(
    tokens,
    norm_gain,
    query_attend,
    key_attend,
    value_attend,
    query_linear,
    key_linear,
    value_linear,
    decay_down,
    decay_up,
    decay_bias,
    log_retain,
    query_gain,
    key_gain,
    diff_lambda,
    mix_gain,
    state_gain,
    init_state,
    output_attend,
    output_linear,
):
    n, fs_size, tp_size = lax.axis_size("sp"), lax.axis_size("fs"), lax.axis_size("tp")
    hpd = query_attend.shape[1]
    weights = (query_attend, key_attend, value_attend, query_linear, key_linear, value_linear)
    projected, low_rank, retained = gather_positions(
        tokens[0],
        jnp.transpose(log_retain[0]),
        norm_gain[None],
        jnp.transpose(decay_down),
        weights,
        n,
        fs_size,
        tp_size,
        hpd,
    )
    vmem = pl.BlockSpec(memory_space=pltpu.VMEM)
    mixed = pl.pallas_call(
        functools.partial(mix_kernel, hpd, tp_size),
        out_shape=jax.ShapeDtypeStruct((projected.shape[0], DV_A + HDV), jnp.bfloat16),
        in_specs=[pl.BlockSpec(memory_space=pltpu.SMEM)] + [vmem] * 10,
        out_specs=vmem,
    )(
        diff_lambda,
        projected,
        low_rank,
        retained,
        decay_up,
        decay_bias,
        query_gain[None],
        key_gain,
        mix_gain[None],
        state_gain[None],
        init_state,
    )
    arrived = exchange_heads(mixed, n, fs_size, tp_size, hpd)
    heads = arrived.shape[0]
    out = jnp.einsum(
        "htw,hwo->to",
        arrived[:, :, :DV_A],
        output_attend.reshape(heads, DV_A, -1),
        preferred_element_type=jnp.float32,
    ) + jnp.einsum(
        "htw,hwo->to",
        arrived[:, :, DV_A:],
        output_linear.reshape(heads, HDV, -1),
        preferred_element_type=jnp.float32,
    )
    return out.astype(jnp.bfloat16)[None]


def solution(mesh):
    in_specs = (
        P(("grp", "fs"), "sp", None),
        P(),
        P(None, ("fs", "tp"), None),
        P(None, ("fs", "tp"), None),
        P(None, ("fs", "tp"), None),
        P(None, ("fs", "tp"), None),
        P(None, ("fs", "tp"), None),
        P(None, ("fs", "tp"), None),
        P(),
        P(),
        P(),
        P(("grp", "fs"), "sp", None),
        P(),
        P(),
        P(),
        P(),
        P(),
        P("grp", ("fs", "tp"), None, None),
        P(None, "tp"),
        P(None, "tp"),
    )
    out_specs = P(("grp", "fs"), "sp", "tp")
    fs_size, tp_size, sp_size = mesh.shape["fs"], mesh.shape["tp"], mesh.shape["sp"]
    pairs = MIXER_HEADS // tp_size
    chosen = pair_body if pairs == sp_size and tp_size == 2 and fs_size == 2 else body
    return jax.shard_map(chosen, mesh=mesh, in_specs=in_specs, out_specs=out_specs, check_vma=False)
```
